256 devices in a mesh: ep: 16 (over y, x), tp: 16 (over z, core).
Axes of the slice: x: 4, y: 4, z: 8, core: 2. Of those that a mesh axis runs over, the one named last changes fastest.
Arguments:
- query_heads_rows: bfloat16 [8192, 2048], P('ep', 'tp'), may hold values from -9 to 9
- key_heads_rows: bfloat16 [8192, 2048], P('ep', 'tp'), may hold values from -9 to 9
- value_heads_rows: bfloat16 [8192, 2048], P('ep', 'tp'), may hold values from -6 to 6
- write_strength_logit: bfloat16 [16, 8192], P('tp', 'ep'), may hold values from -3.5 to -1
- decay_preactivation: bfloat16 [16, 8192], P('tp', 'ep'), may hold values from -5 to 5
- head_decay_logarithm: float32 [16], P('tp'), may hold values from -20 to -3
- extra_log_decay: float32 [16, 8192], P('tp', 'ep'), may hold values from -0.7 to 0
- output_weight: bfloat16 [2048, 2048], P('tp'), may hold values from -2 to 2
- second_batch_tokens: bfloat16 [32768, 2048], P(('ep', 'tp')), may hold values from -6 to 6
- expert_norm_scale: float32 [2048], replicated, may hold values from 0.1 to 1.9
- expert_choice_index: int32 [32768, 2], P(('ep', 'tp')), may hold values from 0 to 15, as said below
- group_router_weight: float32 [32768], P(('ep', 'tp')), may hold values from 0.25 to 1
- expert_logit_difference: float32 [32768], P(('ep', 'tp')), may hold values from -8 to 8
- expert_gate_weight: bfloat16 [16, 1024, 2048], P('ep', 'tp'), may hold values from -0.125 to 0.125
- expert_up_weight: bfloat16 [16, 1024, 2048], P('ep', 'tp'), may hold values from -0.125 to 0.125
- expert_down_weight: bfloat16 [16, 1024, 2048], P('ep', 'tp'), may hold values from -0.375 to 0.375
Outputs:
- mixer_output_first: bfloat16 [8192, 2048], P(('ep', 'tp'))
- expert_out: bfloat16 [32768, 2048], P(('ep', 'tp'))
The draws below stay inside these ranges and needn't reach their ends.
Inputs may be any that keep to these rules, and one draw needn't show every extreme that they name: `expert_choice_index`: each row names two different experts of one group, the experts a * 4 to a * 4 + 3 for some a. In the rows of one device (aligned blocks of 128 rows) no expert is named more than 32 times, and in every device's rows some expert is named exactly 32 times.
All inputs are finite; a program needn't handle non-finite values.
Results may differ from the reference program's by a relative error of at most 0.018.
Values may be sent and summed in bfloat16 or wider, within the bound.
A program may use at most 64 MiB of HBM per device.

```python
import jax
import jax.numpy as jnp
from jax import lax

D = 2048
HEADS = 16
DK = 128
DV = 128
BLOCK = 64
TOK_AEP = 512
SEQ = 8192
TOK_B = 128
CAP = 32
TOKENS_B = 32768
FF = 1024
EXPERTS = 16
GROUPS = 4
EPG = 4
TOPK = 2


def shared_directions(key):
    return jax.random.truncated_normal(jax.random.fold_in(key, 71), -3.0, 3.0, (HEADS, DK))


def coherent_rows(key, salt, lowest, highest):
    level_key, noise_key = jax.random.split(jax.random.fold_in(key, salt))
    direction = shared_directions(key)
    noise = jax.random.truncated_normal(noise_key, -3.0, 3.0, (SEQ, HEADS, DK))
    levels = jax.random.uniform(level_key, (SEQ // BLOCK, HEADS), minval=lowest, maxval=highest)
    per_position = jnp.repeat(levels, BLOCK, axis=0)
    rows = per_position[:, :, None] * direction[None, :, :] + noise
    return rows.reshape(SEQ, HEADS * DK).astype(jnp.bfloat16)


def draw_query_heads_rows(key, part):
    return coherent_rows(key, 13, 0.8, 1.2)


def draw_key_heads_rows(key, part):
    return coherent_rows(key, 12, 1.2, 1.8)


def draw_head_decay_logarithm(key, part):
    pick_key, slow_key, fast_key = jax.random.split(key, 3)
    slow_share = 0.5
    chosen = jax.random.uniform(pick_key, (HEADS,)) < slow_share
    slow_rate = jnp.log(jnp.log(10.0) / (2.4 * SEQ)) + jax.random.uniform(slow_key, (HEADS,), minval=-0.3, maxval=0.3)
    fast_rate = jnp.log(1.0 / 32.0) + jax.random.uniform(fast_key, (HEADS,), minval=-0.3, maxval=0.3)
    return jnp.where(chosen, slow_rate, fast_rate).astype(jnp.float32)


def draw_decay_preactivation(key, part):
    jitter_key, device_key, block_key, run_key = jax.random.split(key, 4)
    segments_count = SEQ // TOK_AEP
    jitter = 0.5 * jax.random.truncated_normal(jitter_key, -3.0, 3.0, (HEADS, SEQ))
    per_device = jax.random.uniform(device_key, (segments_count,), minval=-1.5, maxval=1.5)
    run_start = jax.random.randint(run_key, (), 0, max(segments_count - 2, 1))
    segment_index = jnp.arange(segments_count, dtype=jnp.int32)
    in_run = (segment_index >= run_start) & (segment_index < run_start + 3)
    per_device = jnp.where(in_run, -3.0, per_device)
    per_block = jax.random.uniform(block_key, (SEQ // BLOCK,), minval=-0.5, maxval=0.5)
    offsets = jnp.repeat(per_device, TOK_AEP) + jnp.repeat(per_block, BLOCK)
    return jnp.clip(jitter + offsets[None, :], -5.0, 5.0).astype(jnp.bfloat16)


def draw_extra_log_decay(key, part):
    place_key, depth_key = jax.random.split(key)
    half_length = SEQ // 2
    places = jax.random.randint(place_key, (HEADS, 2), 0, half_length) + jnp.array([0, half_length], jnp.int32)[None, :]
    depths = jnp.log(jax.random.uniform(depth_key, (HEADS, 2), minval=0.5, maxval=0.8))
    positions = jnp.arange(SEQ, dtype=jnp.int32)
    markers = (positions[None, None, :] == places[:, :, None]).astype(jnp.float32)
    return jnp.sum(markers * depths[:, :, None], axis=1).astype(jnp.float32)


def route_block(block_key):
    hot_key, split_key, order_key = jax.random.split(block_key, 3)
    hot_rows = EPG * CAP // 2
    hot_group = jax.random.randint(hot_key, (), 0, GROUPS)
    remain = jnp.asarray(TOK_B - hot_rows, jnp.int32)
    split_keys = jax.random.split(split_key, GROUPS - 1)
    others = []
    for number in range(GROUPS - 2):
        lowest = jnp.maximum(0, remain - hot_rows * (GROUPS - 2 - number))
        highest = jnp.minimum(hot_rows, remain)
        counted = jax.random.randint(split_keys[number], (), lowest, highest + 1).astype(jnp.int32)
        others.append(counted)
        remain = remain - counted
    others.append(remain)
    other_counts = jnp.stack(others).astype(jnp.int32)
    group_index = jnp.arange(GROUPS, dtype=jnp.int32)
    shifted = jnp.clip(group_index - (group_index > hot_group).astype(jnp.int32), 0, GROUPS - 2)
    counts = jnp.where(group_index == hot_group, hot_rows, other_counts[shifted]).astype(jnp.int32)
    group_ends = jnp.cumsum(counts)
    starts = group_ends - counts
    places = jax.random.permutation(order_key, TOK_B).astype(jnp.int32)
    groups = jnp.sum((places[:, None] >= group_ends[None, :]).astype(jnp.int32), axis=1)
    within = places - starts[groups]
    first_id = groups * EPG + within % EPG
    second = groups * EPG + (within + 1 + within // EPG % (EPG - 1)) % EPG
    return jnp.stack([first_id, second], axis=1).astype(jnp.int32)


def draw_expert_choice_index(key, part):
    block_keys = jax.random.split(key, TOKENS_B // TOK_B)
    return jax.vmap(route_block)(block_keys).reshape(TOKENS_B, TOPK).astype(jnp.int32)


def shard_levels(rng, shape, cuts, smallest, top_value):
    loudness, own = 1.0, jax.random.fold_in(rng, 6)
    for dim, blocks in cuts:
        draws = jnp.exp(jax.random.uniform(jax.random.fold_in(own, dim), (blocks,), jnp.float32, smallest / len(cuts), top_value / len(cuts)))
        loudness = loudness * jnp.repeat(draws, shape[dim] // blocks).reshape([-1 if axis == dim else 1 for axis in range(len(shape))])
    return loudness


def normal_values(own_key, extent, deviation, bound, cuts=(), kind=jnp.bfloat16):
    factor_of = shard_levels(own_key, extent, cuts, -0.22, 0.18) if cuts else 1.0
    drawn = jax.random.normal(own_key, extent, jnp.float32) * deviation * factor_of
    return jnp.minimum(jnp.maximum(drawn, -bound), bound).astype(kind)


def setup_inputs(seed: int = 0) -> dict:
    key_of = jax.random.split(jax.random.key(seed), 17)
    query_heads_rows = draw_query_heads_rows(jax.random.fold_in(key_of[16], 71), 0)
    key_heads_rows = draw_key_heads_rows(jax.random.fold_in(key_of[16], 71), 0)
    value_heads_rows = normal_values(key_of[2], (SEQ, HEADS * DV), 1.0, 6.0, ((0, 16), (1, 16)))
    write_strength_logit = jnp.clip(-3.5 + 2.5 * jax.random.uniform(key_of[3], (HEADS, SEQ), jnp.float32) ** shard_levels(key_of[3], (HEADS, SEQ), ((0, 16), (1, 16)), -0.2, 0.2), -3.5, -1.0).astype(jnp.bfloat16)
    decay_preactivation = draw_decay_preactivation(jax.random.fold_in(key_of[16], 71), 0)
    head_decay_logarithm = draw_head_decay_logarithm(jax.random.fold_in(key_of[16], 71), 0)
    extra_log_decay = draw_extra_log_decay(jax.random.fold_in(key_of[16], 71), 0)
    output_weight = normal_values(key_of[7], (HEADS * DV, D), ((HEADS * DV) // 256) ** -0.5, 2.0, ((0, 16),))
    second_batch_tokens = normal_values(key_of[8], (TOKENS_B, D), 1.0, 6.0, ((0, 256),))
    expert_norm_scale = jnp.clip(1.0 + 0.18 * jax.random.normal(key_of[9], (D,), jnp.float32), 0.1, 1.9)
    expert_choice_index = draw_expert_choice_index(jax.random.fold_in(key_of[16], 71), 0)
    group_router_weight = jnp.clip(0.25 + 0.75 * jax.random.uniform(key_of[11], (TOKENS_B,), jnp.float32) ** shard_levels(key_of[11], (TOKENS_B,), ((0, 256),), -0.2, 0.2), 0.25, 1.0)
    expert_logit_difference = normal_values(key_of[12], (TOKENS_B,), 1.5, 8.0, ((0, 256),), jnp.float32)
    expert_gate_weight = normal_values(key_of[13], (EXPERTS, FF, D), D ** -0.5, 0.125, ((0, 16), (1, 16)))
    expert_up_weight = normal_values(key_of[14], (EXPERTS, FF, D), D ** -0.5, 0.125, ((0, 16), (1, 16)))
    expert_down_weight = normal_values(key_of[15], (EXPERTS, FF, D), (FF // 4) ** -0.5, 0.375, ((0, 16), (1, 16)))
    return dict(query_heads_rows=query_heads_rows, key_heads_rows=key_heads_rows, value_heads_rows=value_heads_rows, write_strength_logit=write_strength_logit, decay_preactivation=decay_preactivation, head_decay_logarithm=head_decay_logarithm, extra_log_decay=extra_log_decay, output_weight=output_weight, second_batch_tokens=second_batch_tokens, expert_norm_scale=expert_norm_scale, expert_choice_index=expert_choice_index, group_router_weight=group_router_weight, expert_logit_difference=expert_logit_difference, expert_gate_weight=expert_gate_weight, expert_up_weight=expert_up_weight, expert_down_weight=expert_down_weight)


precise_setting = lax.Precision.HIGHEST
norm_eps = 1e-06

def unit_rows(matrix):
    return matrix * lax.rsqrt(lax.optimization_barrier(jnp.sum(matrix * matrix, axis=-1, keepdims=True)) + norm_eps)

def block_terms(query_block, key_block, value_block, decay_logarithm, strength):
    span_len = query_block.shape[2]
    dim_value = value_block.shape[-1]
    cumulative = jnp.cumsum(decay_logarithm, axis=-1)
    within = jnp.tril(jnp.ones((span_len, span_len), bool))
    strict = jnp.tril(jnp.ones((span_len, span_len), bool), -1)
    spread = cumulative[..., :, None] - cumulative[..., None, :]
    decayed = jnp.where(within, jnp.exp(jnp.where(within, spread, 0.0)), 0.0)
    weighted = key_block * strength[..., None]
    lower_part = jnp.where(strict, jnp.einsum('hnid,hnjd->hnij', weighted, key_block, precision=precise_setting) * decayed, 0.0)
    system = lower_part + jnp.eye(span_len, dtype=jnp.float32)
    rhs_cols = jnp.concatenate([value_block * strength[..., None], weighted * jnp.exp(cumulative)[..., None]], axis=-1)
    solved = jax.scipy.linalg.solve_triangular(system, rhs_cols, lower=True, unit_diagonal=True)
    updated_values = solved[..., :dim_value]
    delta_corrections = solved[..., dim_value:]
    scores = jnp.where(within, jnp.einsum('hnid,hnjd->hnij', query_block, key_block, precision=precise_setting) * decayed, 0.0)
    decayed_queries = query_block * jnp.exp(cumulative)[..., None]
    decayed_keys = key_block * jnp.exp(cumulative[..., -1:] - cumulative)[..., None]
    block_retention = jnp.exp(cumulative[..., -1])
    return (decayed_queries, decayed_keys, updated_values, delta_corrections, scores, block_retention)

def carry_step(recurrent_state, inputs):
    decayed_queries, decayed_keys, updated_values, delta_corrections, scores, block_retention = inputs
    value_updates = updated_values - jnp.einsum('jdb,jbu->jdu', delta_corrections, recurrent_state, precision=precise_setting)
    final_output = jnp.einsum('jdb,jbu->jdu', decayed_queries, recurrent_state, precision=precise_setting)
    final_output = final_output + jnp.einsum('hcj,hjv->hcv', scores, value_updates, precision=precise_setting)
    recurrent_state = recurrent_state * block_retention[:, None, None] + jnp.einsum('rpq,rpd->rqd', decayed_keys, value_updates, precision=precise_setting)
    return (recurrent_state, final_output)

def mixer_portion(query_heads_rows, key_heads_rows, value_heads_rows, write_strength_logit, decay_preactivation, head_decay_logarithm, extra_log_decay, output_weight):
    length = query_heads_rows.shape[0]
    blocks = length // BLOCK

    def heads_first(matrix):
        spread_out = matrix.astype(jnp.float32).reshape(length, HEADS, -1).transpose(1, 0, 2)
        return spread_out.reshape(HEADS, blocks, BLOCK, -1)
    query_block = unit_rows(heads_first(query_heads_rows)) * DK ** (-0.5)
    key_block = unit_rows(heads_first(key_heads_rows))
    value_block = heads_first(value_heads_rows)
    strength = jax.nn.sigmoid(write_strength_logit.astype(jnp.float32)).reshape(HEADS, blocks, BLOCK)
    decay_logarithm = -jnp.exp(head_decay_logarithm)[:, None] * jax.nn.softplus(decay_preactivation.astype(jnp.float32)) + extra_log_decay
    decay_logarithm = decay_logarithm.reshape(HEADS, blocks, BLOCK)
    terms = block_terms(query_block, key_block, value_block, decay_logarithm, strength)
    inputs = tuple((jnp.moveaxis(term, 1, 0) for term in terms))
    _, outputs = lax.scan(carry_step, jnp.zeros((HEADS, DK, DV), jnp.float32), inputs)
    attention_result = outputs.transpose(0, 2, 1, 3).reshape(length, HEADS * DV).astype(jnp.bfloat16)
    return jnp.dot(attention_result.astype(jnp.float32), output_weight.astype(jnp.float32), preferred_element_type=jnp.float32).astype(jnp.bfloat16)

def experts_part(second_batch_tokens, expert_norm_scale, expert_choice_index, group_router_weight, expert_logit_difference, expert_gate_weight, expert_up_weight, expert_down_weight):
    widened = second_batch_tokens.astype(jnp.float32)
    normed = (widened * lax.rsqrt(lax.optimization_barrier(jnp.mean(widened * widened, axis=-1, keepdims=True)) + norm_eps) * expert_norm_scale).astype(jnp.bfloat16)
    token_count = second_batch_tokens.shape[0]
    width_model = second_batch_tokens.shape[1]
    flat_ids = expert_choice_index.reshape(-1).astype(jnp.int32)
    copy_count = flat_ids.shape[0]
    sorted_order = jnp.argsort(flat_ids, stable=True).astype(jnp.int32)
    sorted_ids = flat_ids[sorted_order]
    counts = lax.optimization_barrier(jnp.sum((flat_ids[:, None] == jnp.arange(EXPERTS, dtype=jnp.int32)[None, :]).astype(jnp.int32), axis=0))
    starts = jnp.cumsum(counts) - counts
    padded = (counts + 127) // 128 * 128
    pad_ends = jnp.cumsum(padded)
    pad_starts = pad_ends - padded
    destination = (pad_starts[sorted_ids] + jnp.arange(copy_count, dtype=jnp.int32) - starts[sorted_ids]).astype(jnp.int32)
    segments = -(-copy_count // 128) + EXPERTS
    source = jnp.full((segments * 128,), token_count, jnp.int32).at[destination].set((sorted_order // TOPK).astype(jnp.int32))
    padded_rows = jnp.concatenate([normed, jnp.zeros((1, width_model), jnp.bfloat16)], axis=0)
    gathered = padded_rows[source]
    seg_expert = jnp.minimum(jnp.searchsorted(pad_ends, jnp.arange(segments, dtype=jnp.int32) * 128, side='right'), EXPERTS - 1).astype(jnp.int32)

    def one_segment(operands):
        segment_rows, expert = operands
        gating = jnp.dot(segment_rows.astype(jnp.float32), expert_gate_weight[expert].T.astype(jnp.float32), preferred_element_type=jnp.float32)
        upward = jnp.dot(segment_rows.astype(jnp.float32), expert_up_weight[expert].T.astype(jnp.float32), preferred_element_type=jnp.float32)
        hidden = (jax.nn.silu(gating) * upward).astype(jnp.bfloat16)
        return jnp.dot(hidden.astype(jnp.float32), expert_down_weight[expert].astype(jnp.float32), preferred_element_type=jnp.float32).astype(jnp.bfloat16)
    results = lax.map(one_segment, (gathered.reshape(segments, 128, width_model), seg_expert))
    per_copy = results.reshape(-1, width_model)[destination]
    unsorted = jnp.zeros((copy_count, width_model), jnp.bfloat16).at[sorted_order].set(per_copy)
    copies = unsorted.reshape(token_count, TOPK, width_model).astype(jnp.float32)
    leading = jax.nn.sigmoid(expert_logit_difference)
    weights = group_router_weight[:, None] * jnp.stack([leading, 1.0 - leading], axis=-1)
    return lax.optimization_barrier(jnp.sum(weights[..., None] * copies, axis=1)).astype(jnp.bfloat16)

def reference(query_heads_rows, key_heads_rows, value_heads_rows, write_strength_logit, decay_preactivation, head_decay_logarithm, extra_log_decay, output_weight, second_batch_tokens, expert_norm_scale, expert_choice_index, group_router_weight, expert_logit_difference, expert_gate_weight, expert_up_weight, expert_down_weight):
    mixer_output_first = mixer_portion(query_heads_rows, key_heads_rows, value_heads_rows, write_strength_logit, decay_preactivation, head_decay_logarithm, extra_log_decay, output_weight)
    expert_out = experts_part(second_batch_tokens, expert_norm_scale, expert_choice_index, group_router_weight, expert_logit_difference, expert_gate_weight, expert_up_weight, expert_down_weight)
    return (mixer_output_first, expert_out)
```

```python
import jax
import jax.numpy as jnp
from jax import lax
from jax.experimental import pallas as pl
from jax.experimental.pallas import tpu as pltpu
from jax.sharding import PartitionSpec as P

f32 = jnp.float32
bf16 = jnp.bfloat16
MESH = pl.DeviceIdType.MESH
EPS = 1e-06
SEG = 512
DH = 128
W = 2048
CAP = 32
EXPERTS = 16
EP = 16
NZ = 8
SH = 64
TOK = 128
SLOTS = EXPERTS * CAP


def dg(a, b, ca=1, cb=0):
    return lax.dot_general(a, b, (((ca,), (cb,)), ((), ())), preferred_element_type=f32)


def bdot(a, b, ca=1, cb=0):
    return dg(a.astype(bf16), b.astype(bf16), ca, cb)


def halves(a):
    hi = a.astype(bf16)
    return hi, (a - hi.astype(f32)).astype(bf16)


def dot3(a, b, ca=1, cb=0):
    ah, al = halves(a)
    bh, bl = halves(b)
    return dg(ah, bh, ca, cb) + dg(ah, bl, ca, cb) + dg(al, bh, ca, cb)


def iota(shape, dim):
    return lax.broadcasted_iota(jnp.int32, shape, dim)


def softplus(a):
    return jnp.maximum(a, 0.0) + jnp.log(1.0 + jnp.exp(-jnp.abs(a)))


def sigmoid(a):
    return 1.0 / (1.0 + jnp.exp(-a))


def kernel(
    q_ref, k_ref, v_ref, lg_ref, pre_ref, hdl_ref, ex_ref, wo_ref,
    tok_ref, sc_ref, ch_ref, grw_ref, eld_ref, wg_ref, wu_ref, wd_ref,
    o1_ref, o2_ref,
    gu, dw, obuf, xbuf, ybuf, rbuf, acc,
    a_s, s_s, x_s, ol_s, p_s, m_s, st_own, st_all, att_s,
    mine, theirs, pbuf, rrp, rrm, rsp, rsm,
    sp, rp, sm, rm, ps, pr, dsend, drecv, bsend, brecv, ssend, srecv, xs, qs_p, qr_p, qs_m, qr_m,
):
    ep = lax.axis_index("ep")
    tp = lax.axis_index("tp")
    z, c = tp // 2, tp % 2
    y, x = ep // 4, ep % 4
    up = ((z + 1) % NZ) * 2 + c
    down = ((z + NZ - 1) % NZ) * 2 + c
    mate = tp + 1 - 2 * c

    def peer(i):
        return ((y + i // 4) % 4) * 4 + (x + i % 4) % 4

    barrier = pltpu.get_barrier_semaphore()
    for i in range(1, EP):
        pl.semaphore_signal(barrier, inc=1, device_id={"ep": peer(i)}, device_id_type=MESH)
    for t in (up, down, mate):
        pl.semaphore_signal(barrier, inc=1, device_id={"tp": t}, device_id_type=MESH)
    pl.semaphore_wait(barrier, EP - 1 + 3)

    def remote(src, dst, send, recv, **where):
        return pltpu.make_async_remote_copy(
            src_ref=src, dst_ref=dst, send_sem=send, recv_sem=recv, device_id=where, device_id_type=MESH
        )

    def place(zs, core, piece, rows):
        whole = dw.at[zs, core] if piece == 2 else gu.at[zs, piece, core]
        return whole if rows is None else whole.at[pl.ds(rows, SH // 2)]

    own = (wg_ref.at[0], wu_ref.at[0], wd_ref.at[0])

    def ring(s, piece, forward):
        slot = (z + NZ - s) % NZ if forward else (z + s) % NZ
        rows = None if s < 3 else (0 if forward else SH // 2)
        src = own[piece] if s == 0 else place(slot, c, piece, rows)
        dst = place(slot, c, piece, rows)
        if forward:
            return remote(src, dst, sp.at[s, piece], rp.at[s, piece], tp=up)
        return remote(src, dst, sm.at[s, piece], rm.at[s, piece], tp=down)

    def across(n, piece):
        if n == 0:
            slot, rows = z, None
        elif n <= 3:
            slot, rows = (z + NZ - n) % NZ, None
        elif n <= 6:
            slot, rows = (z + n - 3) % NZ, None
        else:
            slot, rows = (z + 4) % NZ, (0 if n == 7 else SH // 2)
        src = own[piece] if n == 0 else place(slot, c, piece, rows)
        return remote(src, place(slot, c, piece, rows), ps.at[n, piece], pr.at[n, piece], tp=mate)

    for piece in range(3):
        ring(0, piece, True).start()
        ring(0, piece, False).start()
    for piece in range(3):
        across(0, piece).start()

    def pump(s, piece):
        ring(s - 1, piece, True).wait_recv()
        if s < 4:
            ring(s, piece, True).start()
        across(s if s < 4 else 7, piece).start()
        ring(s - 1, piece, False).wait_recv()
        if s < 4:
            ring(s, piece, False).start()
        across(3 + s if s < 4 else 8, piece).start()

    gu[z, 0, c] = wg_ref[0]
    gu[z, 1, c] = wu_ref[0]
    dw[z, c] = wd_ref[0]

    wide = tok_ref[...].astype(f32)
    normed = (
        wide * lax.rsqrt(jnp.sum(wide * wide, axis=1, keepdims=True) * (1.0 / W) + EPS) * sc_ref[...]
    ).astype(bf16)
    first, second = ch_ref[:, 0:1], ch_ref[:, 1:2]
    lane16 = iota((TOK, EXPERTS), 1)
    is_first, is_second = lane16 == first, lane16 == second
    member = jnp.where(is_first | is_second, 1.0, 0.0)
    before = jnp.where(iota((TOK, TOK), 1) < iota((TOK, TOK), 0), 1.0, 0.0)
    spot = bdot(before, member) + (lane16 * CAP).astype(f32)
    slot1 = jnp.sum(jnp.where(is_first, spot, 0.0), axis=1, keepdims=True).astype(jnp.int32)
    slot2 = jnp.sum(jnp.where(is_second, spot, 0.0), axis=1, keepdims=True).astype(jnp.int32)
    lanes = iota((TOK, SLOTS), 1)
    pick1 = jnp.where(lanes == slot1, 1.0, 0.0).astype(bf16)
    pick2 = jnp.where(lanes == slot2, 1.0, 0.0).astype(bf16)
    obuf[...] = dg(pick1 + pick2, normed, 0, 0).astype(bf16)

    def dispatch(i):
        return remote(
            obuf.at[pl.ds(peer(i) * CAP, CAP)], xbuf.at[pl.ds(ep * CAP, CAP)], dsend.at[i], drecv.at[i], ep=peer(i)
        )

    def bring_back(i):
        return remote(
            ybuf.at[pl.ds(peer(i) * CAP, CAP)], rbuf.at[pl.ds(ep * CAP, CAP)], bsend.at[i], brecv.at[i], ep=peer(i)
        )

    for i in range(1, EP):
        dispatch(i).start()
    home = pl.ds(pl.multiple_of(ep * CAP, CAP), CAP)
    xbuf[home, :] = obuf[home, :]

    kb, qb = k_ref[...], q_ref[...]
    ld = -jnp.exp(hdl_ref[...]) * softplus(pre_ref[...].astype(f32)) + ex_ref[...]
    beta = sigmoid(lg_ref[...].astype(f32))
    kf = kb.astype(f32)
    k2h, k2l = halves(kf * kf)
    ones = jnp.ones((8, DH), bf16)
    rk_row = lax.rsqrt((dg(ones, k2h, 1, 1) + dg(ones, k2l, 1, 1))[0:1] + EPS)
    upper = jnp.where(iota((SEG, SEG), 0) <= iota((SEG, SEG), 1), 1.0, 0.0).astype(bf16)
    ld8 = jnp.broadcast_to(ld, (8, SEG))
    l1, rest = halves(ld8)
    l2 = (ld8 - l1.astype(f32) - rest.astype(f32)).astype(bf16)
    c_row = (dg(l1, upper) + dg(rest, upper) + dg(l2, upper))[0:1]
    last = c_row[:, SEG - 1 : SEG]
    rhs, kds, qds = [], [], []
    for n in range(SEG // DH):
        rows = slice(n * DH, (n + 1) * DH)
        ii = iota((DH, SEG), 0) + n * DH
        jj = iota((DH, SEG), 1)
        c_col = jnp.sum(jnp.where(jj <= ii, ld, 0.0), axis=1, keepdims=True)
        b_col = jnp.sum(jnp.where(jj == ii, beta, 0.0), axis=1, keepdims=True)
        kt = kf[rows]
        qt = qb[rows].astype(f32)
        rk_col = lax.rsqrt(jnp.sum(kt * kt, axis=1, keepdims=True) + EPS)
        rq_col = lax.rsqrt(jnp.sum(qt * qt, axis=1, keepdims=True) + EPS) * DH**-0.5
        decay = jnp.where(ii >= jj, jnp.exp(jnp.minimum(c_col - c_row, 0.0)), 0.0) * rk_row
        a_s[rows, :] = jnp.where(ii > jj, dg(kb[rows], kb, 1, 1) * decay * (b_col * rk_col), 0.0)
        s_s[rows, :] = dg(qb[rows], kb, 1, 1) * decay * rq_col
        kn = kt * rk_col
        ec = jnp.exp(c_col)
        rhs.append(jnp.concatenate([b_col * v_ref[rows, :].astype(f32), (b_col * ec) * kn], axis=1))
        p_s[rows, :] = qt * (rq_col * ec)
        ol_s[rows, :] = kn * jnp.exp(last - c_col)
    for n in range(SEG // DH):
        x_s[n * DH : (n + 1) * DH, :] = rhs[n]

    pump(1, 0)

    half = SEG // 2
    i2, j2 = iota((half, half), 0), iota((half, half), 1)

    def same(shift):
        return (i2 >> shift) == (j2 >> shift)

    big = [a_s[0:half, 0:half], a_s[half:, half:]]
    power = [jnp.where(same(4), -b, 0.0) for b in big]
    inv = [jnp.where(i2 == j2, 1.0, 0.0) + p for p in power]
    for _ in range(3):
        power = [dot3(p, p) for p in power]
        inv = [t + dot3(t, p) for t, p in zip(inv, power)]
    pump(1, 1)
    for shift in (4, 5, 6, 7):
        off = [jnp.where(same(shift + 1) & ~same(shift), b, 0.0) for b in big]
        mid = [dot3(t, o) for t, o in zip(inv, off)]
        inv = [t - dot3(m, t) for t, m in zip(inv, mid)]
    x1 = dot3(inv[0], x_s[0:half, :])
    x2 = dot3(inv[1], x_s[half:, :] - dot3(a_s[half:, 0:half], x1))
    x_s[0:half, :] = x1
    x_s[half:, :] = x2
    e = dot3(ol_s[...], x_s[...], 0, 0)
    diag = iota((DH, DH), 0) == iota((DH, DH), 1)
    st_own[:, 0:DH] = (jnp.where(diag, jnp.exp(last), 0.0) - e[:, DH:]).astype(bf16)
    st_own[:, DH:] = e[:, :DH].astype(bf16)

    def state(j):
        return remote(st_own, st_all.at[ep], ssend.at[j], srecv.at[ep], ep=j)

    for j in range(1, EP):

        @pl.when(ep < j)
        def _(j=j):
            state(j).start()

    sx = dot3(s_s[...], x_s[...])
    ol_s[...] = sx[:, :DH]
    p_s[...] = p_s[...] - sx[:, DH:]

    pump(1, 2)

    def experts(slots, start, size, begin):
        xt = xbuf[pl.ds(start, size), :]
        total = None
        for zs in slots:
            both = dg(xt, gu[zs].reshape(4 * SH, W), 1, 1)
            g, u = both[:, : 2 * SH], both[:, 2 * SH :]
            h = (g * sigmoid(g) * u).astype(bf16)
            part = dg(h, dw[zs].reshape(2 * SH, W))
            total = part if total is None else total + part
        return total if begin else acc[pl.ds(start, size), :] + total

    MT = 128

    def group(s):
        for n in ((0,) if s == 0 else (s, 3 + s)):
            for piece in range(3):
                across(n, piece).wait_recv()
        slots = (z,) if s == 0 else ((z + NZ - s) % NZ, (z + s) % NZ)

        def body(m, carry):
            start = pl.multiple_of(m * MT, MT)
            acc[pl.ds(start, MT), :] = experts(slots, start, MT, s == 0)
            return carry

        lax.fori_loop(0, SEG // MT, body, 0)

    for i in range(1, EP):
        dispatch(i).wait_recv()
    group(0)
    pump(2, 0)

    m_s[...] = jnp.zeros((DH, DH), f32)
    for j in range(EP - 1):

        @pl.when(j < ep)
        def _(j=j):
            remote(st_own, st_all.at[j], ssend.at[0], srecv.at[j], ep=0).wait_recv()
            m_s[...] = bdot(st_all[j, :, 0:DH], m_s[...]) + st_all[j, :, DH:].astype(f32)

    att = (ol_s[...] + bdot(p_s[...], m_s[...])).astype(bf16)
    att_s[...] = att.reshape(NZ, 2, CAP, DH)
    pump(2, 1)
    theirs[...] = dg(att_s[:, 1 - c].reshape(SEG // 2, DH), wo_ref[...]).astype(bf16).reshape(NZ, CAP, W)
    swap = remote(theirs, pbuf, xs.at[0], xs.at[1], tp=mate)
    swap.start()
    mine[...] = dg(att_s[:, c].reshape(SEG // 2, DH), wo_ref[...]).reshape(NZ, CAP, W)
    pump(2, 2)
    group(1)
    pump(3, 0)
    swap.wait_recv()

    def grow(zs):
        return mine[zs] + pbuf[zs].astype(f32)

    def sums(s, forward):
        if forward:
            return remote(rsp.at[s], rrp.at[s], qs_p.at[s], qr_p.at[s], tp=up)
        return remote(rsm.at[s], rrm.at[s], qs_m.at[s], qr_m.at[s], tp=down)

    rsp[0] = grow((z + 4) % NZ).astype(bf16)
    rsm[0] = grow((z + NZ - 3) % NZ).astype(bf16)
    pump(3, 1)
    group(2)
    pump(3, 2)
    sums(0, True).start()
    sums(0, False).start()
    group(3)
    for piece in range(3):
        pump(4, piece)

    for n in (7, 8):
        for piece in range(3):
            across(n, piece).wait_recv()
    for i in range(4):
        yy = (y + i) % 4
        start = pl.multiple_of(yy * (4 * CAP), 4 * CAP)
        ybuf[pl.ds(start, 4 * CAP), :] = experts(((z + 4) % NZ,), start, 4 * CAP, False).astype(bf16)
        for n in range(4):
            if i + n:
                bring_back(4 * i + n).start()
    rbuf[home, :] = ybuf[home, :]

    for s in range(1, 4):
        sums(s - 1, True).wait_recv()
        rsp[s] = (rrp[s - 1].astype(f32) + grow((z + 4 - s) % NZ)).astype(bf16)
        sums(s, True).start()
        if s < 3:
            sums(s - 1, False).wait_recv()
            rsm[s] = (rrm[s - 1].astype(f32) + grow((z + NZ - 3 + s) % NZ)).astype(bf16)
            sums(s, False).start()
    sums(2, False).wait_recv()
    sums(3, True).wait_recv()
    o1_ref[...] = (grow(z) + rrp[3].astype(f32) + rrm[2].astype(f32)).astype(bf16)

    diag = iota((TOK, TOK), 0) == iota((TOK, TOK), 1)
    lead = sigmoid(eld_ref[...])
    w1 = jnp.sum(jnp.where(diag, grw_ref[...] * lead, 0.0), axis=1, keepdims=True)
    w2 = jnp.sum(jnp.where(diag, grw_ref[...] * (1.0 - lead), 0.0), axis=1, keepdims=True)
    for i in range(1, EP):
        bring_back(i).wait_recv()
    o2_ref[...] = (w1 * dg(pick1, rbuf[...]) + w2 * dg(pick2, rbuf[...])).astype(bf16)

    for s in range(4):
        for piece in range(3):
            ring(s, piece, True).wait_send()
            ring(s, piece, False).wait_send()
        sums(s, True).wait_send()
        if s < 3:
            sums(s, False).wait_send()
    for n in range(9):
        for piece in range(3):
            across(n, piece).wait_send()
    for i in range(1, EP):
        dispatch(i).wait_send()
        bring_back(i).wait_send()
    swap.wait_send()
    for j in range(1, EP):

        @pl.when(ep < j)
        def _(j=j):
            state(j).wait_send()


def shards(q, k, v, lg, pre, hdl, ex, wo, tok, sc, ch, grw, eld, wg, wu, wd):
    V = pltpu.VMEM
    dma = pltpu.SemaphoreType.DMA
    scratch = [
        V((NZ, 2, 2, SH, W), bf16), V((NZ, 2, SH, W), bf16),
        V((SLOTS, W), bf16), V((SLOTS, W), bf16), V((SLOTS, W), bf16), V((SLOTS, W), bf16), V((SLOTS, W), f32),
        V((SEG, SEG), f32), V((SEG, SEG), f32), V((SEG, 2 * DH), f32), V((SEG, DH), f32), V((SEG, DH), f32),
        V((DH, DH), f32), V((DH, 2 * DH), bf16), V((EP, DH, 2 * DH), bf16), V((NZ, 2, CAP, DH), bf16),
        V((NZ, CAP, W), f32), V((NZ, CAP, W), bf16), V((NZ, CAP, W), bf16),
        V((4, CAP, W), bf16), V((3, CAP, W), bf16), V((4, CAP, W), bf16), V((3, CAP, W), bf16),
        dma((4, 3)), dma((4, 3)), dma((4, 3)), dma((4, 3)), dma((9, 3)), dma((9, 3)),
        dma((EP,)), dma((EP,)), dma((EP,)), dma((EP,)), dma((EP,)), dma((EP,)), dma((2,)),
        dma((4,)), dma((4,)), dma((3,)), dma((3,)),
    ]
    return pl.pallas_call(
        kernel,
        name="mixer_and_experts",
        out_shape=(jax.ShapeDtypeStruct((CAP, W), bf16), jax.ShapeDtypeStruct((TOK, W), bf16)),
        in_specs=[pl.BlockSpec(memory_space=pltpu.VMEM)] * 16,
        out_specs=(pl.BlockSpec(memory_space=pltpu.VMEM),) * 2,
        scratch_shapes=scratch,
        compiler_params=pltpu.CompilerParams(
            collective_id=0, has_side_effects=True, vmem_limit_bytes=60 * 1024 * 1024
        ),
    )(
        q, k, v, lg, pre, hdl.reshape(1, 1), ex, wo,
        tok, sc.reshape(1, W), ch, grw.reshape(1, TOK), eld.reshape(1, TOK), wg, wu, wd,
    )


def solution(mesh):
    both = ("ep", "tp")
    placed = (
        P("ep", "tp"), P("ep", "tp"), P("ep", "tp"),
        P("tp", "ep"), P("tp", "ep"), P("tp"), P("tp", "ep"), P("tp", None),
        P(both, None), P(), P(both, None), P(both), P(both),
        P("ep", "tp", None), P("ep", "tp", None), P("ep", "tp", None),
    )
    return jax.shard_map(
        shards, mesh=mesh, in_specs=placed, out_specs=(P(both, None), P(both, None)), check_vma=False
    )
```

```python
import jax
import jax.numpy as jnp
from jax import lax
from jax.experimental import pallas as pl
from jax.experimental.pallas import tpu as pltpu
from jax.sharding import PartitionSpec as P

f32 = jnp.float32
bf16 = jnp.bfloat16
MESH = pl.DeviceIdType.MESH
EPS = 1e-06
SEG = 512
DH = 128
W = 2048
CAP = 32
EXPERTS = 16
EP = 16
NZ = 8
SH = 64
TOK = 128
SLOTS = EXPERTS * CAP
RELAY = {10: 15, 8: 4, 9: 13, 11: 7, 6: 7, 14: 13, 2: 1}
ORDER = list(RELAY)
DIRECT = [i for i in range(1, 16) if i not in RELAY]


def minus(i, j):
    return ((i // 4 - j // 4) % 4) * 4 + (i % 4 - j % 4) % 4


def dg(a, b, ca=1, cb=0):
    return lax.dot_general(a, b, (((ca,), (cb,)), ((), ())), preferred_element_type=f32)


def bdot(a, b, ca=1, cb=0):
    return dg(a.astype(bf16), b.astype(bf16), ca, cb)


def halves(a):
    hi = a.astype(bf16)
    return hi, (a - hi.astype(f32)).astype(bf16)


def dot3(a, b, ca=1, cb=0):
    ah, al = halves(a)
    bh, bl = halves(b)
    return dg(ah, bh, ca, cb) + dg(ah, bl, ca, cb) + dg(al, bh, ca, cb)


def iota(shape, dim):
    return lax.broadcasted_iota(jnp.int32, shape, dim)


def softplus(a):
    return jnp.maximum(a, 0.0) + jnp.log(1.0 + jnp.exp(-jnp.abs(a)))


def sigmoid(a):
    return 1.0 / (1.0 + jnp.exp(-a))


def kernel(
    q_hbm, k_hbm, v_hbm, lg_ref, pre_ref, hdl_ref, ex_ref, wo_hbm,
    tok_hbm, sc_ref, ch_ref, grw_ref, eld_ref, wg_hbm, wu_hbm, wd_hbm,
    o1_ref, o2_ref,
    q_ref, k_ref, v_ref, wo_ref, tok_ref,
    gu, dw, obuf, xbuf, ybuf, rbuf, acc, dhop, bhop, h_s,
    a_s, s_s, x_s, ol_s, p_s, m_s, st_own, st_all, att_s,
    mine, theirs, pbuf, rrp, rrm, rsp, rsm,
    sp, rp, sm, rm, ps, pr, dsend, drecv, dhs, dhr, bsend, brecv, bhs, bhr,
    ssend, srecv, xs, qs_p, qr_p, qs_m, qr_m, ins,
):
    ep = lax.axis_index("ep")
    tp = lax.axis_index("tp")
    z, c = tp // 2, tp % 2
    y, x = ep // 4, ep % 4
    up = ((z + 1) % NZ) * 2 + c
    down = ((z + NZ - 1) % NZ) * 2 + c
    mate = tp + 1 - 2 * c

    def peer(i):
        return ((y + i // 4) % 4) * 4 + (x + i % 4) % 4

    def loaded(n):
        pairs = (
            (wg_hbm.at[0], gu.at[z, 0, c]), (wu_hbm.at[0], gu.at[z, 1, c]), (wd_hbm.at[0], dw.at[z, c]),
            (tok_hbm, tok_ref), (k_hbm, k_ref), (q_hbm, q_ref), (v_hbm, v_ref), (wo_hbm, wo_ref),
        )
        return pltpu.make_async_copy(*pairs[n], ins.at[n])

    for n in range(8):
        loaded(n).start()

    barrier = pltpu.get_barrier_semaphore()
    for i in range(1, EP):
        pl.semaphore_signal(barrier, inc=1, device_id={"ep": peer(i)}, device_id_type=MESH)
    for t in (up, down, mate):
        pl.semaphore_signal(barrier, inc=1, device_id={"tp": t}, device_id_type=MESH)
    pl.semaphore_wait(barrier, EP - 1 + 3)

    def remote(src, dst, send, recv, **where):
        return pltpu.make_async_remote_copy(
            src_ref=src, dst_ref=dst, send_sem=send, recv_sem=recv, device_id=where, device_id_type=MESH
        )

    def place(zs, core, piece, rows):
        whole = dw.at[zs, core] if piece == 2 else gu.at[zs, piece, core]
        return whole if rows is None else whole.at[pl.ds(rows, SH // 2)]

    def ring(s, piece, forward):
        slot = (z + NZ - s) % NZ if forward else (z + s) % NZ
        rows = None if s < 3 else (0 if forward else SH // 2)
        here = place(slot, c, piece, rows)
        if forward:
            return remote(here, here, sp.at[s, piece], rp.at[s, piece], tp=up)
        return remote(here, here, sm.at[s, piece], rm.at[s, piece], tp=down)

    def across(n, piece):
        if n == 0:
            slot, rows = z, None
        elif n <= 3:
            slot, rows = (z + NZ - n) % NZ, None
        elif n <= 6:
            slot, rows = (z + n - 3) % NZ, None
        else:
            slot, rows = (z + 4) % NZ, (0 if n == 7 else SH // 2)
        here = place(slot, c, piece, rows)
        return remote(here, here, ps.at[n, piece], pr.at[n, piece], tp=mate)

    for piece in range(3):
        loaded(piece).wait()
    for piece in range(3):
        ring(0, piece, True).start()
        ring(0, piece, False).start()
    for piece in range(3):
        across(0, piece).start()

    def pump(s, piece):
        ring(s - 1, piece, True).wait_recv()
        if s < 4:
            ring(s, piece, True).start()
        across(s if s < 4 else 7, piece).start()
        ring(s - 1, piece, False).wait_recv()
        if s < 4:
            ring(s, piece, False).start()
        across(3 + s if s < 4 else 8, piece).start()

    loaded(3).wait()
    wide = tok_ref[...].astype(f32)
    normed = (
        wide * lax.rsqrt(jnp.sum(wide * wide, axis=1, keepdims=True) * (1.0 / W) + EPS) * sc_ref[...]
    ).astype(bf16)
    eye = iota((TOK, TOK), 0) == iota((TOK, TOK), 1)
    first = jnp.sum(jnp.where(eye, ch_ref[0:1, :], 0), axis=1, keepdims=True)
    second = jnp.sum(jnp.where(eye, ch_ref[1:2, :], 0), axis=1, keepdims=True)
    lane16 = iota((TOK, EXPERTS), 1)
    is_first, is_second = lane16 == first, lane16 == second
    member = jnp.where(is_first | is_second, 1.0, 0.0)
    before = jnp.where(iota((TOK, TOK), 1) < iota((TOK, TOK), 0), 1.0, 0.0)
    spot = bdot(before, member) + (lane16 * CAP).astype(f32)
    slot1 = jnp.sum(jnp.where(is_first, spot, 0.0), axis=1, keepdims=True).astype(jnp.int32)
    slot2 = jnp.sum(jnp.where(is_second, spot, 0.0), axis=1, keepdims=True).astype(jnp.int32)
    lanes = iota((TOK, SLOTS), 1)
    pick1 = jnp.where(lanes == slot1, 1.0, 0.0).astype(bf16)
    pick2 = jnp.where(lanes == slot2, 1.0, 0.0).astype(bf16)
    obuf[...] = dg(pick1 + pick2, normed, 0, 0).astype(bf16)

    def route(src, dst, hop, send, recv, hsend, hrecv):
        def first_leg(i):
            block = src.at[pl.ds(peer(i) * CAP, CAP)]
            if i in RELAY:
                n = ORDER.index(i)
                return remote(block, hop.at[n], send.at[i], hrecv.at[n], ep=peer(RELAY[i]))
            return remote(block, dst.at[pl.ds(ep * CAP, CAP)], send.at[i], recv.at[i], ep=peer(i))

        def second_leg(i):
            n = ORDER.index(i)
            origin = peer(minus(0, RELAY[i]))
            there = dst.at[pl.ds(origin * CAP, CAP)]
            return remote(hop.at[n], there, hsend.at[n], recv.at[i], ep=peer(minus(i, RELAY[i])))

        def last(i):
            return remote(src.at[pl.ds(0, CAP)], dst.at[pl.ds(0, CAP)], send.at[i], recv.at[i], ep=peer(i))

        def forward(i):
            first_leg(i).wait_recv()
            second_leg(i).start()

        def drain():
            for i in range(1, EP):
                first_leg(i).wait_send()
            for i in ORDER:
                second_leg(i).wait_send()

        return first_leg, forward, last, drain

    d_first, d_forward, d_last, d_drain = route(obuf, xbuf, dhop, dsend, drecv, dhs, dhr)
    b_first, b_forward, b_last, b_drain = route(ybuf, rbuf, bhop, bsend, brecv, bhs, bhr)
    for i in ORDER + DIRECT:
        d_first(i).start()
    home = pl.ds(pl.multiple_of(ep * CAP, CAP), CAP)
    xbuf[home, :] = obuf[home, :]

    for n in (4, 5, 6):
        loaded(n).wait()
    kb, qb = k_ref[...], q_ref[...]
    ld = -jnp.exp(jnp.full((1, 1), hdl_ref[0], f32)) * softplus(pre_ref[...].astype(f32)) + ex_ref[...]
    beta = sigmoid(lg_ref[...].astype(f32))
    kf = kb.astype(f32)
    k2h, k2l = halves(kf * kf)
    ones = jnp.ones((8, DH), bf16)
    rk_row = lax.rsqrt((dg(ones, k2h, 1, 1) + dg(ones, k2l, 1, 1))[0:1] + EPS)
    upper = jnp.where(iota((SEG, SEG), 0) <= iota((SEG, SEG), 1), 1.0, 0.0).astype(bf16)
    ld8 = jnp.broadcast_to(ld, (8, SEG))
    l1, rest = halves(ld8)
    l2 = (ld8 - l1.astype(f32) - rest.astype(f32)).astype(bf16)
    c_row = (dg(l1, upper) + dg(rest, upper) + dg(l2, upper))[0:1]
    last = c_row[:, SEG - 1 : SEG]
    rhs, kds, qds = [], [], []
    for n in range(SEG // DH):
        rows = slice(n * DH, (n + 1) * DH)
        ii = iota((DH, SEG), 0) + n * DH
        jj = iota((DH, SEG), 1)
        c_col = jnp.sum(jnp.where(jj <= ii, ld, 0.0), axis=1, keepdims=True)
        b_col = jnp.sum(jnp.where(jj == ii, beta, 0.0), axis=1, keepdims=True)
        kt = kf[rows]
        qt = qb[rows].astype(f32)
        rk_col = lax.rsqrt(jnp.sum(kt * kt, axis=1, keepdims=True) + EPS)
        rq_col = lax.rsqrt(jnp.sum(qt * qt, axis=1, keepdims=True) + EPS) * DH**-0.5
        decay = jnp.where(ii >= jj, jnp.exp(jnp.minimum(c_col - c_row, 0.0)), 0.0) * rk_row
        a_s[rows, :] = jnp.where(ii > jj, dg(kb[rows], kb, 1, 1) * decay * (b_col * rk_col), 0.0)
        s_s[rows, :] = dg(qb[rows], kb, 1, 1) * decay * rq_col
        kn = kt * rk_col
        ec = jnp.exp(c_col)
        rhs.append(jnp.concatenate([b_col * v_ref[rows, :].astype(f32), (b_col * ec) * kn], axis=1))
        p_s[rows, :] = qt * (rq_col * ec)
        ol_s[rows, :] = kn * jnp.exp(last - c_col)
    for n in range(SEG // DH):
        x_s[n * DH : (n + 1) * DH, :] = rhs[n]

    half = SEG // 2
    i2, j2 = iota((half, half), 0), iota((half, half), 1)

    def same(shift):
        return (i2 >> shift) == (j2 >> shift)

    big = [a_s[0:half, 0:half], a_s[half:, half:]]
    power = [jnp.where(same(4), -b, 0.0) for b in big]
    inv = [jnp.where(i2 == j2, 1.0, 0.0) + p for p in power]
    for _ in range(3):
        power = [dot3(p, p) for p in power]
        inv = [t + dot3(t, p) for t, p in zip(inv, power)]
    for shift in (4, 5, 6, 7):
        off = [jnp.where(same(shift + 1) & ~same(shift), b, 0.0) for b in big]
        mid = [dot3(t, o) for t, o in zip(inv, off)]
        inv = [t - dot3(m, t) for t, m in zip(inv, mid)]
    x1 = dot3(inv[0], x_s[0:half, :])
    x2 = dot3(inv[1], x_s[half:, :] - dot3(a_s[half:, 0:half], x1))
    x_s[0:half, :] = x1
    x_s[half:, :] = x2
    e = dot3(ol_s[...], x_s[...], 0, 0)
    diag = iota((DH, DH), 0) == iota((DH, DH), 1)
    st_own[:, 0:DH] = (jnp.where(diag, jnp.exp(last), 0.0) - e[:, DH:]).astype(bf16)
    st_own[:, DH:] = e[:, :DH].astype(bf16)

    def state(j):
        return remote(st_own, st_all.at[ep], ssend.at[j], srecv.at[ep], ep=j)

    for j in range(1, EP):

        @pl.when(ep < j)
        def _(j=j):
            state(j).start()

    pump(1, 0)
    sx = dot3(s_s[...], x_s[...])
    ol_s[...] = sx[:, :DH]
    p_s[...] = p_s[...] - sx[:, DH:]
    for i in ORDER[:4]:
        d_forward(i)
    pump(1, 1)
    for i in ORDER[4:]:
        d_forward(i)
    pump(1, 2)
    pump(2, 0)

    def experts(slots, start, size, begin):
        xt = xbuf[pl.ds(start, size), :]
        total = None
        for zs in slots:
            both = dg(xt, gu[zs].reshape(4 * SH, W), 1, 1)
            g, u = both[:, : 2 * SH], both[:, 2 * SH :]
            h = (g * sigmoid(g) * u).astype(bf16)
            part = dg(h, dw[zs].reshape(2 * SH, W))
            total = part if total is None else total + part
        return total if begin else acc[pl.ds(start, size), :] + total

    MT = 256

    def group(s):
        for n in ((0,) if s == 0 else (s, 3 + s)):
            for piece in range(3):
                across(n, piece).wait_recv()
        slots = (z,) if s == 0 else ((z + NZ - s) % NZ, (z + s) % NZ)

        def body(m, carry):
            start = pl.multiple_of(m * MT, MT)
            acc[pl.ds(start, MT), :] = experts(slots, start, MT, s == 0)
            return carry

        lax.fori_loop(0, SEG // MT, body, 0)

    for i in range(1, EP):
        d_last(i).wait_recv()
    group(0)
    pump(2, 1)
    group(1)

    m_s[...] = jnp.zeros((DH, DH), f32)
    for j in range(EP - 1):

        @pl.when(j < ep)
        def _(j=j):
            remote(st_own, st_all.at[j], ssend.at[0], srecv.at[j], ep=0).wait_recv()
            m_s[...] = bdot(st_all[j, :, 0:DH], m_s[...]) + st_all[j, :, DH:].astype(f32)

    att = (ol_s[...] + bdot(p_s[...], m_s[...])).astype(bf16)
    att_s[...] = att.reshape(NZ, 2, CAP, DH)
    loaded(7).wait()
    theirs[...] = dg(att_s[:, 1 - c].reshape(SEG // 2, DH), wo_ref[...]).astype(bf16).reshape(NZ, CAP, W)
    swap = remote(theirs, pbuf, xs.at[0], xs.at[1], tp=mate)
    swap.start()
    mine[...] = dg(att_s[:, c].reshape(SEG // 2, DH), wo_ref[...]).reshape(NZ, CAP, W)
    pump(2, 2)
    pump(3, 0)
    swap.wait_recv()

    def grow(zs):
        return mine[zs] + pbuf[zs].astype(f32)

    def sums(s, forward):
        if forward:
            return remote(rsp.at[s], rrp.at[s], qs_p.at[s], qr_p.at[s], tp=up)
        return remote(rsm.at[s], rrm.at[s], qs_m.at[s], qr_m.at[s], tp=down)

    rsp[0] = grow((z + 4) % NZ).astype(bf16)
    rsm[0] = grow((z + NZ - 3) % NZ).astype(bf16)
    pump(3, 1)
    group(2)
    pump(3, 2)
    sums(0, True).start()
    sums(0, False).start()
    group(3)
    far = (z + 4) % NZ
    for piece in range(2):
        pump(4, piece)
    for n in (7, 8):
        for piece in range(2):
            across(n, piece).wait_recv()
    both = dg(xbuf[...], gu[far].reshape(4 * SH, W), 1, 1)
    g, u = both[:, : 2 * SH], both[:, 2 * SH :]
    h_s[...] = (g * sigmoid(g) * u).astype(bf16)
    pump(4, 2)
    for n in (7, 8):
        across(n, 2).wait_recv()
    for i in (2, 1, 3, 0):
        start = pl.multiple_of(((y + i) % 4) * (4 * CAP), 4 * CAP)
        part = pl.ds(start, 4 * CAP)
        ybuf[part, :] = (acc[part, :] + dg(h_s[part, :], dw[far].reshape(2 * SH, W))).astype(bf16)
        for n in (2, 0, 1, 3):
            if i + n:
                b_first(4 * i + n).start()
    rbuf[home, :] = ybuf[home, :]

    for i in ORDER[:3]:
        b_forward(i)
    for s in range(1, 4):
        sums(s - 1, True).wait_recv()
        rsp[s] = (rrp[s - 1].astype(f32) + grow((z + 4 - s) % NZ)).astype(bf16)
        sums(s, True).start()
        if s < 3:
            sums(s - 1, False).wait_recv()
            rsm[s] = (rrm[s - 1].astype(f32) + grow((z + NZ - 3 + s) % NZ)).astype(bf16)
            sums(s, False).start()
        for i in ORDER[1 + 2 * s : 3 + 2 * s]:
            b_forward(i)
    sums(2, False).wait_recv()
    sums(3, True).wait_recv()
    o1_ref[...] = (grow(z) + rrp[3].astype(f32) + rrm[2].astype(f32)).astype(bf16)

    lead = sigmoid(eld_ref[...])
    w1 = jnp.sum(jnp.where(eye, grw_ref[...] * lead, 0.0), axis=1, keepdims=True)
    w2 = jnp.sum(jnp.where(eye, grw_ref[...] * (1.0 - lead), 0.0), axis=1, keepdims=True)
    for i in range(1, EP):
        b_last(i).wait_recv()
    o2_ref[...] = (w1 * dg(pick1, rbuf[...]) + w2 * dg(pick2, rbuf[...])).astype(bf16)

    for s in range(4):
        for piece in range(3):
            ring(s, piece, True).wait_send()
            ring(s, piece, False).wait_send()
        sums(s, True).wait_send()
        if s < 3:
            sums(s, False).wait_send()
    for n in range(9):
        for piece in range(3):
            across(n, piece).wait_send()
    d_drain()
    b_drain()
    swap.wait_send()
    for j in range(1, EP):

        @pl.when(ep < j)
        def _(j=j):
            state(j).wait_send()


def shards(q, k, v, lg, pre, hdl, ex, wo, tok, sc, ch, grw, eld, wg, wu, wd):
    V = pltpu.VMEM
    dma = pltpu.SemaphoreType.DMA
    scratch = [
        V((SEG, DH), bf16), V((SEG, DH), bf16), V((SEG, DH), bf16), V((DH, W), bf16), V((TOK, W), bf16),
        V((NZ, 2, 2, SH, W), bf16), V((NZ, 2, SH, W), bf16),
        V((SLOTS, W), bf16), V((SLOTS, W), bf16), V((SLOTS, W), bf16), V((SLOTS, W), bf16), V((SLOTS, W), f32),
        V((7, CAP, W), bf16), V((7, CAP, W), bf16), V((SLOTS, 2 * SH), bf16),
        V((SEG, SEG), f32), V((SEG, SEG), f32), V((SEG, 2 * DH), f32), V((SEG, DH), f32), V((SEG, DH), f32),
        V((DH, DH), f32), V((DH, 2 * DH), bf16), V((EP, DH, 2 * DH), bf16), V((NZ, 2, CAP, DH), bf16),
        V((NZ, CAP, W), f32), V((NZ, CAP, W), bf16), V((NZ, CAP, W), bf16),
        V((4, CAP, W), bf16), V((3, CAP, W), bf16), V((4, CAP, W), bf16), V((3, CAP, W), bf16),
        dma((4, 3)), dma((4, 3)), dma((4, 3)), dma((4, 3)), dma((9, 3)), dma((9, 3)),
        dma((EP,)), dma((EP,)), dma((7,)), dma((7,)), dma((EP,)), dma((EP,)), dma((7,)), dma((7,)),
        dma((EP,)), dma((EP,)), dma((2,)), dma((4,)), dma((4,)), dma((3,)), dma((3,)), dma((8,)),
    ]
    vm = pl.BlockSpec(memory_space=pltpu.VMEM)
    hbm = pl.BlockSpec(memory_space=pl.ANY)
    outs = pl.pallas_call(
        kernel,
        name="mixer_and_experts",
        out_shape=(jax.ShapeDtypeStruct((CAP, W), bf16), jax.ShapeDtypeStruct((TOK, W), bf16)),
        in_specs=[hbm, hbm, hbm, vm, vm, pl.BlockSpec(memory_space=pltpu.SMEM), vm, hbm, hbm, vm, vm, vm, vm, hbm, hbm, hbm],
        out_specs=(vm, vm),
        scratch_shapes=scratch,
        compiler_params=pltpu.CompilerParams(
            collective_id=0, has_side_effects=True, vmem_limit_bytes=60 * 1024 * 1024
        ),
    )(
        q, k, v, lg, pre, hdl, ex, wo,
        tok, sc.reshape(1, W), ch.T, grw.reshape(1, TOK), eld.reshape(1, TOK), wg, wu, wd,
    )
    return pl.pallas_call(
        hand_over,
        name="hand_over",
        out_shape=(jax.ShapeDtypeStruct((CAP, W), bf16), jax.ShapeDtypeStruct((TOK, W), bf16)),
        in_specs=[vm, vm],
        out_specs=(vm, vm),
        compiler_params=pltpu.CompilerParams(vmem_limit_bytes=60 * 1024 * 1024),
    )(*outs)


def hand_over(a_ref, b_ref, c_ref, d_ref):
    c_ref[...] = a_ref[...]
    d_ref[...] = b_ref[...]


def solution(mesh):
    both = ("ep", "tp")
    placed = (
        P("ep", "tp"), P("ep", "tp"), P("ep", "tp"),
        P("tp", "ep"), P("tp", "ep"), P("tp"), P("tp", "ep"), P("tp", None),
        P(both, None), P(), P(both, None), P(both), P(both),
        P("ep", "tp", None), P("ep", "tp", None), P("ep", "tp", None),
    )
    return jax.shard_map(
        shards, mesh=mesh, in_specs=placed, out_specs=(P(both, None), P(both, None)), check_vma=False
    )
```

```python
import jax
import jax.numpy as jnp
from jax import lax
from jax.experimental import pallas as pl
from jax.experimental.pallas import tpu as pltpu
from jax.sharding import PartitionSpec as P

f32 = jnp.float32
bf16 = jnp.bfloat16
MESH = pl.DeviceIdType.MESH
EPS = 1e-06
SEG = 512
DH = 128
W = 2048
CAP = 32
EXPERTS = 16
EP = 16
NZ = 8
SH = 64
TOK = 128
CHUNKS = 4
COLS = W // CHUNKS
PIECES = 2 + CHUNKS
SLOTS = EXPERTS * CAP
RELAY = {10: 15, 8: 4, 9: 13, 11: 7, 6: 7, 14: 13, 2: 1}
ORDER = list(RELAY)
DIRECT = [i for i in range(1, 16) if i not in RELAY]


def minus(i, j):
    return ((i // 4 - j // 4) % 4) * 4 + (i % 4 - j % 4) % 4


def dg(a, b, ca=1, cb=0):
    return lax.dot_general(a, b, (((ca,), (cb,)), ((), ())), preferred_element_type=f32)


def bdot(a, b, ca=1, cb=0):
    return dg(a.astype(bf16), b.astype(bf16), ca, cb)


def halves(a):
    hi = a.astype(bf16)
    return hi, (a - hi.astype(f32)).astype(bf16)


def dot3(a, b, ca=1, cb=0):
    ah, al = halves(a)
    bh, bl = halves(b)
    return dg(ah, bh, ca, cb) + dg(ah, bl, ca, cb) + dg(al, bh, ca, cb)


def iota(shape, dim):
    return lax.broadcasted_iota(jnp.int32, shape, dim)


def softplus(a):
    return jnp.maximum(a, 0.0) + jnp.log(1.0 + jnp.exp(-jnp.abs(a)))


def sigmoid(a):
    return 1.0 / (1.0 + jnp.exp(-a))


def kernel(
    q_hbm, k_hbm, v_hbm, lg_ref, pre_ref, hdl_ref, ex_ref, wo_hbm,
    tok_hbm, sc_ref, ch_ref, grw_ref, eld_ref, wg_hbm, wu_hbm, wd_hbm,
    o1_ref, o2_ref,
    q_ref, k_ref, v_ref, wo_ref, tok_ref,
    gu, dw, obuf, xbuf, ybuf, rbuf, dhop, bhop, h_s,
    a_s, s_s, x_s, ol_s, p_s, m_s, st_own, st_all, att_s,
    mine, theirs, pbuf, rrp, rrm, rsp, rsm,
    sp, rp, sm, rm, ps, pr, dsend, drecv, dhs, dhr, bsend, brecv, bhs, bhr,
    ssend, srecv, xs, qs_p, qr_p, qs_m, qr_m, ins,
):
    ep = lax.axis_index("ep")
    tp = lax.axis_index("tp")
    z, c = tp // 2, tp % 2
    y, x = ep // 4, ep % 4
    up = ((z + 1) % NZ) * 2 + c
    down = ((z + NZ - 1) % NZ) * 2 + c
    mate = tp + 1 - 2 * c

    def peer(i):
        return ((y + i // 4) % 4) * 4 + (x + i % 4) % 4

    def loaded(n):
        pairs = (
            (wg_hbm.at[0], gu.at[z, 0, c]), (wu_hbm.at[0], gu.at[z, 1, c]),
            (tok_hbm, tok_ref), (k_hbm, k_ref), (q_hbm, q_ref), (v_hbm, v_ref), (wo_hbm, wo_ref),
            *((wd_hbm.at[0, :, pl.ds(n * COLS, COLS)], dw.at[n, z, c]) for n in range(CHUNKS)),
        )
        return pltpu.make_async_copy(*pairs[n], ins.at[n])

    for n in (0, 1, 7, 2, 3, 4, 5, 8, 9, 10, 6):
        loaded(n).start()

    barrier = pltpu.get_barrier_semaphore()
    for i in range(1, EP):
        pl.semaphore_signal(barrier, inc=1, device_id={"ep": peer(i)}, device_id_type=MESH)
    for t in (up, down, mate):
        pl.semaphore_signal(barrier, inc=1, device_id={"tp": t}, device_id_type=MESH)
    pl.semaphore_wait(barrier, EP - 1 + 3)

    def remote(src, dst, send, recv, **where):
        return pltpu.make_async_remote_copy(
            src_ref=src, dst_ref=dst, send_sem=send, recv_sem=recv, device_id=where, device_id_type=MESH
        )

    def place(zs, core, piece, rows):
        whole = gu.at[zs, piece, core] if piece < 2 else dw.at[piece - 2, zs, core]
        return whole if rows is None else whole.at[pl.ds(rows, SH // 2)]

    def ring(s, piece, forward):
        slot = (z + NZ - s) % NZ if forward else (z + s) % NZ
        rows = None if s < 3 else (0 if forward else SH // 2)
        here = place(slot, c, piece, rows)
        if forward:
            return remote(here, here, sp.at[s, piece], rp.at[s, piece], tp=up)
        return remote(here, here, sm.at[s, piece], rm.at[s, piece], tp=down)

    def across(n, piece):
        if n == 0:
            slot, rows = z, None
        elif n <= 3:
            slot, rows = (z + NZ - n) % NZ, None
        elif n <= 6:
            slot, rows = (z + n - 3) % NZ, None
        else:
            slot, rows = (z + 4) % NZ, (0 if n == 7 else SH // 2)
        here = place(slot, c, piece, rows)
        return remote(here, here, ps.at[n, piece], pr.at[n, piece], tp=mate)

    def step(piece, s):
        if s == 0:
            across(0, piece).start()
            ring(0, piece, True).start()
            ring(0, piece, False).start()
            return
        ring(s - 1, piece, True).wait_recv()
        ring(s, piece, True).start()
        across(s, piece).start()
        ring(s - 1, piece, False).wait_recv()
        ring(s, piece, False).start()
        across(3 + s, piece).start()

    def finish(piece):
        ring(3, piece, True).wait_recv()
        across(7, piece).start()
        ring(3, piece, False).wait_recv()
        across(8, piece).start()

    for n in (0, 1, 7):
        loaded(n).wait()
    for piece in range(3):
        step(piece, 0)

    loaded(2).wait()
    wide = tok_ref[...].astype(f32)
    normed = (
        wide * lax.rsqrt(jnp.sum(wide * wide, axis=1, keepdims=True) * (1.0 / W) + EPS) * sc_ref[...]
    ).astype(bf16)
    eye = iota((TOK, TOK), 0) == iota((TOK, TOK), 1)
    first = jnp.sum(jnp.where(eye, ch_ref[0:1, :], 0), axis=1, keepdims=True)
    second = jnp.sum(jnp.where(eye, ch_ref[1:2, :], 0), axis=1, keepdims=True)
    lane16 = iota((TOK, EXPERTS), 1)
    is_first, is_second = lane16 == first, lane16 == second
    member = jnp.where(is_first | is_second, 1.0, 0.0)
    before = jnp.where(iota((TOK, TOK), 1) < iota((TOK, TOK), 0), 1.0, 0.0)
    spot = bdot(before, member) + (lane16 * CAP).astype(f32)
    slot1 = jnp.sum(jnp.where(is_first, spot, 0.0), axis=1, keepdims=True).astype(jnp.int32)
    slot2 = jnp.sum(jnp.where(is_second, spot, 0.0), axis=1, keepdims=True).astype(jnp.int32)
    lanes = iota((TOK, SLOTS), 1)
    pick1 = jnp.where(lanes == slot1, 1.0, 0.0).astype(bf16)
    pick2 = jnp.where(lanes == slot2, 1.0, 0.0).astype(bf16)
    obuf[...] = dg(pick1 + pick2, normed, 0, 0).astype(bf16)

    def route(src, dst, hop, send, recv, hsend, hrecv):
        def first_leg(i):
            block = src.at[pl.ds(peer(i) * CAP, CAP)]
            if i in RELAY:
                n = ORDER.index(i)
                return remote(block, hop.at[n], send.at[i], hrecv.at[n], ep=peer(RELAY[i]))
            return remote(block, dst.at[pl.ds(ep * CAP, CAP)], send.at[i], recv.at[i], ep=peer(i))

        def second_leg(i):
            n = ORDER.index(i)
            origin = peer(minus(0, RELAY[i]))
            there = dst.at[pl.ds(origin * CAP, CAP)]
            return remote(hop.at[n], there, hsend.at[n], recv.at[i], ep=peer(minus(i, RELAY[i])))

        def last(i):
            return remote(src.at[pl.ds(0, CAP)], dst.at[pl.ds(0, CAP)], send.at[i], recv.at[i], ep=peer(i))

        def forward(i):
            first_leg(i).wait_recv()
            second_leg(i).start()

        def drain():
            for i in range(1, EP):
                first_leg(i).wait_send()
            for i in ORDER:
                second_leg(i).wait_send()

        return first_leg, forward, last, drain

    d_first, d_forward, d_last, d_drain = route(obuf, xbuf, dhop, dsend, drecv, dhs, dhr)
    back = [
        route(ybuf.at[n], rbuf.at[n], bhop.at[n], bsend.at[n], brecv.at[n], bhs.at[n], bhr.at[n])
        for n in range(CHUNKS)
    ]
    for i in ORDER + DIRECT:
        d_first(i).start()
    home = pl.ds(pl.multiple_of(ep * CAP, CAP), CAP)
    xbuf[home, :] = obuf[home, :]

    for n in (3, 4, 5):
        loaded(n).wait()
    kb, qb = k_ref[...], q_ref[...]
    ld = -jnp.exp(jnp.full((1, 1), hdl_ref[0], f32)) * softplus(pre_ref[...].astype(f32)) + ex_ref[...]
    beta = sigmoid(lg_ref[...].astype(f32))
    kf = kb.astype(f32)
    k2h, k2l = halves(kf * kf)
    ones = jnp.ones((8, DH), bf16)
    rk_row = lax.rsqrt((dg(ones, k2h, 1, 1) + dg(ones, k2l, 1, 1))[0:1] + EPS)
    upper = jnp.where(iota((SEG, SEG), 0) <= iota((SEG, SEG), 1), 1.0, 0.0).astype(bf16)
    ld8 = jnp.broadcast_to(ld, (8, SEG))
    l1, rest = halves(ld8)
    l2 = (ld8 - l1.astype(f32) - rest.astype(f32)).astype(bf16)
    c_row = (dg(l1, upper) + dg(rest, upper) + dg(l2, upper))[0:1]
    last = c_row[:, SEG - 1 : SEG]
    rhs, kds, qds = [], [], []
    for n in range(SEG // DH):
        rows = slice(n * DH, (n + 1) * DH)
        ii = iota((DH, SEG), 0) + n * DH
        jj = iota((DH, SEG), 1)
        c_col = jnp.sum(jnp.where(jj <= ii, ld, 0.0), axis=1, keepdims=True)
        b_col = jnp.sum(jnp.where(jj == ii, beta, 0.0), axis=1, keepdims=True)
        kt = kf[rows]
        qt = qb[rows].astype(f32)
        rk_col = lax.rsqrt(jnp.sum(kt * kt, axis=1, keepdims=True) + EPS)
        rq_col = lax.rsqrt(jnp.sum(qt * qt, axis=1, keepdims=True) + EPS) * DH**-0.5
        decay = jnp.where(ii >= jj, jnp.exp(jnp.minimum(c_col - c_row, 0.0)), 0.0) * rk_row
        a_s[rows, :] = jnp.where(ii > jj, dg(kb[rows], kb, 1, 1) * decay * (b_col * rk_col), 0.0)
        s_s[rows, :] = dg(qb[rows], kb, 1, 1) * decay * rq_col
        kn = kt * rk_col
        ec = jnp.exp(c_col)
        rhs.append(jnp.concatenate([b_col * v_ref[rows, :].astype(f32), (b_col * ec) * kn], axis=1))
        p_s[rows, :] = qt * (rq_col * ec)
        ol_s[rows, :] = kn * jnp.exp(last - c_col)
    for n in range(SEG // DH):
        x_s[n * DH : (n + 1) * DH, :] = rhs[n]

    half = SEG // 2
    i2, j2 = iota((half, half), 0), iota((half, half), 1)

    def same(shift):
        return (i2 >> shift) == (j2 >> shift)

    big = [a_s[0:half, 0:half], a_s[half:, half:]]
    power = [jnp.where(same(4), -b, 0.0) for b in big]
    inv = [jnp.where(i2 == j2, 1.0, 0.0) + p for p in power]
    for _ in range(3):
        power = [dot3(p, p) for p in power]
        inv = [t + dot3(t, p) for t, p in zip(inv, power)]
    for shift in (4, 5, 6, 7):
        off = [jnp.where(same(shift + 1) & ~same(shift), b, 0.0) for b in big]
        mid = [dot3(t, o) for t, o in zip(inv, off)]
        inv = [t - dot3(m, t) for t, m in zip(inv, mid)]
    x1 = dot3(inv[0], x_s[0:half, :])
    x2 = dot3(inv[1], x_s[half:, :] - dot3(a_s[half:, 0:half], x1))
    x_s[0:half, :] = x1
    x_s[half:, :] = x2
    e = dot3(ol_s[...], x_s[...], 0, 0)
    diag = iota((DH, DH), 0) == iota((DH, DH), 1)
    st_own[:, 0:DH] = (jnp.where(diag, jnp.exp(last), 0.0) - e[:, DH:]).astype(bf16)
    st_own[:, DH:] = e[:, :DH].astype(bf16)

    def state(j):
        return remote(st_own, st_all.at[ep], ssend.at[j], srecv.at[ep], ep=j)

    for j in range(1, EP):

        @pl.when(ep < j)
        def _(j=j):
            state(j).start()

    step(0, 1)
    sx = dot3(s_s[...], x_s[...])
    ol_s[...] = sx[:, :DH]
    p_s[...] = p_s[...] - sx[:, DH:]
    for i in ORDER[:4]:
        d_forward(i)
    step(1, 1)
    step(2, 1)
    for n in (8, 9, 10):
        loaded(n).wait()
    step(3, 0)
    for i in ORDER[4:]:
        d_forward(i)
    step(0, 2)
    step(1, 2)
    step(2, 2)
    step(3, 1)

    m_s[...] = jnp.zeros((DH, DH), f32)
    for j in range(EP - 1):

        @pl.when(j < ep)
        def _(j=j):
            remote(st_own, st_all.at[j], ssend.at[0], srecv.at[j], ep=0).wait_recv()
            m_s[...] = bdot(st_all[j, :, 0:DH], m_s[...]) + st_all[j, :, DH:].astype(f32)

    att = (ol_s[...] + bdot(p_s[...], m_s[...])).astype(bf16)
    att_s[...] = att.reshape(NZ, 2, CAP, DH)
    loaded(6).wait()
    theirs[...] = dg(att_s[:, 1 - c].reshape(SEG // 2, DH), wo_ref[...]).astype(bf16).reshape(NZ, CAP, W)
    swap = remote(theirs, pbuf, xs.at[0], xs.at[1], tp=mate)
    swap.start()
    mine[...] = dg(att_s[:, c].reshape(SEG // 2, DH), wo_ref[...]).reshape(NZ, CAP, W)

    def grow(zs):
        return mine[zs] + pbuf[zs].astype(f32)

    def sums(s, forward):
        if forward:
            return remote(rsp.at[s], rrp.at[s], qs_p.at[s], qr_p.at[s], tp=up)
        return remote(rsm.at[s], rrm.at[s], qs_m.at[s], qr_m.at[s], tp=down)

    def hidden(zs):
        both = dg(xbuf[...], gu[zs].reshape(4 * SH, W), 1, 1)
        g, u = both[:, : 2 * SH], both[:, 2 * SH :]
        h_s[:, pl.ds(pl.multiple_of(zs * 2 * SH, 2 * SH), 2 * SH)] = (g * sigmoid(g) * u).astype(bf16)

    def group(s):
        for n in ((0,) if s == 0 else (s, 3 + s)):
            for piece in range(2):
                across(n, piece).wait_recv()
        for zs in (z,) if s == 0 else ((z + NZ - s) % NZ, (z + s) % NZ):
            hidden(zs)

    def results(n):
        for m in range(9):
            across(m, 2 + n).wait_recv()
        ybuf[n] = dg(h_s[...], dw[n].reshape(16 * SH, COLS)).astype(bf16)
        for i in ORDER + DIRECT:
            back[n][0](i).start()
        rbuf[n, home, :] = ybuf[n, home, :]

    def relay(n):
        for i in ORDER:
            back[n][1](i)

    def add(s):
        sums(s - 1, True).wait_recv()
        rsp[s] = (rrp[s - 1].astype(f32) + grow((z + 4 - s) % NZ)).astype(bf16)
        sums(s, True).start()
        if s < 3:
            sums(s - 1, False).wait_recv()
            rsm[s] = (rrm[s - 1].astype(f32) + grow((z + NZ - 3 + s) % NZ)).astype(bf16)
            sums(s, False).start()

    step(0, 3)
    for i in range(1, EP):
        d_last(i).wait_recv()
    group(0)
    group(1)
    step(1, 3)
    step(2, 3)
    group(2)
    step(4, 0)
    step(3, 2)
    step(5, 0)
    swap.wait_recv()
    rsp[0] = grow((z + 4) % NZ).astype(bf16)
    rsm[0] = grow((z + NZ - 3) % NZ).astype(bf16)
    group(3)
    finish(0)
    finish(1)
    finish(2)
    step(4, 1)
    for n in (7, 8):
        for piece in range(2):
            across(n, piece).wait_recv()
    hidden((z + 4) % NZ)
    step(3, 3)
    results(0)
    step(5, 1)
    step(4, 2)
    finish(3)
    step(5, 2)
    results(1)
    step(4, 3)
    relay(0)
    step(5, 3)
    finish(4)
    sums(0, True).start()
    sums(0, False).start()
    results(2)
    relay(1)
    finish(5)
    results(3)
    add(1)
    relay(2)
    add(2)
    relay(3)
    add(3)
    sums(2, False).wait_recv()
    sums(3, True).wait_recv()
    o1_ref[...] = (grow(z) + rrp[3].astype(f32) + rrm[2].astype(f32)).astype(bf16)

    lead = sigmoid(eld_ref[...])
    w1 = jnp.sum(jnp.where(eye, grw_ref[...] * lead, 0.0), axis=1, keepdims=True)
    w2 = jnp.sum(jnp.where(eye, grw_ref[...] * (1.0 - lead), 0.0), axis=1, keepdims=True)
    for n in range(CHUNKS):
        for i in range(1, EP):
            back[n][2](i).wait_recv()
        mixed = w1 * dg(pick1, rbuf[n]) + w2 * dg(pick2, rbuf[n])
        o2_ref[:, n * COLS : (n + 1) * COLS] = mixed.astype(bf16)

    for s in range(4):
        for piece in range(PIECES):
            ring(s, piece, True).wait_send()
            ring(s, piece, False).wait_send()
        sums(s, True).wait_send()
        if s < 3:
            sums(s, False).wait_send()
    for n in range(9):
        for piece in range(PIECES):
            across(n, piece).wait_send()
    d_drain()
    for n in range(CHUNKS):
        back[n][3]()
    swap.wait_send()
    for j in range(1, EP):

        @pl.when(ep < j)
        def _(j=j):
            state(j).wait_send()


def shards(q, k, v, lg, pre, hdl, ex, wo, tok, sc, ch, grw, eld, wg, wu, wd):
    V = pltpu.VMEM
    dma = pltpu.SemaphoreType.DMA
    scratch = [
        V((SEG, DH), bf16), V((SEG, DH), bf16), V((SEG, DH), bf16), V((DH, W), bf16), V((TOK, W), bf16),
        V((NZ, 2, 2, SH, W), bf16), V((CHUNKS, NZ, 2, SH, COLS), bf16),
        V((SLOTS, W), bf16), V((SLOTS, W), bf16), V((CHUNKS, SLOTS, COLS), bf16), V((CHUNKS, SLOTS, COLS), bf16),
        V((7, CAP, W), bf16), V((CHUNKS, 7, CAP, COLS), bf16), V((SLOTS, 16 * SH), bf16),
        V((SEG, SEG), f32), V((SEG, SEG), f32), V((SEG, 2 * DH), f32), V((SEG, DH), f32), V((SEG, DH), f32),
        V((DH, DH), f32), V((DH, 2 * DH), bf16), V((EP, DH, 2 * DH), bf16), V((NZ, 2, CAP, DH), bf16),
        V((NZ, CAP, W), f32), V((NZ, CAP, W), bf16), V((NZ, CAP, W), bf16),
        V((4, CAP, W), bf16), V((3, CAP, W), bf16), V((4, CAP, W), bf16), V((3, CAP, W), bf16),
        dma((4, PIECES)), dma((4, PIECES)), dma((4, PIECES)), dma((4, PIECES)), dma((9, PIECES)), dma((9, PIECES)),
        dma((EP,)), dma((EP,)), dma((7,)), dma((7,)),
        dma((CHUNKS, EP)), dma((CHUNKS, EP)), dma((CHUNKS, 7)), dma((CHUNKS, 7)),
        dma((EP,)), dma((EP,)), dma((2,)), dma((4,)), dma((4,)), dma((3,)), dma((3,)), dma((11,)),
    ]
    vm = pl.BlockSpec(memory_space=pltpu.VMEM)
    hbm = pl.BlockSpec(memory_space=pl.ANY)
    outs = pl.pallas_call(
        kernel,
        name="mixer_and_experts",
        out_shape=(jax.ShapeDtypeStruct((CAP, W), bf16), jax.ShapeDtypeStruct((TOK, W), bf16)),
        in_specs=[hbm, hbm, hbm, vm, vm, pl.BlockSpec(memory_space=pltpu.SMEM), vm, hbm, hbm, vm, vm, vm, vm, hbm, hbm, hbm],
        out_specs=(vm, vm),
        scratch_shapes=scratch,
        compiler_params=pltpu.CompilerParams(
            collective_id=0, has_side_effects=True, vmem_limit_bytes=60 * 1024 * 1024
        ),
    )(
        q, k, v, lg, pre, hdl, ex, wo,
        tok, sc.reshape(1, W), ch.T, grw.reshape(1, TOK), eld.reshape(1, TOK), wg, wu, wd,
    )
    return pl.pallas_call(
        hand_over,
        name="hand_over",
        out_shape=(jax.ShapeDtypeStruct((CAP, W), bf16), jax.ShapeDtypeStruct((TOK, W), bf16)),
        in_specs=[vm, vm],
        out_specs=(vm, vm),
        compiler_params=pltpu.CompilerParams(vmem_limit_bytes=60 * 1024 * 1024),
    )(*outs)


def hand_over(a_ref, b_ref, c_ref, d_ref):
    c_ref[...] = a_ref[...]
    d_ref[...] = b_ref[...]


def solution(mesh):
    both = ("ep", "tp")
    placed = (
        P("ep", "tp"), P("ep", "tp"), P("ep", "tp"),
        P("tp", "ep"), P("tp", "ep"), P("tp"), P("tp", "ep"), P("tp", None),
        P(both, None), P(), P(both, None), P(both), P(both),
        P("ep", "tp", None), P("ep", "tp", None), P("ep", "tp", None),
    )
    return jax.shard_map(
        shards, mesh=mesh, in_specs=placed, out_specs=(P(both, None), P(both, None)), check_vma=False
    )
```

```python
import jax
import jax.numpy as jnp
from jax import lax
from jax.experimental import pallas as pl
from jax.experimental.pallas import tpu as pltpu
from jax.sharding import PartitionSpec as P

f32 = jnp.float32
bf16 = jnp.bfloat16
MESH = pl.DeviceIdType.MESH
EPS = 1e-06
SEG = 512
DH = 128
W = 2048
CAP = 32
EXPERTS = 16
EP = 16
NZ = 8
SH = 64
TOK = 128
CHUNKS = 4
COLS = W // CHUNKS
PIECES = 2 + CHUNKS
SLOTS = EXPERTS * CAP
RELAY = {10: 15, 8: 4, 9: 13, 11: 7, 6: 7, 14: 13, 2: 1}
ORDER = list(RELAY)
DIRECT = [i for i in range(1, 16) if i not in RELAY]


def minus(i, j):
    return ((i // 4 - j // 4) % 4) * 4 + (i % 4 - j % 4) % 4


def dg(a, b, ca=1, cb=0):
    return lax.dot_general(a, b, (((ca,), (cb,)), ((), ())), preferred_element_type=f32)


def bdot(a, b, ca=1, cb=0):
    return dg(a.astype(bf16), b.astype(bf16), ca, cb)


def halves(a):
    hi = a.astype(bf16)
    return hi, (a - hi.astype(f32)).astype(bf16)


def dot3(a, b, ca=1, cb=0):
    ah, al = halves(a)
    bh, bl = halves(b)
    return dg(ah, bh, ca, cb) + dg(ah, bl, ca, cb) + dg(al, bh, ca, cb)


def iota(shape, dim):
    return lax.broadcasted_iota(jnp.int32, shape, dim)


def softplus(a):
    return jnp.maximum(a, 0.0) + jnp.log(1.0 + jnp.exp(-jnp.abs(a)))


def sigmoid(a):
    return 1.0 / (1.0 + jnp.exp(-a))


def kernel(
    q_hbm, k_hbm, v_hbm, lg_hbm, pre_hbm, hdl_hbm, ex_hbm, wo_hbm,
    tok_hbm, sc_hbm, ch_hbm, grw_hbm, eld_hbm, wg_hbm, wu_hbm, wd_hbm,
    o1_ref, o2_ref,
    q_ref, k_ref, v_ref, wo_ref, tok_ref, lg_ref, pre_ref, hdl_ref, ex_ref, sc_ref, ch_ref, grw_ref, eld_ref,
    gu, dw, obuf, xbuf, ybuf, rbuf, dhop, bhop, h_s,
    a_s, s_s, x_s, ol_s, p_s, m_s, st_own, st_all, att_s,
    mine, theirs, pbuf, rrp, rrm, rsp, rsm,
    rs, rr, ps, pr, dsem, dhr, bsem, brecv, bhr,
    ssend, srecv, xs, qs, qr_p, qr_m, ins,
):
    ep = lax.axis_index("ep")
    tp = lax.axis_index("tp")
    z, c = tp // 2, tp % 2
    y, x = ep // 4, ep % 4
    up = ((z + 1) % NZ) * 2 + c
    down = ((z + NZ - 1) % NZ) * 2 + c
    mate = tp + 1 - 2 * c

    def peer(i):
        return ((y + i // 4) % 4) * 4 + (x + i % 4) % 4

    def loaded(n):
        pairs = (
            (wg_hbm.at[0], gu.at[z, 0, c]), (wu_hbm.at[0], gu.at[z, 1, c]),
            (tok_hbm, tok_ref), (k_hbm, k_ref), (q_hbm, q_ref), (v_hbm, v_ref), (wo_hbm, wo_ref),
            (sc_hbm, sc_ref), (ch_hbm, ch_ref), (lg_hbm, lg_ref), (pre_hbm, pre_ref), (hdl_hbm, hdl_ref),
            (ex_hbm, ex_ref), (grw_hbm, grw_ref), (eld_hbm, eld_ref),
            *((wd_hbm.at[0, :, pl.ds(n * COLS, COLS)], dw.at[n, z, c]) for n in range(CHUNKS)),
        )
        return pltpu.make_async_copy(*pairs[n], ins.at[(0, *range(14), 14, 15, 15, 15)[n]])

    for n in (0, 1, 15, 2, 7, 8, 3, 4, 5, 9, 10, 11, 12, 13, 14, 16, 17, 18, 6):
        loaded(n).start()

    barrier = pltpu.get_barrier_semaphore()
    for i in range(1, EP):
        pl.semaphore_signal(barrier, inc=1, device_id={"ep": peer(i)}, device_id_type=MESH)
    for t in (up, down, mate):
        pl.semaphore_signal(barrier, inc=1, device_id={"tp": t}, device_id_type=MESH)
    pl.semaphore_wait(barrier, EP - 1 + 3)

    def remote(src, dst, send, recv, **where):
        return pltpu.make_async_remote_copy(
            src_ref=src, dst_ref=dst, send_sem=send, recv_sem=recv, device_id=where, device_id_type=MESH
        )

    def absorb(like, sem):
        pltpu.make_async_copy(like, like, sem).wait()

    def place(zs, core, piece, rows):
        whole = gu.at[zs, piece, core] if piece < 2 else dw.at[piece - 2, zs, core]
        return whole if rows is None else whole.at[pl.ds(rows, SH // 2)]

    def ring(s, piece, forward):
        slot = (z + NZ - s) % NZ if forward else (z + s) % NZ
        rows = None if s < 3 else (0 if forward else SH // 2)
        here = place(slot, c, piece, rows)
        if forward:
            return remote(here, here, rs.at[min(piece // 2, 1)], rr.at[s, piece], tp=up)
        return remote(here, here, rs.at[min(piece // 2, 1)], rr.at[s, piece], tp=down)

    def arrived(s, piece):
        like = gu.at[0, 0] if piece < 2 else dw.at[0, 0]
        absorb(like if s < 3 else like.at[0], rr.at[s, piece])

    def across(n, piece):
        if n == 0:
            slot, rows = z, None
        elif n <= 3:
            slot, rows = (z + NZ - n) % NZ, None
        elif n <= 6:
            slot, rows = (z + n - 3) % NZ, None
        else:
            slot, rows = (z + 4) % NZ, (0 if n == 7 else SH // 2)
        here = place(slot, c, piece, rows)
        wave = 0 if n == 0 else (n - 1) % 3 + 1 if n < 7 else 4
        return remote(here, here, ps.at[min(piece // 2, 1)], pr.at[wave if piece < 2 else 3 + piece], tp=mate)

    def step(piece, s):
        if s == 0:
            across(0, piece).start()
            ring(0, piece, True).start()
            ring(0, piece, False).start()
            return
        arrived(s - 1, piece)
        ring(s, piece, True).start()
        ring(s, piece, False).start()
        across(s, piece).start()
        across(3 + s, piece).start()

    def finish(piece):
        arrived(3, piece)
        across(7, piece).start()
        across(8, piece).start()

    absorb(gu.at[0, :, 0], ins.at[0])
    loaded(15).wait()
    for piece in range(3):
        step(piece, 0)

    for n in (2, 7, 8):
        loaded(n).wait()
    wide = tok_ref[...].astype(f32)
    normed = (
        wide * lax.rsqrt(jnp.sum(wide * wide, axis=1, keepdims=True) * (1.0 / W) + EPS) * sc_ref[...]
    ).astype(bf16)
    eye = iota((TOK, TOK), 0) == iota((TOK, TOK), 1)
    first = jnp.sum(jnp.where(eye, ch_ref[0:1, :], 0), axis=1, keepdims=True)
    second = jnp.sum(jnp.where(eye, ch_ref[1:2, :], 0), axis=1, keepdims=True)
    lane16 = iota((TOK, EXPERTS), 1)
    is_first, is_second = lane16 == first, lane16 == second
    member = jnp.where(is_first | is_second, 1.0, 0.0)
    before = jnp.where(iota((TOK, TOK), 1) < iota((TOK, TOK), 0), 1.0, 0.0)
    spot = bdot(before, member) + (lane16 * CAP).astype(f32)
    slot1 = jnp.sum(jnp.where(is_first, spot, 0.0), axis=1, keepdims=True).astype(jnp.int32)
    slot2 = jnp.sum(jnp.where(is_second, spot, 0.0), axis=1, keepdims=True).astype(jnp.int32)
    lanes = iota((TOK, SLOTS), 1)
    pick1 = jnp.where(lanes == slot1, 1.0, 0.0).astype(bf16)
    pick2 = jnp.where(lanes == slot2, 1.0, 0.0).astype(bf16)
    obuf[...] = dg(pick1 + pick2, normed, 0, 0).astype(bf16)

    def route(src, dst, hop, send, recv, hsend, hrecv):
        def first_leg(i):
            block = src.at[pl.ds(peer(i) * CAP, CAP)]
            if i in RELAY:
                n = ORDER.index(i)
                return remote(block, hop.at[n], send, hrecv(n), ep=peer(RELAY[i]))
            return remote(block, dst.at[pl.ds(ep * CAP, CAP)], send, recv, ep=peer(i))

        def second_leg(i):
            n = ORDER.index(i)
            origin = peer(minus(0, RELAY[i]))
            there = dst.at[pl.ds(origin * CAP, CAP)]
            return remote(hop.at[n], there, hsend, recv, ep=peer(minus(i, RELAY[i])))

        def forward(lo, hi):
            absorb(hop.at[pl.ds(lo, hi - lo)], hrecv(lo))
            for i in ORDER[lo:hi]:
                second_leg(i).start()

        return first_leg, forward

    others = pl.ds(0, (EP - 1) * CAP)
    d_first, d_forward = route(obuf, xbuf, dhop, dsem.at[0], dsem.at[1], dsem.at[2], lambda n: dhr.at[n // 4])
    back = [
        route(
            ybuf.at[n], rbuf.at[n], bhop.at[n], bsem.at[0], brecv.at[n], bsem.at[1],
            lambda m, n=n: bhr.at[n + (m // 4 if n == CHUNKS - 1 else 0)],
        )
        for n in range(CHUNKS)
    ]
    for i in ORDER + DIRECT:
        d_first(i).start()
    home = pl.ds(pl.multiple_of(ep * CAP, CAP), CAP)
    xbuf[home, :] = obuf[home, :]

    for n in (3, 4, 5, 9, 10, 11, 12):
        loaded(n).wait()
    kb, qb = k_ref[...], q_ref[...]
    ld = -jnp.exp(jnp.full((1, 1), hdl_ref[0], f32)) * softplus(pre_ref[...].astype(f32)) + ex_ref[...]
    beta = sigmoid(lg_ref[...].astype(f32))
    kf = kb.astype(f32)
    k2h, k2l = halves(kf * kf)
    ones = jnp.ones((8, DH), bf16)
    rk_row = lax.rsqrt((dg(ones, k2h, 1, 1) + dg(ones, k2l, 1, 1))[0:1] + EPS)
    upper = jnp.where(iota((SEG, SEG), 0) <= iota((SEG, SEG), 1), 1.0, 0.0).astype(bf16)
    ld8 = jnp.broadcast_to(ld, (8, SEG))
    l1, rest = halves(ld8)
    l2 = (ld8 - l1.astype(f32) - rest.astype(f32)).astype(bf16)
    c_row = (dg(l1, upper) + dg(rest, upper) + dg(l2, upper))[0:1]
    last = c_row[:, SEG - 1 : SEG]
    rhs, kds, qds = [], [], []
    for n in range(SEG // DH):
        rows = slice(n * DH, (n + 1) * DH)
        ii = iota((DH, SEG), 0) + n * DH
        jj = iota((DH, SEG), 1)
        c_col = jnp.sum(jnp.where(jj <= ii, ld, 0.0), axis=1, keepdims=True)
        b_col = jnp.sum(jnp.where(jj == ii, beta, 0.0), axis=1, keepdims=True)
        kt = kf[rows]
        qt = qb[rows].astype(f32)
        rk_col = lax.rsqrt(jnp.sum(kt * kt, axis=1, keepdims=True) + EPS)
        rq_col = lax.rsqrt(jnp.sum(qt * qt, axis=1, keepdims=True) + EPS) * DH**-0.5
        decay = jnp.where(ii >= jj, jnp.exp(jnp.minimum(c_col - c_row, 0.0)), 0.0) * rk_row
        a_s[rows, :] = jnp.where(ii > jj, dg(kb[rows], kb, 1, 1) * decay * (b_col * rk_col), 0.0)
        s_s[rows, :] = dg(qb[rows], kb, 1, 1) * decay * rq_col
        kn = kt * rk_col
        ec = jnp.exp(c_col)
        rhs.append(jnp.concatenate([b_col * v_ref[rows, :].astype(f32), (b_col * ec) * kn], axis=1))
        p_s[rows, :] = qt * (rq_col * ec)
        ol_s[rows, :] = kn * jnp.exp(last - c_col)
    for n in range(SEG // DH):
        x_s[n * DH : (n + 1) * DH, :] = rhs[n]

    half = SEG // 2
    i2, j2 = iota((half, half), 0), iota((half, half), 1)

    def same(shift):
        return (i2 >> shift) == (j2 >> shift)

    big = [a_s[0:half, 0:half], a_s[half:, half:]]
    power = [jnp.where(same(4), -b, 0.0) for b in big]
    inv = [jnp.where(i2 == j2, 1.0, 0.0) + p for p in power]
    for _ in range(3):
        power = [dot3(p, p) for p in power]
        inv = [t + dot3(t, p) for t, p in zip(inv, power)]
    for shift in (4, 5, 6, 7):
        off = [jnp.where(same(shift + 1) & ~same(shift), b, 0.0) for b in big]
        mid = [dot3(t, o) for t, o in zip(inv, off)]
        inv = [t - dot3(m, t) for t, m in zip(inv, mid)]
    x1 = dot3(inv[0], x_s[0:half, :])
    x2 = dot3(inv[1], x_s[half:, :] - dot3(a_s[half:, 0:half], x1))
    x_s[0:half, :] = x1
    x_s[half:, :] = x2
    e = dot3(ol_s[...], x_s[...], 0, 0)
    diag = iota((DH, DH), 0) == iota((DH, DH), 1)
    st_own[:, 0:DH] = (jnp.where(diag, jnp.exp(last), 0.0) - e[:, DH:]).astype(bf16)
    st_own[:, DH:] = e[:, :DH].astype(bf16)

    def state(j):
        return remote(st_own, st_all.at[ep], ssend.at[j], srecv.at[ep], ep=j)

    for j in range(1, EP):

        @pl.when(ep < j)
        def _(j=j):
            state(j).start()

    step(0, 1)
    sx = dot3(s_s[...], x_s[...])
    ol_s[...] = sx[:, :DH]
    p_s[...] = p_s[...] - sx[:, DH:]
    d_forward(0, 4)
    step(1, 1)
    step(2, 1)
    absorb(dw.at[pl.ds(1, 3), 0, 0], ins.at[15])
    step(3, 0)
    d_forward(4, 7)
    step(0, 2)
    step(1, 2)
    step(2, 2)
    step(3, 1)

    m_s[...] = jnp.zeros((DH, DH), f32)
    for j in range(EP - 1):

        @pl.when(j < ep)
        def _(j=j):
            remote(st_own, st_all.at[j], ssend.at[0], srecv.at[j], ep=0).wait_recv()
            m_s[...] = bdot(st_all[j, :, 0:DH], m_s[...]) + st_all[j, :, DH:].astype(f32)

    att = (ol_s[...] + bdot(p_s[...], m_s[...])).astype(bf16)
    att_s[...] = att.reshape(NZ, 2, CAP, DH)
    for n in (6, 13, 14):
        loaded(n).wait()
    theirs[...] = dg(att_s[:, 1 - c].reshape(SEG // 2, DH), wo_ref[...]).astype(bf16).reshape(NZ, CAP, W)
    swap = remote(theirs, pbuf, xs.at[0], xs.at[1], tp=mate)
    swap.start()
    mine[...] = dg(att_s[:, c].reshape(SEG // 2, DH), wo_ref[...]).reshape(NZ, CAP, W)

    def grow(zs, k):
        cols = slice(k * W // 2, (k + 1) * W // 2)
        return mine[zs, :, cols] + pbuf[zs, :, cols].astype(f32)

    def sums(s, k, forward):
        if forward:
            return remote(rsp.at[s, k], rrp.at[s, k], qs.at[0], qr_p.at[s, k], tp=up)
        return remote(rsm.at[s, k], rrm.at[s, k], qs.at[1], qr_m.at[s, k], tp=down)

    def hidden(zs):
        both = dg(xbuf[...], gu[zs].reshape(4 * SH, W), 1, 1)
        g, u = both[:, : 2 * SH], both[:, 2 * SH :]
        h_s[:, pl.ds(pl.multiple_of(zs * 2 * SH, 2 * SH), 2 * SH)] = (g * sigmoid(g) * u).astype(bf16)

    def crossed(s):
        absorb(gu.at[0] if 0 < s < 4 else gu.at[0, 0], pr.at[s])

    def group(s):
        for zs in {0: (z,), 4: ((z + 4) % NZ,)}.get(s, ((z + NZ - s) % NZ, (z + s) % NZ)):
            hidden(zs)

    def results(n):
        absorb(dw.at[n, :, 0], pr.at[5 + n])
        ybuf[n] = dg(h_s[...], dw[n].reshape(16 * SH, COLS)).astype(bf16)
        rbuf[n, home, :] = ybuf[n, home, :]

    def send(n, messages):
        for i in messages:
            back[n][0](i).start()

    def relay(n):
        if n < CHUNKS - 1:
            back[n][1](0, 7)
        else:
            back[n][1](0, 4)
            back[n][1](4, 7)

    def begin(k):
        sums(0, k, True).start()
        sums(0, k, False).start()

    def add(s, k):
        sums(s - 1, k, True).wait_recv()
        rsp[s, k] = (rrp[s - 1, k].astype(f32) + grow((z + 4 - s) % NZ, k)).astype(bf16)
        sums(s, k, True).start()
        if s < 3:
            sums(s - 1, k, False).wait_recv()
            rsm[s, k] = (rrm[s - 1, k].astype(f32) + grow((z + NZ - 3 + s) % NZ, k)).astype(bf16)
            sums(s, k, False).start()

    def total(k):
        sums(2, k, False).wait_recv()
        sums(3, k, True).wait_recv()
        o1_ref[:, k * W // 2 : (k + 1) * W // 2] = (
            grow(z, k) + rrp[3, k].astype(f32) + rrm[2, k].astype(f32)
        ).astype(bf16)

    lead = sigmoid(eld_ref[...])
    w1 = jnp.sum(jnp.where(eye, grw_ref[...] * lead, 0.0), axis=1, keepdims=True)
    w2 = jnp.sum(jnp.where(eye, grw_ref[...] * (1.0 - lead), 0.0), axis=1, keepdims=True)

    def mix(n):
        absorb(rbuf.at[n, others], brecv.at[n])
        mixed = w1 * dg(pick1, rbuf[n]) + w2 * dg(pick2, rbuf[n])
        o2_ref[:, n * COLS : (n + 1) * COLS] = mixed.astype(bf16)

    step(0, 3)
    absorb(xbuf.at[others], dsem.at[1])
    crossed(0)
    group(0)
    crossed(1)
    group(1)
    step(1, 3)
    step(2, 3)
    step(4, 0)
    crossed(2)
    group(2)
    step(3, 2)
    step(5, 0)
    swap.wait_recv()
    for k in range(2):
        rsp[0, k] = grow((z + 4) % NZ, k).astype(bf16)
        rsm[0, k] = grow((z + NZ - 3) % NZ, k).astype(bf16)
    crossed(3)
    group(3)
    finish(0)
    finish(1)
    finish(2)
    crossed(4)
    step(4, 1)
    group(4)
    results(0)
    send(0, ORDER + DIRECT)
    step(3, 3)
    step(5, 1)
    step(4, 2)
    begin(0)
    finish(3)
    step(5, 2)
    results(1)
    send(1, ORDER + DIRECT)
    step(4, 3)
    begin(1)
    relay(0)
    step(5, 3)
    add(1, 0)
    finish(4)
    results(2)
    send(2, ORDER)
    add(1, 1)
    relay(1)
    finish(5)
    results(3)
    send(3, ORDER)
    send(2, DIRECT)
    send(3, DIRECT)
    add(2, 0)
    add(2, 1)
    mix(0)
    relay(2)
    add(3, 0)
    relay(3)
    add(3, 1)
    mix(1)
    total(0)
    total(1)
    mix(2)
    mix(3)

    absorb(gu.at[pl.ds(0, 7), :, 0], rs.at[0])
    absorb(dw.at[:, pl.ds(0, 7), 0], rs.at[1])
    absorb(gu.at[:, :, 0], ps.at[0])
    absorb(dw.at[:, :, 0], ps.at[1])
    absorb(obuf.at[others], dsem.at[0])
    absorb(dhop, dsem.at[2])
    absorb(ybuf.at[:, others], bsem.at[0])
    absorb(bhop, bsem.at[1])
    absorb(rsp, qs.at[0])
    absorb(rsm, qs.at[1])
    swap.wait_send()
    for j in range(1, EP):

        @pl.when(ep < j)
        def _(j=j):
            state(j).wait_send()


def shards(q, k, v, lg, pre, hdl, ex, wo, tok, sc, ch, grw, eld, wg, wu, wd):
    V = pltpu.VMEM
    dma = pltpu.SemaphoreType.DMA
    scratch = [
        V((SEG, DH), bf16), V((SEG, DH), bf16), V((SEG, DH), bf16), V((DH, W), bf16), V((TOK, W), bf16),
        V((1, SEG), bf16), V((1, SEG), bf16), pltpu.SMEM((1,), f32), V((1, SEG), f32),
        V((1, W), f32), V((2, TOK), jnp.int32), V((1, TOK), f32), V((1, TOK), f32),
        V((NZ, 2, 2, SH, W), bf16), V((CHUNKS, NZ, 2, SH, COLS), bf16),
        V((SLOTS, W), bf16), V((SLOTS, W), bf16), V((CHUNKS, SLOTS, COLS), bf16), V((CHUNKS, SLOTS, COLS), bf16),
        V((7, CAP, W), bf16), V((CHUNKS, 7, CAP, COLS), bf16), V((SLOTS, 16 * SH), bf16),
        V((SEG, SEG), f32), V((SEG, SEG), f32), V((SEG, 2 * DH), f32), V((SEG, DH), f32), V((SEG, DH), f32),
        V((DH, DH), f32), V((DH, 2 * DH), bf16), V((EP, DH, 2 * DH), bf16), V((NZ, 2, CAP, DH), bf16),
        V((NZ, CAP, W), f32), V((NZ, CAP, W), bf16), V((NZ, CAP, W), bf16),
        V((4, 2, CAP, W // 2), bf16), V((3, 2, CAP, W // 2), bf16),
        V((4, 2, CAP, W // 2), bf16), V((3, 2, CAP, W // 2), bf16),
        dma((2,)), dma((4, PIECES)), dma((2,)), dma((5 + CHUNKS,)),
        dma((3,)), dma((2,)), dma((2,)), dma((CHUNKS,)), dma((CHUNKS + 1,)),
        dma((EP,)), dma((EP,)), dma((2,)), dma((2,)), dma((4, 2)), dma((3, 2)), dma((16,)),
    ]
    vm = pl.BlockSpec(memory_space=pltpu.VMEM)
    hbm = pl.BlockSpec(memory_space=pl.ANY)
    outs = pl.pallas_call(
        kernel,
        name="mixer_and_experts",
        out_shape=(V((CAP, W), bf16), V((TOK, W), bf16)),
        in_specs=[hbm] * 16,
        out_specs=(vm, vm),
        scratch_shapes=scratch,
        compiler_params=pltpu.CompilerParams(
            collective_id=0, has_side_effects=True, vmem_limit_bytes=60 * 1024 * 1024
        ),
    )(
        q, k, v, lg, pre, hdl, ex, wo,
        tok, sc.reshape(1, W), ch.T, grw.reshape(1, TOK), eld.reshape(1, TOK), wg, wu, wd,
    )
    return pl.pallas_call(
        hand_over,
        name="hand_over",
        out_shape=(jax.ShapeDtypeStruct((CAP, W), bf16), jax.ShapeDtypeStruct((TOK, W), bf16)),
        in_specs=[vm, vm],
        out_specs=(vm, vm),
        compiler_params=pltpu.CompilerParams(vmem_limit_bytes=4 * 1024 * 1024),
    )(*outs)


def hand_over(a_ref, b_ref, c_ref, d_ref):
    c_ref[...] = a_ref[...]
    d_ref[...] = b_ref[...]


def solution(mesh):
    both = ("ep", "tp")
    placed = (
        P("ep", "tp"), P("ep", "tp"), P("ep", "tp"),
        P("tp", "ep"), P("tp", "ep"), P("tp"), P("tp", "ep"), P("tp", None),
        P(both, None), P(), P(both, None), P(both), P(both),
        P("ep", "tp", None), P("ep", "tp", None), P("ep", "tp", None),
    )
    return jax.shard_map(
        shards, mesh=mesh, in_specs=placed, out_specs=(P(both, None), P(both, None)), check_vma=False
    )
```

```python
import jax
import jax.numpy as jnp
from jax import lax
from jax.experimental import pallas as pl
from jax.experimental.pallas import tpu as pltpu
from jax.sharding import PartitionSpec as P

f32 = jnp.float32
bf16 = jnp.bfloat16
MESH = pl.DeviceIdType.MESH
EPS = 1e-06
SEG = 512
DH = 128
W = 2048
CAP = 32
EXPERTS = 16
EP = 16
NZ = 8
SH = 64
TOK = 128
CHUNKS = 4
COLS = W // CHUNKS
PIECES = 2 + CHUNKS
SLOTS = EXPERTS * CAP
ROWS = (slice(0, SLOTS // 2), slice(SLOTS // 2, SLOTS))
RELAY = {10: 15, 8: 4, 9: 13, 11: 7, 6: 7, 14: 13, 2: 1}
ORDER = list(RELAY)
DIRECT = [i for i in range(1, 16) if i not in RELAY]


def minus(i, j):
    return ((i // 4 - j // 4) % 4) * 4 + (i % 4 - j % 4) % 4


def dg(a, b, ca=1, cb=0):
    return lax.dot_general(a, b, (((ca,), (cb,)), ((), ())), preferred_element_type=f32)


def bdot(a, b, ca=1, cb=0):
    return dg(a.astype(bf16), b.astype(bf16), ca, cb)


def halves(a):
    hi = a.astype(bf16)
    return hi, (a - hi.astype(f32)).astype(bf16)


def dot3(a, b, ca=1, cb=0):
    ah, al = halves(a)
    bh, bl = halves(b)
    return dg(ah, bh, ca, cb) + dg(ah, bl, ca, cb) + dg(al, bh, ca, cb)


def iota(shape, dim):
    return lax.broadcasted_iota(jnp.int32, shape, dim)


def softplus(a):
    return jnp.maximum(a, 0.0) + jnp.log(1.0 + jnp.exp(-jnp.abs(a)))


def sigmoid(a):
    return 1.0 / (1.0 + jnp.exp(-a))


def kernel(
    q_hbm, k_hbm, v_hbm, lg_hbm, pre_hbm, hdl_hbm, ex_hbm, wo_hbm,
    tok_hbm, sc_hbm, ch_hbm, grw_hbm, eld_hbm, wg_hbm, wu_hbm, wd_hbm,
    o1_ref, o2_ref,
    q_ref, k_ref, v_ref, wo_ref, tok_ref, lg_ref, pre_ref, hdl_ref, ex_ref, sc_ref, ch_ref, grw_ref, eld_ref,
    gu, dw, obuf, xbuf, ybuf, rbuf, dhop, bhop, h_s,
    a_s, s_s, x_s, ol_s, p_s, m_s, st_own, st_all, att_s,
    mine, theirs, pbuf, rrp, rrm, rsp, rsm,
    rs, rr, ps, pr, dsem, dhr, bsem, brecv, bhr,
    ssend, srecv, xs, qs, qr_p, qr_m, ins,
):
    ep = lax.axis_index("ep")
    tp = lax.axis_index("tp")
    z, c = tp // 2, tp % 2
    y, x = ep // 4, ep % 4
    up = ((z + 1) % NZ) * 2 + c
    down = ((z + NZ - 1) % NZ) * 2 + c
    mate = tp + 1 - 2 * c

    def peer(i):
        return ((y + i // 4) % 4) * 4 + (x + i % 4) % 4

    def loaded(n):
        pairs = (
            (wg_hbm.at[0], gu.at[z, 0, c]), (wu_hbm.at[0], gu.at[z, 1, c]),
            (tok_hbm, tok_ref), (k_hbm, k_ref), (q_hbm, q_ref), (v_hbm, v_ref), (wo_hbm, wo_ref),
            (sc_hbm, sc_ref), (ch_hbm, ch_ref), (lg_hbm, lg_ref), (pre_hbm, pre_ref), (hdl_hbm, hdl_ref),
            (ex_hbm, ex_ref), (grw_hbm, grw_ref), (eld_hbm, eld_ref),
            *((wd_hbm.at[0, :, pl.ds(n * COLS, COLS)], dw.at[n, z, c]) for n in range(CHUNKS)),
        )
        return pltpu.make_async_copy(*pairs[n], ins.at[(0, *range(14), 14, 15, 15, 15)[n]])

    for n in (0, 1, 15, 2, 7, 8, 3, 4, 5, 9, 10, 11, 12, 13, 14, 16, 17, 18, 6):
        loaded(n).start()

    barrier = pltpu.get_barrier_semaphore()
    for i in range(1, EP):
        pl.semaphore_signal(barrier, inc=1, device_id={"ep": peer(i)}, device_id_type=MESH)
    for t in (up, down, mate):
        pl.semaphore_signal(barrier, inc=1, device_id={"tp": t}, device_id_type=MESH)
    pl.semaphore_wait(barrier, EP - 1 + 3)

    def remote(src, dst, send, recv, **where):
        return pltpu.make_async_remote_copy(
            src_ref=src, dst_ref=dst, send_sem=send, recv_sem=recv, device_id=where, device_id_type=MESH
        )

    def absorb(like, sem):
        pltpu.make_async_copy(like, like, sem).wait()

    def place(zs, core, piece, rows):
        whole = gu.at[zs, piece, core] if piece < 2 else dw.at[piece - 2, zs, core]
        return whole if rows is None else whole.at[pl.ds(rows, SH // 2)]

    def ring(s, piece, forward):
        slot = (z + NZ - s) % NZ if forward else (z + s) % NZ
        rows = None if s < 3 else (0 if forward else SH // 2)
        here = place(slot, c, piece, rows)
        if forward:
            return remote(here, here, rs.at[min(piece // 2, 1)], rr.at[s, piece], tp=up)
        return remote(here, here, rs.at[min(piece // 2, 1)], rr.at[s, piece], tp=down)

    def arrived(s, piece):
        like = gu.at[0, 0] if piece < 2 else dw.at[0, 0]
        absorb(like if s < 3 else like.at[0], rr.at[s, piece])

    def across(n, piece):
        if n == 0:
            slot, rows = z, None
        elif n <= 3:
            slot, rows = (z + NZ - n) % NZ, None
        elif n <= 6:
            slot, rows = (z + n - 3) % NZ, None
        else:
            slot, rows = (z + 4) % NZ, (0 if n == 7 else SH // 2)
        here = place(slot, c, piece, rows)
        wave = 0 if n == 0 else (n - 1) % 3 + 1 if n < 7 else 4
        return remote(here, here, ps.at[min(piece // 2, 1)], pr.at[wave if piece < 2 else 3 + piece], tp=mate)

    def step(piece, s):
        if s == 0:
            across(0, piece).start()
            ring(0, piece, True).start()
            ring(0, piece, False).start()
            return
        arrived(s - 1, piece)
        ring(s, piece, True).start()
        ring(s, piece, False).start()
        across(s, piece).start()
        across(3 + s, piece).start()

    def finish(piece):
        arrived(3, piece)
        across(7, piece).start()
        across(8, piece).start()

    absorb(gu.at[0, :, 0], ins.at[0])
    loaded(15).wait()
    for piece in range(3):
        step(piece, 0)

    for n in (2, 7, 8):
        loaded(n).wait()
    wide = tok_ref[...].astype(f32)
    normed = (
        wide * lax.rsqrt(jnp.sum(wide * wide, axis=1, keepdims=True) * (1.0 / W) + EPS) * sc_ref[...]
    ).astype(bf16)
    eye = iota((TOK, TOK), 0) == iota((TOK, TOK), 1)
    first = jnp.sum(jnp.where(eye, ch_ref[0:1, :], 0), axis=1, keepdims=True)
    second = jnp.sum(jnp.where(eye, ch_ref[1:2, :], 0), axis=1, keepdims=True)
    lane16 = iota((TOK, EXPERTS), 1)
    is_first, is_second = lane16 == first, lane16 == second
    member = jnp.where(is_first | is_second, 1.0, 0.0)
    before = jnp.where(iota((TOK, TOK), 1) < iota((TOK, TOK), 0), 1.0, 0.0)
    spot = bdot(before, member) + (lane16 * CAP).astype(f32)
    slot1 = jnp.sum(jnp.where(is_first, spot, 0.0), axis=1, keepdims=True).astype(jnp.int32)
    slot2 = jnp.sum(jnp.where(is_second, spot, 0.0), axis=1, keepdims=True).astype(jnp.int32)
    lanes = iota((TOK, SLOTS), 1)
    pick1 = jnp.where(lanes == slot1, 1.0, 0.0).astype(bf16)
    pick2 = jnp.where(lanes == slot2, 1.0, 0.0).astype(bf16)
    obuf[...] = dg(pick1 + pick2, normed, 0, 0).astype(bf16)

    def route(src, dst, hop, send, recv, hsend, hrecv):
        def first_leg(i):
            block = src.at[pl.ds(peer(i) * CAP, CAP)]
            if i in RELAY:
                n = ORDER.index(i)
                return remote(block, hop.at[n], send, hrecv(n), ep=peer(RELAY[i]))
            return remote(block, dst.at[pl.ds(ep * CAP, CAP)], send, recv, ep=peer(i))

        def second_leg(i):
            n = ORDER.index(i)
            origin = peer(minus(0, RELAY[i]))
            there = dst.at[pl.ds(origin * CAP, CAP)]
            return remote(hop.at[n], there, hsend, recv, ep=peer(minus(i, RELAY[i])))

        def forward(lo, hi):
            absorb(hop.at[pl.ds(lo, hi - lo)], hrecv(lo))
            for i in ORDER[lo:hi]:
                second_leg(i).start()

        return first_leg, forward

    others = pl.ds(0, (EP - 1) * CAP)
    d_first, d_forward = route(obuf, xbuf, dhop, dsem.at[0], dsem.at[1], dsem.at[2], lambda n: dhr.at[n // 4])
    back = [
        route(
            ybuf.at[n], rbuf.at[n], bhop.at[n], bsem.at[0], brecv.at[n], bsem.at[1],
            lambda m, n=n: bhr.at[n + (m // 4 if n == CHUNKS - 1 else 0)],
        )
        for n in range(CHUNKS)
    ]
    for i in ORDER + DIRECT:
        d_first(i).start()
    home = pl.ds(pl.multiple_of(ep * CAP, CAP), CAP)
    xbuf[home, :] = obuf[home, :]

    for n in (3, 4, 5, 9, 10, 11, 12):
        loaded(n).wait()
    kb, qb = k_ref[...], q_ref[...]
    ld = -jnp.exp(jnp.full((1, 1), hdl_ref[0], f32)) * softplus(pre_ref[...].astype(f32)) + ex_ref[...]
    beta = sigmoid(lg_ref[...].astype(f32))
    kf = kb.astype(f32)
    k2h, k2l = halves(kf * kf)
    ones = jnp.ones((8, DH), bf16)
    rk_row = lax.rsqrt((dg(ones, k2h, 1, 1) + dg(ones, k2l, 1, 1))[0:1] + EPS)
    upper = jnp.where(iota((SEG, SEG), 0) <= iota((SEG, SEG), 1), 1.0, 0.0).astype(bf16)
    ld8 = jnp.broadcast_to(ld, (8, SEG))
    l1, rest = halves(ld8)
    l2 = (ld8 - l1.astype(f32) - rest.astype(f32)).astype(bf16)
    c_row = (dg(l1, upper) + dg(rest, upper) + dg(l2, upper))[0:1]
    last = c_row[:, SEG - 1 : SEG]
    rhs, kds, qds = [], [], []
    for n in range(SEG // DH):
        rows = slice(n * DH, (n + 1) * DH)
        ii = iota((DH, SEG), 0) + n * DH
        jj = iota((DH, SEG), 1)
        c_col = jnp.sum(jnp.where(jj <= ii, ld, 0.0), axis=1, keepdims=True)
        b_col = jnp.sum(jnp.where(jj == ii, beta, 0.0), axis=1, keepdims=True)
        kt = kf[rows]
        qt = qb[rows].astype(f32)
        rk_col = lax.rsqrt(jnp.sum(kt * kt, axis=1, keepdims=True) + EPS)
        rq_col = lax.rsqrt(jnp.sum(qt * qt, axis=1, keepdims=True) + EPS) * DH**-0.5
        decay = jnp.where(ii >= jj, jnp.exp(jnp.minimum(c_col - c_row, 0.0)), 0.0) * rk_row
        a_s[rows, :] = jnp.where(ii > jj, dg(kb[rows], kb, 1, 1) * decay * (b_col * rk_col), 0.0)
        s_s[rows, :] = dg(qb[rows], kb, 1, 1) * decay * rq_col
        kn = kt * rk_col
        ec = jnp.exp(c_col)
        rhs.append(jnp.concatenate([b_col * v_ref[rows, :].astype(f32), (b_col * ec) * kn], axis=1))
        p_s[rows, :] = qt * (rq_col * ec)
        ol_s[rows, :] = kn * jnp.exp(last - c_col)
    for n in range(SEG // DH):
        x_s[n * DH : (n + 1) * DH, :] = rhs[n]

    half = SEG // 2
    i2, j2 = iota((half, half), 0), iota((half, half), 1)

    def same(shift):
        return (i2 >> shift) == (j2 >> shift)

    big = [a_s[0:half, 0:half], a_s[half:, half:]]
    power = [jnp.where(same(4), -b, 0.0) for b in big]
    inv = [jnp.where(i2 == j2, 1.0, 0.0) + p for p in power]
    for _ in range(3):
        power = [dot3(p, p) for p in power]
        inv = [t + dot3(t, p) for t, p in zip(inv, power)]
    for shift in (4, 5, 6, 7):
        off = [jnp.where(same(shift + 1) & ~same(shift), b, 0.0) for b in big]
        mid = [dot3(t, o) for t, o in zip(inv, off)]
        inv = [t - dot3(m, t) for t, m in zip(inv, mid)]
    x1 = dot3(inv[0], x_s[0:half, :])
    x2 = dot3(inv[1], x_s[half:, :] - dot3(a_s[half:, 0:half], x1))
    x_s[0:half, :] = x1
    x_s[half:, :] = x2
    e = dot3(ol_s[...], x_s[...], 0, 0)
    diag = iota((DH, DH), 0) == iota((DH, DH), 1)
    st_own[:, 0:DH] = (jnp.where(diag, jnp.exp(last), 0.0) - e[:, DH:]).astype(bf16)
    st_own[:, DH:] = e[:, :DH].astype(bf16)

    def state(j):
        return remote(st_own, st_all.at[ep], ssend.at[j], srecv.at[ep], ep=j)

    for j in range(1, EP):

        @pl.when(ep < j)
        def _(j=j):
            state(j).start()

    step(0, 1)
    sx = dot3(s_s[...], x_s[...])
    ol_s[...] = sx[:, :DH]
    p_s[...] = p_s[...] - sx[:, DH:]
    d_forward(0, 4)
    step(1, 1)
    step(2, 1)
    absorb(dw.at[pl.ds(1, 3), 0, 0], ins.at[15])
    step(3, 0)
    d_forward(4, 7)
    step(0, 2)
    step(1, 2)
    step(2, 2)
    step(3, 1)

    m_s[...] = jnp.zeros((DH, DH), f32)
    for j in range(EP - 1):

        @pl.when(j < ep)
        def _(j=j):
            remote(st_own, st_all.at[j], ssend.at[0], srecv.at[j], ep=0).wait_recv()
            m_s[...] = bdot(st_all[j, :, 0:DH], m_s[...]) + st_all[j, :, DH:].astype(f32)

    att = (ol_s[...] + bdot(p_s[...], m_s[...])).astype(bf16)
    att_s[...] = att.reshape(NZ, 2, CAP, DH)
    for n in (6, 13, 14):
        loaded(n).wait()
    theirs[...] = dg(att_s[:, 1 - c].reshape(SEG // 2, DH), wo_ref[...]).astype(bf16).reshape(NZ, CAP, W)
    swap = remote(theirs, pbuf, xs.at[0], xs.at[1], tp=mate)
    swap.start()
    mine[...] = dg(att_s[:, c].reshape(SEG // 2, DH), wo_ref[...]).reshape(NZ, CAP, W)

    def grow(zs, k):
        cols = slice(k * W // 2, (k + 1) * W // 2)
        return mine[zs, :, cols] + pbuf[zs, :, cols].astype(f32)

    def sums(s, k, forward):
        if forward:
            return remote(rsp.at[s, k], rrp.at[s, k], qs.at[0], qr_p.at[s, k], tp=up)
        return remote(rsm.at[s, k], rrm.at[s, k], qs.at[1], qr_m.at[s, k], tp=down)

    def hidden(zs):
        weights = gu[zs].reshape(4 * SH, W)
        both = [dg(xbuf[rows, :], weights, 1, 1) for rows in ROWS]
        for rows, b in zip(ROWS, both):
            g, u = b[:, : 2 * SH], b[:, 2 * SH :]
            h_s[rows, pl.ds(pl.multiple_of(zs * 2 * SH, 2 * SH), 2 * SH)] = (g * sigmoid(g) * u).astype(bf16)

    def crossed(s):
        absorb(gu.at[0] if 0 < s < 4 else gu.at[0, 0], pr.at[s])

    def group(s):
        for zs in {0: (z,), 4: ((z + 4) % NZ,)}.get(s, ((z + NZ - s) % NZ, (z + s) % NZ)):
            hidden(zs)

    def results(n):
        absorb(dw.at[n, :, 0], pr.at[5 + n])
        ybuf[n] = dg(h_s[...], dw[n].reshape(16 * SH, COLS)).astype(bf16)
        rbuf[n, home, :] = ybuf[n, home, :]

    def send(n, messages):
        for i in messages:
            back[n][0](i).start()

    def relay(n):
        if n < CHUNKS - 1:
            back[n][1](0, 7)
        else:
            back[n][1](0, 4)
            back[n][1](4, 7)

    def begin(k):
        sums(0, k, True).start()
        sums(0, k, False).start()

    def add(s, k):
        sums(s - 1, k, True).wait_recv()
        rsp[s, k] = (rrp[s - 1, k].astype(f32) + grow((z + 4 - s) % NZ, k)).astype(bf16)
        sums(s, k, True).start()
        if s < 3:
            sums(s - 1, k, False).wait_recv()
            rsm[s, k] = (rrm[s - 1, k].astype(f32) + grow((z + NZ - 3 + s) % NZ, k)).astype(bf16)
            sums(s, k, False).start()

    def total(k):
        sums(2, k, False).wait_recv()
        sums(3, k, True).wait_recv()
        o1_ref[:, k * W // 2 : (k + 1) * W // 2] = (
            grow(z, k) + rrp[3, k].astype(f32) + rrm[2, k].astype(f32)
        ).astype(bf16)

    lead = sigmoid(eld_ref[...])
    w1 = jnp.sum(jnp.where(eye, grw_ref[...] * lead, 0.0), axis=1, keepdims=True)
    w2 = jnp.sum(jnp.where(eye, grw_ref[...] * (1.0 - lead), 0.0), axis=1, keepdims=True)

    def mix(n):
        absorb(rbuf.at[n, others], brecv.at[n])
        mixed = w1 * dg(pick1, rbuf[n]) + w2 * dg(pick2, rbuf[n])
        o2_ref[:, n * COLS : (n + 1) * COLS] = mixed.astype(bf16)

    step(0, 3)
    absorb(xbuf.at[others], dsem.at[1])
    crossed(0)
    group(0)
    crossed(1)
    group(1)
    step(1, 3)
    step(2, 3)
    step(4, 0)
    crossed(2)
    group(2)
    step(3, 2)
    step(5, 0)
    swap.wait_recv()
    for k in range(2):
        rsp[0, k] = grow((z + 4) % NZ, k).astype(bf16)
        rsm[0, k] = grow((z + NZ - 3) % NZ, k).astype(bf16)
    crossed(3)
    group(3)
    finish(0)
    finish(1)
    finish(2)
    @pl.when(c == 0)
    def _():
        crossed(4)
        group(4)
        results(0)
        send(0, ORDER + DIRECT)
        step(4, 1)

    @pl.when(c == 1)
    def _():
        step(4, 1)
        crossed(4)
        group(4)
        results(0)
        send(0, ORDER + DIRECT)

    step(3, 3)
    step(5, 1)
    step(4, 2)
    begin(0)
    finish(3)
    step(5, 2)
    results(1)
    send(1, ORDER + DIRECT)
    step(4, 3)
    begin(1)
    relay(0)
    step(5, 3)
    add(1, 0)
    finish(4)
    results(2)
    send(2, ORDER)
    relay(1)
    send(2, DIRECT)
    add(1, 1)
    finish(5)
    results(3)
    send(3, ORDER)
    add(2, 0)
    relay(2)
    send(3, DIRECT)
    add(2, 1)
    mix(0)
    mix(1)
    add(3, 0)
    relay(3)
    add(3, 1)
    mix(2)
    total(0)
    total(1)
    mix(3)

    absorb(gu.at[pl.ds(0, 7), :, 0], rs.at[0])
    absorb(dw.at[:, pl.ds(0, 7), 0], rs.at[1])
    absorb(gu.at[:, :, 0], ps.at[0])
    absorb(dw.at[:, :, 0], ps.at[1])
    absorb(obuf.at[others], dsem.at[0])
    absorb(dhop, dsem.at[2])
    absorb(ybuf.at[:, others], bsem.at[0])
    absorb(bhop, bsem.at[1])
    absorb(rsp, qs.at[0])
    absorb(rsm, qs.at[1])
    swap.wait_send()
    for j in range(1, EP):

        @pl.when(ep < j)
        def _(j=j):
            state(j).wait_send()


def shards(q, k, v, lg, pre, hdl, ex, wo, tok, sc, ch, grw, eld, wg, wu, wd):
    V = pltpu.VMEM
    dma = pltpu.SemaphoreType.DMA
    scratch = [
        V((SEG, DH), bf16), V((SEG, DH), bf16), V((SEG, DH), bf16), V((DH, W), bf16), V((TOK, W), bf16),
        V((1, SEG), bf16), V((1, SEG), bf16), pltpu.SMEM((1,), f32), V((1, SEG), f32),
        V((1, W), f32), V((2, TOK), jnp.int32), V((1, TOK), f32), V((1, TOK), f32),
        V((NZ, 2, 2, SH, W), bf16), V((CHUNKS, NZ, 2, SH, COLS), bf16),
        V((SLOTS, W), bf16), V((SLOTS, W), bf16), V((CHUNKS, SLOTS, COLS), bf16), V((CHUNKS, SLOTS, COLS), bf16),
        V((7, CAP, W), bf16), V((CHUNKS, 7, CAP, COLS), bf16), V((SLOTS, 16 * SH), bf16),
        V((SEG, SEG), f32), V((SEG, SEG), f32), V((SEG, 2 * DH), f32), V((SEG, DH), f32), V((SEG, DH), f32),
        V((DH, DH), f32), V((DH, 2 * DH), bf16), V((EP, DH, 2 * DH), bf16), V((NZ, 2, CAP, DH), bf16),
        V((NZ, CAP, W), f32), V((NZ, CAP, W), bf16), V((NZ, CAP, W), bf16),
        V((4, 2, CAP, W // 2), bf16), V((3, 2, CAP, W // 2), bf16),
        V((4, 2, CAP, W // 2), bf16), V((3, 2, CAP, W // 2), bf16),
        dma((2,)), dma((4, PIECES)), dma((2,)), dma((5 + CHUNKS,)),
        dma((3,)), dma((2,)), dma((2,)), dma((CHUNKS,)), dma((CHUNKS + 1,)),
        dma((EP,)), dma((EP,)), dma((2,)), dma((2,)), dma((4, 2)), dma((3, 2)), dma((16,)),
    ]
    vm = pl.BlockSpec(memory_space=pltpu.VMEM)
    hbm = pl.BlockSpec(memory_space=pl.ANY)
    outs = pl.pallas_call(
        kernel,
        name="mixer_and_experts",
        out_shape=(V((CAP, W), bf16), V((TOK, W), bf16)),
        in_specs=[hbm] * 16,
        out_specs=(vm, vm),
        scratch_shapes=scratch,
        compiler_params=pltpu.CompilerParams(
            collective_id=0, has_side_effects=True, vmem_limit_bytes=60 * 1024 * 1024
        ),
    )(
        q, k, v, lg, pre, hdl, ex, wo,
        tok, sc.reshape(1, W), ch.T, grw.reshape(1, TOK), eld.reshape(1, TOK), wg, wu, wd,
    )
    return pl.pallas_call(
        hand_over,
        name="hand_over",
        out_shape=(jax.ShapeDtypeStruct((CAP, W), bf16), jax.ShapeDtypeStruct((TOK, W), bf16)),
        in_specs=[vm, vm],
        out_specs=(vm, vm),
        compiler_params=pltpu.CompilerParams(vmem_limit_bytes=4 * 1024 * 1024),
    )(*outs)


def hand_over(a_ref, b_ref, c_ref, d_ref):
    c_ref[...] = a_ref[...]
    d_ref[...] = b_ref[...]


def solution(mesh):
    both = ("ep", "tp")
    placed = (
        P("ep", "tp"), P("ep", "tp"), P("ep", "tp"),
        P("tp", "ep"), P("tp", "ep"), P("tp"), P("tp", "ep"), P("tp", None),
        P(both, None), P(), P(both, None), P(both), P(both),
        P("ep", "tp", None), P("ep", "tp", None), P("ep", "tp", None),
    )
    return jax.shard_map(
        shards, mesh=mesh, in_specs=placed, out_specs=(P(both, None), P(both, None)), check_vma=False
    )
```

```python
import jax
import jax.numpy as jnp
from jax import lax
from jax.experimental import pallas as pl
from jax.experimental.pallas import tpu as pltpu
from jax.sharding import PartitionSpec as P

f32 = jnp.float32
bf16 = jnp.bfloat16
MESH = pl.DeviceIdType.MESH
EPS = 1e-06
SEG = 512
DH = 128
W = 2048
CAP = 32
EXPERTS = 16
EP = 16
NZ = 8
SH = 64
TOK = 128
CHUNKS = 4
COLS = W // CHUNKS
PIECES = 2 + CHUNKS
SLOTS = EXPERTS * CAP
ROWS = (slice(0, SLOTS // 2), slice(SLOTS // 2, SLOTS))
RELAY = {10: 15, 8: 4, 9: 13, 11: 7, 6: 7, 14: 13, 2: 1}
ORDER = list(RELAY)
DIRECT = [i for i in range(1, 16) if i not in RELAY]


def minus(i, j):
    return ((i // 4 - j // 4) % 4) * 4 + (i % 4 - j % 4) % 4


def dg(a, b, ca=1, cb=0):
    return lax.dot_general(a, b, (((ca,), (cb,)), ((), ())), preferred_element_type=f32)


def bdot(a, b, ca=1, cb=0):
    return dg(a.astype(bf16), b.astype(bf16), ca, cb)


def halves(a):
    hi = a.astype(bf16)
    return hi, (a - hi.astype(f32)).astype(bf16)


def dot3(a, b, ca=1, cb=0):
    ah, al = halves(a)
    bh, bl = halves(b)
    return dg(ah, bh, ca, cb) + dg(ah, bl, ca, cb) + dg(al, bh, ca, cb)


def iota(shape, dim):
    return lax.broadcasted_iota(jnp.int32, shape, dim)


def softplus(a):
    return jnp.maximum(a, 0.0) + jnp.log(1.0 + jnp.exp(-jnp.abs(a)))


def sigmoid(a):
    return 1.0 / (1.0 + jnp.exp(-a))


def kernel(
    q_hbm, k_hbm, v_hbm, lg_hbm, pre_hbm, hdl_hbm, ex_hbm, wo_hbm,
    tok_hbm, sc_hbm, ch_hbm, grw_hbm, eld_hbm, wg_hbm, wu_hbm, wd_hbm,
    o1_ref, o2_ref,
    q_ref, k_ref, v_ref, wo_ref, tok_ref, lg_ref, pre_ref, hdl_ref, ex_ref, sc_ref, ch_ref, grw_ref, eld_ref,
    gu, dw, obuf, xbuf, ybuf, rbuf, dhop, bhop, h_s,
    a_s, s_s, x_s, ol_s, p_s, m_s, st_own, st_all, att_s,
    mine, theirs, pbuf, rrp, rrm, rsp, rsm,
    rs, rr, ps, pr, dsem, dhr, bsem, brecv, bhr,
    ssend, srecv, xs, qs, qr_p, qr_m, ins,
):
    ep = lax.axis_index("ep")
    tp = lax.axis_index("tp")
    z, c = tp // 2, tp % 2
    y, x = ep // 4, ep % 4
    up = ((z + 1) % NZ) * 2 + c
    down = ((z + NZ - 1) % NZ) * 2 + c
    mate = tp + 1 - 2 * c

    def peer(i):
        return ((y + i // 4) % 4) * 4 + (x + i % 4) % 4

    def loaded(n):
        pairs = (
            (wg_hbm.at[0], gu.at[z, 0, c]), (wu_hbm.at[0], gu.at[z, 1, c]),
            (tok_hbm, tok_ref), (k_hbm, k_ref), (q_hbm, q_ref), (v_hbm, v_ref), (wo_hbm, wo_ref),
            (sc_hbm, sc_ref), (ch_hbm, ch_ref), (lg_hbm, lg_ref), (pre_hbm, pre_ref), (hdl_hbm, hdl_ref),
            (ex_hbm, ex_ref), (grw_hbm, grw_ref), (eld_hbm, eld_ref),
            *((wd_hbm.at[0, :, pl.ds(n * COLS, COLS)], dw.at[n, z, c]) for n in range(CHUNKS)),
        )
        return pltpu.make_async_copy(*pairs[n], ins.at[(0, *range(14), 14, 15, 15, 15)[n]])

    barrier = pltpu.get_barrier_semaphore()
    for i in ORDER + DIRECT:
        pl.semaphore_signal(barrier, inc=1, device_id={"ep": peer(i)}, device_id_type=MESH)
    for t in (up, down, mate):
        pl.semaphore_signal(barrier, inc=1, device_id={"tp": t}, device_id_type=MESH)
    for n in (0, 1, 15, 2, 7, 8, 3, 4, 5, 9, 10, 11, 12, 13, 14, 16, 17, 18, 6):
        loaded(n).start()
    pl.semaphore_wait(barrier, EP - 1 + 3)

    def remote(src, dst, send, recv, **where):
        return pltpu.make_async_remote_copy(
            src_ref=src, dst_ref=dst, send_sem=send, recv_sem=recv, device_id=where, device_id_type=MESH
        )

    def absorb(like, sem):
        pltpu.make_async_copy(like, like, sem).wait()

    def place(zs, core, piece, rows):
        whole = gu.at[zs, piece, core] if piece < 2 else dw.at[piece - 2, zs, core]
        return whole if rows is None else whole.at[pl.ds(rows, SH // 2)]

    def ring(s, piece, forward):
        slot = (z + NZ - s) % NZ if forward else (z + s) % NZ
        rows = None if s < 3 else (0 if forward else SH // 2)
        here = place(slot, c, piece, rows)
        if forward:
            return remote(here, here, rs.at[min(piece // 2, 1)], rr.at[s, piece], tp=up)
        return remote(here, here, rs.at[min(piece // 2, 1)], rr.at[s, piece], tp=down)

    def arrived(s, piece):
        like = gu.at[0, 0] if piece < 2 else dw.at[0, 0]
        absorb(like if s < 3 else like.at[0], rr.at[s, piece])

    def across(n, piece):
        if n == 0:
            slot, rows = z, None
        elif n <= 3:
            slot, rows = (z + NZ - n) % NZ, None
        elif n <= 6:
            slot, rows = (z + n - 3) % NZ, None
        else:
            slot, rows = (z + 4) % NZ, (0 if n == 7 else SH // 2)
        here = place(slot, c, piece, rows)
        wave = 0 if n == 0 else (n - 1) % 3 + 1 if n < 7 else 4
        return remote(here, here, ps.at[min(piece // 2, 1)], pr.at[wave if piece < 2 else 3 + piece], tp=mate)

    def step(piece, s):
        if s == 0:
            across(0, piece).start()
            ring(0, piece, True).start()
            ring(0, piece, False).start()
            return
        arrived(s - 1, piece)
        ring(s, piece, True).start()
        ring(s, piece, False).start()
        across(s, piece).start()
        across(3 + s, piece).start()

    def finish(piece):
        arrived(3, piece)
        across(7, piece).start()
        across(8, piece).start()

    absorb(gu.at[0, :, 0], ins.at[0])
    loaded(15).wait()
    for piece in range(3):
        step(piece, 0)

    for n in (2, 7, 8):
        loaded(n).wait()
    wide = tok_ref[...].astype(f32)
    normed = (
        wide * lax.rsqrt(jnp.sum(wide * wide, axis=1, keepdims=True) * (1.0 / W) + EPS) * sc_ref[...]
    ).astype(bf16)
    eye = iota((TOK, TOK), 0) == iota((TOK, TOK), 1)
    first = jnp.sum(jnp.where(eye, ch_ref[0:1, :], 0), axis=1, keepdims=True)
    second = jnp.sum(jnp.where(eye, ch_ref[1:2, :], 0), axis=1, keepdims=True)
    lane16 = iota((TOK, EXPERTS), 1)
    is_first, is_second = lane16 == first, lane16 == second
    member = jnp.where(is_first | is_second, 1.0, 0.0)
    before = jnp.where(iota((TOK, TOK), 1) < iota((TOK, TOK), 0), 1.0, 0.0)
    spot = bdot(before, member) + (lane16 * CAP).astype(f32)
    slot1 = jnp.sum(jnp.where(is_first, spot, 0.0), axis=1, keepdims=True).astype(jnp.int32)
    slot2 = jnp.sum(jnp.where(is_second, spot, 0.0), axis=1, keepdims=True).astype(jnp.int32)
    lanes = iota((TOK, SLOTS), 1)
    pick1 = jnp.where(lanes == slot1, 1.0, 0.0).astype(bf16)
    pick2 = jnp.where(lanes == slot2, 1.0, 0.0).astype(bf16)
    obuf[...] = dg(pick1 + pick2, normed, 0, 0).astype(bf16)

    def route(src, dst, hop, send, recv, hsend, hrecv):
        def first_leg(i):
            block = src.at[pl.ds(peer(i) * CAP, CAP)]
            if i in RELAY:
                n = ORDER.index(i)
                return remote(block, hop.at[n], send, hrecv(n), ep=peer(RELAY[i]))
            return remote(block, dst.at[pl.ds(ep * CAP, CAP)], send, recv, ep=peer(i))

        def second_leg(i):
            n = ORDER.index(i)
            origin = peer(minus(0, RELAY[i]))
            there = dst.at[pl.ds(origin * CAP, CAP)]
            return remote(hop.at[n], there, hsend, recv, ep=peer(minus(i, RELAY[i])))

        def forward(lo, hi):
            absorb(hop.at[pl.ds(lo, hi - lo)], hrecv(lo))
            for i in ORDER[lo:hi]:
                second_leg(i).start()

        return first_leg, forward

    others = pl.ds(0, (EP - 1) * CAP)
    d_first, d_forward = route(obuf, xbuf, dhop, dsem.at[0], dsem.at[1], dsem.at[2], lambda n: dhr.at[n // 4])
    back = [
        route(
            ybuf.at[n], rbuf.at[n], bhop.at[n], bsem.at[0], brecv.at[n], bsem.at[1],
            lambda m, n=n: bhr.at[n + (m // 4 if n == CHUNKS - 1 else 0)],
        )
        for n in range(CHUNKS)
    ]
    for i in ORDER + DIRECT:
        d_first(i).start()
    home = pl.ds(pl.multiple_of(ep * CAP, CAP), CAP)
    xbuf[home, :] = obuf[home, :]

    for n in (3, 4, 5, 9, 10, 11, 12):
        loaded(n).wait()
    kb, qb = k_ref[...], q_ref[...]
    ld = -jnp.exp(jnp.full((1, 1), hdl_ref[0], f32)) * softplus(pre_ref[...].astype(f32)) + ex_ref[...]
    beta = sigmoid(lg_ref[...].astype(f32))
    kf = kb.astype(f32)
    k2h, k2l = halves(kf * kf)
    ones = jnp.ones((8, DH), bf16)
    rk_row = lax.rsqrt((dg(ones, k2h, 1, 1) + dg(ones, k2l, 1, 1))[0:1] + EPS)
    upper = jnp.where(iota((SEG, SEG), 0) <= iota((SEG, SEG), 1), 1.0, 0.0).astype(bf16)
    ld8 = jnp.broadcast_to(ld, (8, SEG))
    l1, rest = halves(ld8)
    l2 = (ld8 - l1.astype(f32) - rest.astype(f32)).astype(bf16)
    c_row = (dg(l1, upper) + dg(rest, upper) + dg(l2, upper))[0:1]
    last = c_row[:, SEG - 1 : SEG]
    rhs, kds, qds = [], [], []
    for n in range(SEG // DH):
        rows = slice(n * DH, (n + 1) * DH)
        ii = iota((DH, SEG), 0) + n * DH
        jj = iota((DH, SEG), 1)
        c_col = jnp.sum(jnp.where(jj <= ii, ld, 0.0), axis=1, keepdims=True)
        b_col = jnp.sum(jnp.where(jj == ii, beta, 0.0), axis=1, keepdims=True)
        kt = kf[rows]
        qt = qb[rows].astype(f32)
        rk_col = lax.rsqrt(jnp.sum(kt * kt, axis=1, keepdims=True) + EPS)
        rq_col = lax.rsqrt(jnp.sum(qt * qt, axis=1, keepdims=True) + EPS) * DH**-0.5
        decay = jnp.where(ii >= jj, jnp.exp(jnp.minimum(c_col - c_row, 0.0)), 0.0) * rk_row
        a_s[rows, :] = jnp.where(ii > jj, dg(kb[rows], kb, 1, 1) * decay * (b_col * rk_col), 0.0)
        s_s[rows, :] = dg(qb[rows], kb, 1, 1) * decay * rq_col
        kn = kt * rk_col
        ec = jnp.exp(c_col)
        rhs.append(jnp.concatenate([b_col * v_ref[rows, :].astype(f32), (b_col * ec) * kn], axis=1))
        p_s[rows, :] = qt * (rq_col * ec)
        ol_s[rows, :] = kn * jnp.exp(last - c_col)
    for n in range(SEG // DH):
        x_s[n * DH : (n + 1) * DH, :] = rhs[n]

    half = SEG // 2
    i2, j2 = iota((half, half), 0), iota((half, half), 1)

    def same(shift):
        return (i2 >> shift) == (j2 >> shift)

    big = [a_s[0:half, 0:half], a_s[half:, half:]]
    power = [jnp.where(same(4), -b, 0.0) for b in big]
    inv = [jnp.where(i2 == j2, 1.0, 0.0) + p for p in power]
    for _ in range(3):
        power = [dot3(p, p) for p in power]
        inv = [t + dot3(t, p) for t, p in zip(inv, power)]
    for shift in (4, 5, 6, 7):
        off = [jnp.where(same(shift + 1) & ~same(shift), b, 0.0) for b in big]
        mid = [dot3(t, o) for t, o in zip(inv, off)]
        inv = [t - dot3(m, t) for t, m in zip(inv, mid)]
    x1 = dot3(inv[0], x_s[0:half, :])
    x2 = dot3(inv[1], x_s[half:, :] - dot3(a_s[half:, 0:half], x1))
    x_s[0:half, :] = x1
    x_s[half:, :] = x2
    e = dot3(ol_s[...], x_s[...], 0, 0)
    diag = iota((DH, DH), 0) == iota((DH, DH), 1)
    st_own[:, 0:DH] = (jnp.where(diag, jnp.exp(last), 0.0) - e[:, DH:]).astype(bf16)
    st_own[:, DH:] = e[:, :DH].astype(bf16)

    def state(j):
        return remote(st_own, st_all.at[ep], ssend.at[j], srecv.at[ep], ep=j)

    for j in range(1, EP):

        @pl.when(ep < j)
        def _(j=j):
            state(j).start()

    step(0, 1)
    sx = dot3(s_s[...], x_s[...])
    ol_s[...] = sx[:, :DH]
    p_s[...] = p_s[...] - sx[:, DH:]
    d_forward(0, 4)
    step(1, 1)
    step(2, 1)
    absorb(dw.at[pl.ds(1, 3), 0, 0], ins.at[15])
    step(3, 0)
    d_forward(4, 7)
    step(0, 2)
    step(1, 2)
    step(2, 2)
    step(3, 1)

    m_s[...] = jnp.zeros((DH, DH), f32)
    for j in range(EP - 1):

        @pl.when(j < ep)
        def _(j=j):
            remote(st_own, st_all.at[j], ssend.at[0], srecv.at[j], ep=0).wait_recv()
            m_s[...] = bdot(st_all[j, :, 0:DH], m_s[...]) + st_all[j, :, DH:].astype(f32)

    att = (ol_s[...] + bdot(p_s[...], m_s[...])).astype(bf16)
    att_s[...] = att.reshape(NZ, 2, CAP, DH)
    for n in (6, 13, 14):
        loaded(n).wait()
    theirs[...] = dg(att_s[:, 1 - c].reshape(SEG // 2, DH), wo_ref[...]).astype(bf16).reshape(NZ, CAP, W)
    swap = remote(theirs, pbuf, xs.at[0], xs.at[1], tp=mate)
    swap.start()
    mine[...] = dg(att_s[:, c].reshape(SEG // 2, DH), wo_ref[...]).reshape(NZ, CAP, W)

    def grow(zs, k):
        cols = slice(k * W // 2, (k + 1) * W // 2)
        return mine[zs, :, cols] + pbuf[zs, :, cols].astype(f32)

    def sums(s, k, forward):
        if forward:
            return remote(rsp.at[s, k], rrp.at[s, k], qs.at[0], qr_p.at[s, k], tp=up)
        return remote(rsm.at[s, k], rrm.at[s, k], qs.at[1], qr_m.at[s, k], tp=down)

    def hidden(zs):
        weights = gu[zs].reshape(4 * SH, W)
        both = [dg(xbuf[rows, :], weights, 1, 1) for rows in ROWS]
        for rows, b in zip(ROWS, both):
            g, u = b[:, : 2 * SH], b[:, 2 * SH :]
            h_s[rows, pl.ds(pl.multiple_of(zs * 2 * SH, 2 * SH), 2 * SH)] = (g * sigmoid(g) * u).astype(bf16)

    def crossed(s):
        absorb(gu.at[0] if 0 < s < 4 else gu.at[0, 0], pr.at[s])

    def group(s):
        for zs in {0: (z,), 4: ((z + 4) % NZ,)}.get(s, ((z + NZ - s) % NZ, (z + s) % NZ)):
            hidden(zs)

    def results(n):
        absorb(dw.at[n, :, 0], pr.at[5 + n])
        ybuf[n] = dg(h_s[...], dw[n].reshape(16 * SH, COLS)).astype(bf16)
        rbuf[n, home, :] = ybuf[n, home, :]

    def send(n, messages):
        for i in messages:
            back[n][0](i).start()

    def relay(n):
        if n < CHUNKS - 1:
            back[n][1](0, 7)
        else:
            back[n][1](0, 4)
            back[n][1](4, 7)

    def begin(k):
        sums(0, k, True).start()
        sums(0, k, False).start()

    def add(s, k):
        sums(s - 1, k, True).wait_recv()
        rsp[s, k] = (rrp[s - 1, k].astype(f32) + grow((z + 4 - s) % NZ, k)).astype(bf16)
        sums(s, k, True).start()
        if s < 3:
            sums(s - 1, k, False).wait_recv()
            rsm[s, k] = (rrm[s - 1, k].astype(f32) + grow((z + NZ - 3 + s) % NZ, k)).astype(bf16)
            sums(s, k, False).start()

    def total(k):
        sums(2, k, False).wait_recv()
        sums(3, k, True).wait_recv()
        o1_ref[:, k * W // 2 : (k + 1) * W // 2] = (
            grow(z, k) + rrp[3, k].astype(f32) + rrm[2, k].astype(f32)
        ).astype(bf16)

    lead = sigmoid(eld_ref[...])
    w1 = jnp.sum(jnp.where(eye, grw_ref[...] * lead, 0.0), axis=1, keepdims=True)
    w2 = jnp.sum(jnp.where(eye, grw_ref[...] * (1.0 - lead), 0.0), axis=1, keepdims=True)

    def mix(n):
        absorb(rbuf.at[n, others], brecv.at[n])
        mixed = w1 * dg(pick1, rbuf[n]) + w2 * dg(pick2, rbuf[n])
        o2_ref[:, n * COLS : (n + 1) * COLS] = mixed.astype(bf16)

    step(0, 3)
    absorb(xbuf.at[others], dsem.at[1])
    crossed(0)
    group(0)
    crossed(1)
    group(1)
    step(1, 3)
    step(2, 3)
    step(4, 0)
    crossed(2)
    group(2)
    step(3, 2)
    step(5, 0)
    swap.wait_recv()
    for k in range(2):
        rsp[0, k] = grow((z + 4) % NZ, k).astype(bf16)
        rsm[0, k] = grow((z + NZ - 3) % NZ, k).astype(bf16)
    crossed(3)
    group(3)
    finish(0)
    finish(1)
    @pl.when(c == 0)
    def _():
        crossed(4)
        group(4)
        finish(2)
        results(0)
        send(0, ORDER + DIRECT)
        step(4, 1)

    @pl.when(c == 1)
    def _():
        finish(2)
        step(4, 1)
        crossed(4)
        group(4)
        results(0)
        send(0, ORDER + DIRECT)

    step(3, 3)
    step(5, 1)
    step(4, 2)
    begin(0)
    finish(3)
    step(5, 2)
    results(1)
    send(1, ORDER + DIRECT)
    step(4, 3)
    begin(1)
    relay(0)
    step(5, 3)
    add(1, 0)
    finish(4)
    results(2)
    send(2, ORDER)
    relay(1)
    send(2, DIRECT)
    add(1, 1)
    finish(5)
    results(3)
    send(3, ORDER)
    add(2, 0)
    relay(2)
    send(3, DIRECT)
    add(2, 1)
    mix(0)
    mix(1)
    add(3, 0)
    relay(3)
    add(3, 1)
    mix(2)
    total(0)
    total(1)
    mix(3)

    absorb(gu.at[pl.ds(0, 7), :, 0], rs.at[0])
    absorb(dw.at[:, pl.ds(0, 7), 0], rs.at[1])
    absorb(gu.at[:, :, 0], ps.at[0])
    absorb(dw.at[:, :, 0], ps.at[1])
    absorb(obuf.at[others], dsem.at[0])
    absorb(dhop, dsem.at[2])
    absorb(ybuf.at[:, others], bsem.at[0])
    absorb(bhop, bsem.at[1])
    absorb(rsp, qs.at[0])
    absorb(rsm, qs.at[1])
    swap.wait_send()
    for j in range(1, EP):

        @pl.when(ep < j)
        def _(j=j):
            state(j).wait_send()


def shards(q, k, v, lg, pre, hdl, ex, wo, tok, sc, ch, grw, eld, wg, wu, wd):
    V = pltpu.VMEM
    dma = pltpu.SemaphoreType.DMA
    scratch = [
        V((SEG, DH), bf16), V((SEG, DH), bf16), V((SEG, DH), bf16), V((DH, W), bf16), V((TOK, W), bf16),
        V((1, SEG), bf16), V((1, SEG), bf16), pltpu.SMEM((1,), f32), V((1, SEG), f32),
        V((1, W), f32), V((2, TOK), jnp.int32), V((1, TOK), f32), V((1, TOK), f32),
        V((NZ, 2, 2, SH, W), bf16), V((CHUNKS, NZ, 2, SH, COLS), bf16),
        V((SLOTS, W), bf16), V((SLOTS, W), bf16), V((CHUNKS, SLOTS, COLS), bf16), V((CHUNKS, SLOTS, COLS), bf16),
        V((7, CAP, W), bf16), V((CHUNKS, 7, CAP, COLS), bf16), V((SLOTS, 16 * SH), bf16),
        V((SEG, SEG), f32), V((SEG, SEG), f32), V((SEG, 2 * DH), f32), V((SEG, DH), f32), V((SEG, DH), f32),
        V((DH, DH), f32), V((DH, 2 * DH), bf16), V((EP, DH, 2 * DH), bf16), V((NZ, 2, CAP, DH), bf16),
        V((NZ, CAP, W), f32), V((NZ, CAP, W), bf16), V((NZ, CAP, W), bf16),
        V((4, 2, CAP, W // 2), bf16), V((3, 2, CAP, W // 2), bf16),
        V((4, 2, CAP, W // 2), bf16), V((3, 2, CAP, W // 2), bf16),
        dma((2,)), dma((4, PIECES)), dma((2,)), dma((5 + CHUNKS,)),
        dma((3,)), dma((2,)), dma((2,)), dma((CHUNKS,)), dma((CHUNKS + 1,)),
        dma((EP,)), dma((EP,)), dma((2,)), dma((2,)), dma((4, 2)), dma((3, 2)), dma((16,)),
    ]
    vm = pl.BlockSpec(memory_space=pltpu.VMEM)
    hbm = pl.BlockSpec(memory_space=pl.ANY)
    outs = pl.pallas_call(
        kernel,
        name="mixer_and_experts",
        out_shape=(V((CAP, W), bf16), V((TOK, W), bf16)),
        in_specs=[hbm] * 16,
        out_specs=(vm, vm),
        scratch_shapes=scratch,
        compiler_params=pltpu.CompilerParams(
            collective_id=0, has_side_effects=True, vmem_limit_bytes=60 * 1024 * 1024
        ),
    )(
        q, k, v, lg, pre, hdl, ex, wo,
        tok, sc.reshape(1, W), ch.T, grw.reshape(1, TOK), eld.reshape(1, TOK), wg, wu, wd,
    )
    return pl.pallas_call(
        hand_over,
        name="hand_over",
        out_shape=(jax.ShapeDtypeStruct((CAP, W), bf16), jax.ShapeDtypeStruct((TOK, W), bf16)),
        in_specs=[vm, vm],
        out_specs=(vm, vm),
        compiler_params=pltpu.CompilerParams(vmem_limit_bytes=4 * 1024 * 1024),
    )(*outs)


def hand_over(a_ref, b_ref, c_ref, d_ref):
    c_ref[...] = a_ref[...]
    d_ref[...] = b_ref[...]


def solution(mesh):
    both = ("ep", "tp")
    placed = (
        P("ep", "tp"), P("ep", "tp"), P("ep", "tp"),
        P("tp", "ep"), P("tp", "ep"), P("tp"), P("tp", "ep"), P("tp", None),
        P(both, None), P(), P(both, None), P(both), P(both),
        P("ep", "tp", None), P("ep", "tp", None), P("ep", "tp", None),
    )
    return jax.shard_map(
        shards, mesh=mesh, in_specs=placed, out_specs=(P(both, None), P(both, None)), check_vma=False
    )
```

```python
import jax
import jax.numpy as jnp
from jax import lax
from jax.experimental import pallas as pl
from jax.experimental.pallas import tpu as pltpu
from jax.sharding import PartitionSpec as P

f32 = jnp.float32
bf16 = jnp.bfloat16
MESH = pl.DeviceIdType.MESH
EPS = 1e-06
SEG = 512
DH = 128
W = 2048
CAP = 32
EXPERTS = 16
EP = 16
NZ = 8
SH = 64
TOK = 128
CHUNKS = 4
COLS = W // CHUNKS
PIECES = 2 + CHUNKS
SLOTS = EXPERTS * CAP
ROWS = (slice(0, SLOTS // 2), slice(SLOTS // 2, SLOTS))
RELAY = {10: 15, 8: 4, 9: 13, 11: 7, 6: 7, 14: 13, 2: 1}
ORDER = list(RELAY)
DIRECT = [i for i in range(1, 16) if i not in RELAY]


def minus(i, j):
    return ((i // 4 - j // 4) % 4) * 4 + (i % 4 - j % 4) % 4


def dg(a, b, ca=1, cb=0):
    return lax.dot_general(a, b, (((ca,), (cb,)), ((), ())), preferred_element_type=f32)


def bdot(a, b, ca=1, cb=0):
    return dg(a.astype(bf16), b.astype(bf16), ca, cb)


def halves(a):
    hi = a.astype(bf16)
    return hi, (a - hi.astype(f32)).astype(bf16)


def dot3(a, b, ca=1, cb=0):
    ah, al = halves(a)
    bh, bl = halves(b)
    return dg(ah, bh, ca, cb) + dg(ah, bl, ca, cb) + dg(al, bh, ca, cb)


def iota(shape, dim):
    return lax.broadcasted_iota(jnp.int32, shape, dim)


def softplus(a):
    return jnp.maximum(a, 0.0) + jnp.log(1.0 + jnp.exp(-jnp.abs(a)))


def sigmoid(a):
    return 1.0 / (1.0 + jnp.exp(-a))


def kernel(
    q_hbm, k_hbm, v_hbm, lg_hbm, pre_hbm, hdl_hbm, ex_hbm, wo_hbm,
    tok_hbm, sc_hbm, ch_hbm, grw_hbm, eld_hbm, wg_hbm, wu_hbm, wd_hbm,
    o1_ref, o2_ref,
    q_ref, k_ref, v_ref, wo_ref, tok_ref, lg_ref, pre_ref, hdl_ref, ex_ref, sc_ref, ch_ref, grw_ref, eld_ref,
    gu, dw, obuf, xbuf, ybuf, rbuf, dhop, bhop, h_s,
    a_s, s_s, x_s, ol_s, p_s, m_s, st_own, st_all, att_s,
    mine, theirs, pbuf, rrp, rrm, rsp, rsm,
    rs, rr, ps, pr, dsem, dhr, bsem, brecv, bhr,
    ssend, srecv, xs, qs, qr_p, qr_m, ins,
):
    ep = lax.axis_index("ep")
    tp = lax.axis_index("tp")
    z, c = tp // 2, tp % 2
    y, x = ep // 4, ep % 4
    up = ((z + 1) % NZ) * 2 + c
    down = ((z + NZ - 1) % NZ) * 2 + c
    mate = tp + 1 - 2 * c

    def peer(i):
        return ((y + i // 4) % 4) * 4 + (x + i % 4) % 4

    def loaded(n):
        pairs = (
            (wg_hbm.at[0], gu.at[z, 0, c]), (wu_hbm.at[0], gu.at[z, 1, c]),
            (tok_hbm, tok_ref), (k_hbm, k_ref), (q_hbm, q_ref), (v_hbm, v_ref), (wo_hbm, wo_ref),
            (sc_hbm, sc_ref), (ch_hbm, ch_ref), (lg_hbm, lg_ref), (pre_hbm, pre_ref), (hdl_hbm, hdl_ref),
            (ex_hbm, ex_ref), (grw_hbm, grw_ref), (eld_hbm, eld_ref),
            *((wd_hbm.at[0, :, pl.ds(n * COLS, COLS)], dw.at[n, z, c]) for n in range(CHUNKS)),
        )
        return pltpu.make_async_copy(*pairs[n], ins.at[(0, *range(14), 14, 15, 15, 15)[n]])

    barrier = pltpu.get_barrier_semaphore()
    for i in ORDER + DIRECT:
        pl.semaphore_signal(barrier, inc=1, device_id={"ep": peer(i)}, device_id_type=MESH)
    for t in (up, down, mate):
        pl.semaphore_signal(barrier, inc=1, device_id={"tp": t}, device_id_type=MESH)
    for n in (0, 1, 15, 2, 7, 8, 3, 4, 5, 9, 10, 11, 12, 13, 14, 16, 17, 18, 6):
        loaded(n).start()
    pl.semaphore_wait(barrier, EP - 1 + 3)

    def remote(src, dst, send, recv, **where):
        return pltpu.make_async_remote_copy(
            src_ref=src, dst_ref=dst, send_sem=send, recv_sem=recv, device_id=where, device_id_type=MESH
        )

    def absorb(like, sem):
        pltpu.make_async_copy(like, like, sem).wait()

    def place(zs, core, piece, rows):
        whole = gu.at[zs, piece, core] if piece < 2 else dw.at[piece - 2, zs, core]
        return whole if rows is None else whole.at[pl.ds(rows, SH // 2)]

    def ring(s, piece, forward):
        slot = (z + NZ - s) % NZ if forward else (z + s) % NZ
        rows = None if s < 3 else (0 if forward else SH // 2)
        here = place(slot, c, piece, rows)
        if forward:
            return remote(here, here, rs.at[min(piece // 2, 1)], rr.at[s, piece], tp=up)
        return remote(here, here, rs.at[min(piece // 2, 1)], rr.at[s, piece], tp=down)

    def arrived(s, piece):
        like = gu.at[0, 0] if piece < 2 else dw.at[0, 0]
        absorb(like if s < 3 else like.at[0], rr.at[s, piece])

    def across(n, piece):
        if n == 0:
            slot, rows = z, None
        elif n <= 3:
            slot, rows = (z + NZ - n) % NZ, None
        elif n <= 6:
            slot, rows = (z + n - 3) % NZ, None
        else:
            slot, rows = (z + 4) % NZ, (0 if n == 7 else SH // 2)
        here = place(slot, c, piece, rows)
        wave = 0 if n == 0 else (n - 1) % 3 + 1 if n < 7 else 4
        return remote(here, here, ps.at[min(piece // 2, 1)], pr.at[wave if piece < 2 else 3 + piece], tp=mate)

    def step(piece, s):
        if s == 0:
            across(0, piece).start()
            ring(0, piece, True).start()
            ring(0, piece, False).start()
            return
        arrived(s - 1, piece)
        ring(s, piece, True).start()
        ring(s, piece, False).start()
        across(s, piece).start()
        across(3 + s, piece).start()

    def finish(piece):
        arrived(3, piece)
        across(7, piece).start()
        across(8, piece).start()

    absorb(gu.at[0, :, 0], ins.at[0])
    loaded(15).wait()
    for piece in range(3):
        step(piece, 0)

    for n in (2, 7, 8):
        loaded(n).wait()
    wide = tok_ref[...].astype(f32)
    normed = (
        wide * lax.rsqrt(jnp.sum(wide * wide, axis=1, keepdims=True) * (1.0 / W) + EPS) * sc_ref[...]
    ).astype(bf16)
    eye = iota((TOK, TOK), 0) == iota((TOK, TOK), 1)
    first = jnp.sum(jnp.where(eye, ch_ref[0:1, :], 0), axis=1, keepdims=True)
    second = jnp.sum(jnp.where(eye, ch_ref[1:2, :], 0), axis=1, keepdims=True)
    lane16 = iota((TOK, EXPERTS), 1)
    is_first, is_second = lane16 == first, lane16 == second
    member = jnp.where(is_first | is_second, 1.0, 0.0)
    before = jnp.where(iota((TOK, TOK), 1) < iota((TOK, TOK), 0), 1.0, 0.0)
    spot = bdot(before, member) + (lane16 * CAP).astype(f32)
    slot1 = jnp.sum(jnp.where(is_first, spot, 0.0), axis=1, keepdims=True).astype(jnp.int32)
    slot2 = jnp.sum(jnp.where(is_second, spot, 0.0), axis=1, keepdims=True).astype(jnp.int32)
    lanes = iota((TOK, SLOTS), 1)
    pick1 = jnp.where(lanes == slot1, 1.0, 0.0).astype(bf16)
    pick2 = jnp.where(lanes == slot2, 1.0, 0.0).astype(bf16)
    obuf[...] = dg(pick1 + pick2, normed, 0, 0).astype(bf16)

    def route(src, dst, hop, send, recv, hsend, hrecv):
        def first_leg(i):
            block = src.at[pl.ds(peer(i) * CAP, CAP)]
            if i in RELAY:
                n = ORDER.index(i)
                return remote(block, hop.at[n], send, hrecv(n), ep=peer(RELAY[i]))
            return remote(block, dst.at[pl.ds(ep * CAP, CAP)], send, recv, ep=peer(i))

        def second_leg(i):
            n = ORDER.index(i)
            origin = peer(minus(0, RELAY[i]))
            there = dst.at[pl.ds(origin * CAP, CAP)]
            return remote(hop.at[n], there, hsend, recv, ep=peer(minus(i, RELAY[i])))

        def forward(lo, hi):
            absorb(hop.at[pl.ds(lo, hi - lo)], hrecv(lo))
            for i in ORDER[lo:hi]:
                second_leg(i).start()

        return first_leg, forward

    others = pl.ds(0, (EP - 1) * CAP)
    d_first, d_forward = route(obuf, xbuf, dhop, dsem.at[0], dsem.at[1], dsem.at[2], lambda n: dhr.at[n // 4])
    back = [
        route(
            ybuf.at[n], rbuf.at[n], bhop.at[n], bsem.at[0], brecv.at[n], bsem.at[1],
            lambda m, n=n: bhr.at[n + (m // 4 if n == CHUNKS - 1 else 0)],
        )
        for n in range(CHUNKS)
    ]
    for i in ORDER + DIRECT:
        d_first(i).start()
    home = pl.ds(pl.multiple_of(ep * CAP, CAP), CAP)
    xbuf[home, :] = obuf[home, :]

    for n in (3, 4, 5, 9, 10, 11, 12):
        loaded(n).wait()
    kb, qb = k_ref[...], q_ref[...]
    ld = -jnp.exp(jnp.full((1, 1), hdl_ref[0], f32)) * softplus(pre_ref[...].astype(f32)) + ex_ref[...]
    beta = sigmoid(lg_ref[...].astype(f32))
    kf = kb.astype(f32)
    k2h, k2l = halves(kf * kf)
    ones = jnp.ones((8, DH), bf16)
    rk_row = lax.rsqrt((dg(ones, k2h, 1, 1) + dg(ones, k2l, 1, 1))[0:1] + EPS)
    upper = jnp.where(iota((SEG, SEG), 0) <= iota((SEG, SEG), 1), 1.0, 0.0).astype(bf16)
    ld8 = jnp.broadcast_to(ld, (8, SEG))
    l1, rest = halves(ld8)
    l2 = (ld8 - l1.astype(f32) - rest.astype(f32)).astype(bf16)
    c_row = (dg(l1, upper) + dg(rest, upper) + dg(l2, upper))[0:1]
    last = c_row[:, SEG - 1 : SEG]
    rhs, kds, qds = [], [], []
    for n in range(SEG // DH):
        rows = slice(n * DH, (n + 1) * DH)
        ii = iota((DH, SEG), 0) + n * DH
        jj = iota((DH, SEG), 1)
        c_col = jnp.sum(jnp.where(jj <= ii, ld, 0.0), axis=1, keepdims=True)
        b_col = jnp.sum(jnp.where(jj == ii, beta, 0.0), axis=1, keepdims=True)
        kt = kf[rows]
        qt = qb[rows].astype(f32)
        rk_col = lax.rsqrt(jnp.sum(kt * kt, axis=1, keepdims=True) + EPS)
        rq_col = lax.rsqrt(jnp.sum(qt * qt, axis=1, keepdims=True) + EPS) * DH**-0.5
        decay = jnp.where(ii >= jj, jnp.exp(jnp.minimum(c_col - c_row, 0.0)), 0.0) * rk_row
        a_s[rows, :] = jnp.where(ii > jj, dg(kb[rows], kb, 1, 1) * decay * (b_col * rk_col), 0.0)
        s_s[rows, :] = dg(qb[rows], kb, 1, 1) * decay * rq_col
        kn = kt * rk_col
        ec = jnp.exp(c_col)
        rhs.append(jnp.concatenate([b_col * v_ref[rows, :].astype(f32), (b_col * ec) * kn], axis=1))
        p_s[rows, :] = qt * (rq_col * ec)
        ol_s[rows, :] = kn * jnp.exp(last - c_col)
    for n in range(SEG // DH):
        x_s[n * DH : (n + 1) * DH, :] = rhs[n]

    half = SEG // 2
    i2, j2 = iota((half, half), 0), iota((half, half), 1)

    def same(shift):
        return (i2 >> shift) == (j2 >> shift)

    big = [a_s[0:half, 0:half], a_s[half:, half:]]
    power = [jnp.where(same(4), -b, 0.0) for b in big]
    inv = [jnp.where(i2 == j2, 1.0, 0.0) + p for p in power]
    for _ in range(3):
        power = [dot3(p, p) for p in power]
        inv = [t + dot3(t, p) for t, p in zip(inv, power)]
    for shift in (4, 5, 6, 7):
        off = [jnp.where(same(shift + 1) & ~same(shift), b, 0.0) for b in big]
        mid = [dot3(t, o) for t, o in zip(inv, off)]
        inv = [t - dot3(m, t) for t, m in zip(inv, mid)]
    x1 = dot3(inv[0], x_s[0:half, :])
    x2 = dot3(inv[1], x_s[half:, :] - dot3(a_s[half:, 0:half], x1))
    x_s[0:half, :] = x1
    x_s[half:, :] = x2
    e = dot3(ol_s[...], x_s[...], 0, 0)
    diag = iota((DH, DH), 0) == iota((DH, DH), 1)
    st_own[:, 0:DH] = (jnp.where(diag, jnp.exp(last), 0.0) - e[:, DH:]).astype(bf16)
    st_own[:, DH:] = e[:, :DH].astype(bf16)

    def state(j):
        return remote(st_own, st_all.at[ep], ssend.at[j], srecv.at[ep], ep=j)

    for j in range(1, EP):

        @pl.when(ep < j)
        def _(j=j):
            state(j).start()

    step(0, 1)
    sx = dot3(s_s[...], x_s[...])
    ol_s[...] = sx[:, :DH]
    p_s[...] = p_s[...] - sx[:, DH:]
    d_forward(0, 4)
    step(1, 1)
    step(2, 1)
    absorb(dw.at[pl.ds(1, 3), 0, 0], ins.at[15])
    step(3, 0)
    d_forward(4, 7)
    step(0, 2)
    step(1, 2)
    step(2, 2)
    step(3, 1)

    m_s[...] = jnp.zeros((DH, DH), f32)
    for j in range(EP - 1):

        @pl.when(j < ep)
        def _(j=j):
            remote(st_own, st_all.at[j], ssend.at[0], srecv.at[j], ep=0).wait_recv()
            m_s[...] = bdot(st_all[j, :, 0:DH], m_s[...]) + st_all[j, :, DH:].astype(f32)

    att = (ol_s[...] + bdot(p_s[...], m_s[...])).astype(bf16)
    att_s[...] = att.reshape(NZ, 2, CAP, DH)
    for n in (6, 13, 14):
        loaded(n).wait()
    theirs[...] = dg(att_s[:, 1 - c].reshape(SEG // 2, DH), wo_ref[...]).astype(bf16).reshape(NZ, CAP, W)
    swap = remote(theirs, pbuf, xs.at[0], xs.at[1], tp=mate)
    swap.start()
    mine[...] = dg(att_s[:, c].reshape(SEG // 2, DH), wo_ref[...]).reshape(NZ, CAP, W)

    def grow(zs, k):
        cols = slice(k * W // 2, (k + 1) * W // 2)
        return mine[zs, :, cols] + pbuf[zs, :, cols].astype(f32)

    def sums(s, k, forward):
        if forward:
            return remote(rsp.at[s, k], rrp.at[s, k], qs.at[0], qr_p.at[s, k], tp=up)
        return remote(rsm.at[s, k], rrm.at[s, k], qs.at[1], qr_m.at[s, k], tp=down)

    def hidden(zs):
        weights = gu[zs].reshape(4 * SH, W)
        both = [dg(xbuf[rows, :], weights, 1, 1) for rows in ROWS]
        for rows, b in zip(ROWS, both):
            g, u = b[:, : 2 * SH], b[:, 2 * SH :]
            h_s[rows, pl.ds(pl.multiple_of(zs * 2 * SH, 2 * SH), 2 * SH)] = (g * sigmoid(g) * u).astype(bf16)

    def crossed(s):
        absorb(gu.at[0] if 0 < s < 4 else gu.at[0, 0], pr.at[s])

    def group(s):
        for zs in {0: (z,), 4: ((z + 4) % NZ,)}.get(s, ((z + NZ - s) % NZ, (z + s) % NZ)):
            hidden(zs)

    def results(n):
        absorb(dw.at[n, :, 0], pr.at[5 + n])
        weights = dw[n].reshape(16 * SH, COLS)
        block = 4 * CAP
        for pair in ((2, 1), (3, 0)):
            rows = [pl.ds(pl.multiple_of(((y + d) % 4) * block, block), block) for d in pair]
            both = dg(jnp.concatenate([h_s[r, :] for r in rows], axis=0), weights).astype(bf16)
            for k, r in enumerate(rows):
                ybuf[n, r, :] = both[k * block : (k + 1) * block]
            send(n, [i for i in ORDER if i // 4 in pair])
        rbuf[n, home, :] = ybuf[n, home, :]

    def send(n, messages):
        for i in messages:
            back[n][0](i).start()

    def relay(n):
        if n < CHUNKS - 1:
            back[n][1](0, 7)
        else:
            back[n][1](0, 4)
            back[n][1](4, 7)

    def begin(k):
        sums(0, k, True).start()
        sums(0, k, False).start()

    def add(s, k):
        sums(s - 1, k, True).wait_recv()
        rsp[s, k] = (rrp[s - 1, k].astype(f32) + grow((z + 4 - s) % NZ, k)).astype(bf16)
        sums(s, k, True).start()
        if s < 3:
            sums(s - 1, k, False).wait_recv()
            rsm[s, k] = (rrm[s - 1, k].astype(f32) + grow((z + NZ - 3 + s) % NZ, k)).astype(bf16)
            sums(s, k, False).start()

    def total(k):
        sums(2, k, False).wait_recv()
        sums(3, k, True).wait_recv()
        o1_ref[:, k * W // 2 : (k + 1) * W // 2] = (
            grow(z, k) + rrp[3, k].astype(f32) + rrm[2, k].astype(f32)
        ).astype(bf16)

    lead = sigmoid(eld_ref[...])
    w1 = jnp.sum(jnp.where(eye, grw_ref[...] * lead, 0.0), axis=1, keepdims=True)
    w2 = jnp.sum(jnp.where(eye, grw_ref[...] * (1.0 - lead), 0.0), axis=1, keepdims=True)

    def mix(n):
        absorb(rbuf.at[n, others], brecv.at[n])
        mixed = w1 * dg(pick1, rbuf[n]) + w2 * dg(pick2, rbuf[n])
        o2_ref[:, n * COLS : (n + 1) * COLS] = mixed.astype(bf16)

    step(0, 3)
    absorb(xbuf.at[others], dsem.at[1])
    crossed(0)
    group(0)
    crossed(1)
    group(1)
    step(1, 3)
    step(2, 3)
    step(4, 0)
    crossed(2)
    group(2)
    step(3, 2)
    step(5, 0)
    swap.wait_recv()
    for k in range(2):
        rsp[0, k] = grow((z + 4) % NZ, k).astype(bf16)
        rsm[0, k] = grow((z + NZ - 3) % NZ, k).astype(bf16)
    crossed(3)
    group(3)
    finish(0)
    finish(1)
    @pl.when(c == 0)
    def _():
        crossed(4)
        group(4)
        finish(2)
        results(0)
        send(0, DIRECT)
        step(4, 1)

    @pl.when(c == 1)
    def _():
        finish(2)
        step(4, 1)
        crossed(4)
        group(4)
        results(0)
        send(0, DIRECT)

    step(3, 3)
    step(5, 1)
    step(4, 2)
    begin(0)
    finish(3)
    step(5, 2)
    results(1)
    send(1, DIRECT)
    step(4, 3)
    begin(1)
    relay(0)
    step(5, 3)
    add(1, 0)
    finish(4)
    results(2)
    relay(1)
    send(2, DIRECT)
    add(1, 1)
    finish(5)
    results(3)
    add(2, 0)
    relay(2)
    send(3, DIRECT)
    add(2, 1)
    mix(0)
    mix(1)
    add(3, 0)
    relay(3)
    add(3, 1)
    mix(2)
    total(0)
    total(1)
    mix(3)

    absorb(gu.at[pl.ds(0, 7), :, 0], rs.at[0])
    absorb(dw.at[:, pl.ds(0, 7), 0], rs.at[1])
    absorb(gu.at[:, :, 0], ps.at[0])
    absorb(dw.at[:, :, 0], ps.at[1])
    absorb(obuf.at[others], dsem.at[0])
    absorb(dhop, dsem.at[2])
    absorb(ybuf.at[:, others], bsem.at[0])
    absorb(bhop, bsem.at[1])
    absorb(rsp, qs.at[0])
    absorb(rsm, qs.at[1])
    swap.wait_send()
    for j in range(1, EP):

        @pl.when(ep < j)
        def _(j=j):
            state(j).wait_send()


def shards(q, k, v, lg, pre, hdl, ex, wo, tok, sc, ch, grw, eld, wg, wu, wd):
    V = pltpu.VMEM
    dma = pltpu.SemaphoreType.DMA
    scratch = [
        V((SEG, DH), bf16), V((SEG, DH), bf16), V((SEG, DH), bf16), V((DH, W), bf16), V((TOK, W), bf16),
        V((1, SEG), bf16), V((1, SEG), bf16), pltpu.SMEM((1,), f32), V((1, SEG), f32),
        V((1, W), f32), V((2, TOK), jnp.int32), V((1, TOK), f32), V((1, TOK), f32),
        V((NZ, 2, 2, SH, W), bf16), V((CHUNKS, NZ, 2, SH, COLS), bf16),
        V((SLOTS, W), bf16), V((SLOTS, W), bf16), V((CHUNKS, SLOTS, COLS), bf16), V((CHUNKS, SLOTS, COLS), bf16),
        V((7, CAP, W), bf16), V((CHUNKS, 7, CAP, COLS), bf16), V((SLOTS, 16 * SH), bf16),
        V((SEG, SEG), f32), V((SEG, SEG), f32), V((SEG, 2 * DH), f32), V((SEG, DH), f32), V((SEG, DH), f32),
        V((DH, DH), f32), V((DH, 2 * DH), bf16), V((EP, DH, 2 * DH), bf16), V((NZ, 2, CAP, DH), bf16),
        V((NZ, CAP, W), f32), V((NZ, CAP, W), bf16), V((NZ, CAP, W), bf16),
        V((4, 2, CAP, W // 2), bf16), V((3, 2, CAP, W // 2), bf16),
        V((4, 2, CAP, W // 2), bf16), V((3, 2, CAP, W // 2), bf16),
        dma((2,)), dma((4, PIECES)), dma((2,)), dma((5 + CHUNKS,)),
        dma((3,)), dma((2,)), dma((2,)), dma((CHUNKS,)), dma((CHUNKS + 1,)),
        dma((EP,)), dma((EP,)), dma((2,)), dma((2,)), dma((4, 2)), dma((3, 2)), dma((16,)),
    ]
    vm = pl.BlockSpec(memory_space=pltpu.VMEM)
    hbm = pl.BlockSpec(memory_space=pl.ANY)
    outs = pl.pallas_call(
        kernel,
        name="mixer_and_experts",
        out_shape=(V((CAP, W), bf16), V((TOK, W), bf16)),
        in_specs=[hbm] * 16,
        out_specs=(vm, vm),
        scratch_shapes=scratch,
        compiler_params=pltpu.CompilerParams(
            collective_id=0, has_side_effects=True, vmem_limit_bytes=60 * 1024 * 1024
        ),
    )(
        q, k, v, lg, pre, hdl, ex, wo,
        tok, sc.reshape(1, W), ch.T, grw.reshape(1, TOK), eld.reshape(1, TOK), wg, wu, wd,
    )
    return pl.pallas_call(
        hand_over,
        name="hand_over",
        out_shape=(jax.ShapeDtypeStruct((CAP, W), bf16), jax.ShapeDtypeStruct((TOK, W), bf16)),
        in_specs=[vm, vm],
        out_specs=(vm, vm),
        compiler_params=pltpu.CompilerParams(vmem_limit_bytes=4 * 1024 * 1024),
    )(*outs)


def hand_over(a_ref, b_ref, c_ref, d_ref):
    c_ref[...] = a_ref[...]
    d_ref[...] = b_ref[...]


def solution(mesh):
    both = ("ep", "tp")
    placed = (
        P("ep", "tp"), P("ep", "tp"), P("ep", "tp"),
        P("tp", "ep"), P("tp", "ep"), P("tp"), P("tp", "ep"), P("tp", None),
        P(both, None), P(), P(both, None), P(both), P(both),
        P("ep", "tp", None), P("ep", "tp", None), P("ep", "tp", None),
    )
    return jax.shard_map(
        shards, mesh=mesh, in_specs=placed, out_specs=(P(both, None), P(both, None)), check_vma=False
    )
```

```python
import jax
import jax.numpy as jnp
from jax import lax
from jax.experimental import pallas as pl
from jax.experimental.pallas import tpu as pltpu
from jax.sharding import PartitionSpec as P

f32 = jnp.float32
bf16 = jnp.bfloat16
MESH = pl.DeviceIdType.MESH
EPS = 1e-06
SEG = 512
DH = 128
W = 2048
CAP = 32
EXPERTS = 16
EP = 16
NZ = 8
SH = 64
TOK = 128
CHUNKS = 4
COLS = W // CHUNKS
PIECES = 2 + CHUNKS
SLOTS = EXPERTS * CAP
ROWS = (slice(0, SLOTS // 2), slice(SLOTS // 2, SLOTS))
RELAY = {10: 15, 8: 4, 9: 13, 11: 7, 6: 7, 14: 13, 2: 1}
ORDER = list(RELAY)
DIRECT = [i for i in range(1, 16) if i not in RELAY]


def minus(i, j):
    return ((i // 4 - j // 4) % 4) * 4 + (i % 4 - j % 4) % 4


def dg(a, b, ca=1, cb=0):
    return lax.dot_general(a, b, (((ca,), (cb,)), ((), ())), preferred_element_type=f32)


def bdot(a, b, ca=1, cb=0):
    return dg(a.astype(bf16), b.astype(bf16), ca, cb)


def halves(a):
    hi = a.astype(bf16)
    return hi, (a - hi.astype(f32)).astype(bf16)


def dot3(a, b, ca=1, cb=0):
    ah, al = halves(a)
    bh, bl = halves(b)
    return dg(ah, bh, ca, cb) + dg(ah, bl, ca, cb) + dg(al, bh, ca, cb)


def iota(shape, dim):
    return lax.broadcasted_iota(jnp.int32, shape, dim)


def softplus(a):
    return jnp.maximum(a, 0.0) + jnp.log(1.0 + jnp.exp(-jnp.abs(a)))


def sigmoid(a):
    return 1.0 / (1.0 + jnp.exp(-a))


def kernel(
    q_hbm, k_hbm, v_hbm, lg_hbm, pre_hbm, hdl_hbm, ex_hbm, wo_hbm,
    tok_hbm, sc_hbm, ch_hbm, grw_hbm, eld_hbm, wg_hbm, wu_hbm, wd_hbm,
    o1_ref, o2_ref,
    q_ref, k_ref, v_ref, wo_ref, tok_ref, lg_ref, pre_ref, hdl_ref, ex_ref, sc_ref, ch_ref, grw_ref, eld_ref,
    gu, dw, obuf, xbuf, ybuf, rbuf, dhop, bhop, h_s,
    a_s, s_s, x_s, ol_s, p_s, m_s, st_own, st_all, att_s,
    mine, theirs, pbuf, rrp, rrm, rsp, rsm,
    rs, rr, ps, pr, dsem, dhr, bsem, brecv, bhr,
    ssend, srecv, xs, qs, qr_p, qr_m, ins,
):
    ep = lax.axis_index("ep")
    tp = lax.axis_index("tp")
    z, c = tp // 2, tp % 2
    y, x = ep // 4, ep % 4
    up = ((z + 1) % NZ) * 2 + c
    down = ((z + NZ - 1) % NZ) * 2 + c
    mate = tp + 1 - 2 * c

    def peer(i):
        return ((y + i // 4) % 4) * 4 + (x + i % 4) % 4

    def loaded(n):
        pairs = (
            (wg_hbm.at[0], gu.at[z, 0, c]), (wu_hbm.at[0], gu.at[z, 1, c]),
            (tok_hbm, tok_ref), (k_hbm, k_ref), (q_hbm, q_ref), (v_hbm, v_ref), (wo_hbm, wo_ref),
            (sc_hbm, sc_ref), (ch_hbm, ch_ref), (lg_hbm, lg_ref), (pre_hbm, pre_ref), (hdl_hbm, hdl_ref),
            (ex_hbm, ex_ref), (grw_hbm, grw_ref), (eld_hbm, eld_ref),
            *((wd_hbm.at[0, :, pl.ds(n * COLS, COLS)], dw.at[n, z, c]) for n in range(CHUNKS)),
        )
        return pltpu.make_async_copy(*pairs[n], ins.at[(0, *range(14), 14, 15, 15, 15)[n]])

    barrier = pltpu.get_barrier_semaphore()
    for i in ORDER + DIRECT:
        pl.semaphore_signal(barrier, inc=1, device_id={"ep": peer(i)}, device_id_type=MESH)
    for t in (up, down, mate):
        pl.semaphore_signal(barrier, inc=1, device_id={"tp": t}, device_id_type=MESH)
    for n in (0, 1, 15, 2, 7, 8, 3, 4, 5, 9, 10, 11, 12, 13, 14, 16, 17, 18, 6):
        loaded(n).start()
    pl.semaphore_wait(barrier, EP - 1 + 3)

    def remote(src, dst, send, recv, **where):
        return pltpu.make_async_remote_copy(
            src_ref=src, dst_ref=dst, send_sem=send, recv_sem=recv, device_id=where, device_id_type=MESH
        )

    def absorb(like, sem):
        pltpu.make_async_copy(like, like, sem).wait()

    def place(zs, core, piece, rows):
        whole = gu.at[zs, piece, core] if piece < 2 else dw.at[piece - 2, zs, core]
        return whole if rows is None else whole.at[pl.ds(rows, SH // 2)]

    def ring(s, piece, forward):
        slot = (z + NZ - s) % NZ if forward else (z + s) % NZ
        rows = None if s < 3 else (0 if forward else SH // 2)
        here = place(slot, c, piece, rows)
        if forward:
            return remote(here, here, rs.at[min(piece // 2, 1)], rr.at[s, piece], tp=up)
        return remote(here, here, rs.at[min(piece // 2, 1)], rr.at[s, piece], tp=down)

    def arrived(s, piece):
        like = gu.at[0, 0] if piece < 2 else dw.at[0, 0]
        absorb(like if s < 3 else like.at[0], rr.at[s, piece])

    def across(n, piece):
        if n == 0:
            slot, rows = z, None
        elif n <= 3:
            slot, rows = (z + NZ - n) % NZ, None
        elif n <= 6:
            slot, rows = (z + n - 3) % NZ, None
        else:
            slot, rows = (z + 4) % NZ, (0 if n == 7 else SH // 2)
        here = place(slot, c, piece, rows)
        wave = 0 if n == 0 else (n - 1) % 3 + 1 if n < 7 else 4
        return remote(here, here, ps.at[min(piece // 2, 1)], pr.at[wave if piece < 2 else 3 + piece], tp=mate)

    def step(piece, s):
        if s == 0:
            across(0, piece).start()
            ring(0, piece, True).start()
            ring(0, piece, False).start()
            return
        arrived(s - 1, piece)
        ring(s, piece, True).start()
        ring(s, piece, False).start()
        across(s, piece).start()
        across(3 + s, piece).start()

    def finish(piece):
        arrived(3, piece)
        across(7, piece).start()
        across(8, piece).start()

    absorb(gu.at[0, :, 0], ins.at[0])
    loaded(15).wait()
    for piece in range(3):
        step(piece, 0)

    for n in (2, 7, 8):
        loaded(n).wait()
    wide = tok_ref[...].astype(f32)
    normed = (
        wide * lax.rsqrt(jnp.sum(wide * wide, axis=1, keepdims=True) * (1.0 / W) + EPS) * sc_ref[...]
    ).astype(bf16)
    eye = iota((TOK, TOK), 0) == iota((TOK, TOK), 1)
    first = jnp.sum(jnp.where(eye, ch_ref[0:1, :], 0), axis=1, keepdims=True)
    second = jnp.sum(jnp.where(eye, ch_ref[1:2, :], 0), axis=1, keepdims=True)
    lane16 = iota((TOK, EXPERTS), 1)
    is_first, is_second = lane16 == first, lane16 == second
    member = jnp.where(is_first | is_second, 1.0, 0.0)
    before = jnp.where(iota((TOK, TOK), 1) < iota((TOK, TOK), 0), 1.0, 0.0)
    spot = bdot(before, member) + (lane16 * CAP).astype(f32)
    slot1 = jnp.sum(jnp.where(is_first, spot, 0.0), axis=1, keepdims=True).astype(jnp.int32)
    slot2 = jnp.sum(jnp.where(is_second, spot, 0.0), axis=1, keepdims=True).astype(jnp.int32)
    lanes = iota((TOK, SLOTS), 1)
    pick1 = jnp.where(lanes == slot1, 1.0, 0.0).astype(bf16)
    pick2 = jnp.where(lanes == slot2, 1.0, 0.0).astype(bf16)
    obuf[...] = dg(pick1 + pick2, normed, 0, 0).astype(bf16)

    def route(src, dst, hop, send, recv, hsend, hrecv):
        def first_leg(i):
            block = src.at[pl.ds(peer(i) * CAP, CAP)]
            if i in RELAY:
                n = ORDER.index(i)
                return remote(block, hop.at[n], send, hrecv(n), ep=peer(RELAY[i]))
            return remote(block, dst.at[pl.ds(ep * CAP, CAP)], send, recv, ep=peer(i))

        def second_leg(i):
            n = ORDER.index(i)
            origin = peer(minus(0, RELAY[i]))
            there = dst.at[pl.ds(origin * CAP, CAP)]
            return remote(hop.at[n], there, hsend, recv, ep=peer(minus(i, RELAY[i])))

        def forward(lo, hi):
            absorb(hop.at[pl.ds(lo, hi - lo)], hrecv(lo))
            for i in ORDER[lo:hi]:
                second_leg(i).start()

        return first_leg, forward

    others = pl.ds(0, (EP - 1) * CAP)
    d_first, d_forward = route(obuf, xbuf, dhop, dsem.at[0], dsem.at[1], dsem.at[2], lambda n: dhr.at[n // 4])
    back = [
        route(
            ybuf.at[n], rbuf.at[n], bhop.at[n], bsem.at[0], brecv.at[n], bsem.at[1],
            lambda m, n=n: bhr.at[n + (m // 4 if n == CHUNKS - 1 else 0)],
        )
        for n in range(CHUNKS)
    ]
    for i in ORDER + DIRECT:
        d_first(i).start()
    home = pl.ds(pl.multiple_of(ep * CAP, CAP), CAP)
    xbuf[home, :] = obuf[home, :]

    for n in (3, 4, 5, 9, 10, 11, 12):
        loaded(n).wait()
    kb, qb = k_ref[...], q_ref[...]
    ld = -jnp.exp(jnp.full((1, 1), hdl_ref[0], f32)) * softplus(pre_ref[...].astype(f32)) + ex_ref[...]
    beta = sigmoid(lg_ref[...].astype(f32))
    kf = kb.astype(f32)
    k2h, k2l = halves(kf * kf)
    ones = jnp.ones((8, DH), bf16)
    rk_row = lax.rsqrt((dg(ones, k2h, 1, 1) + dg(ones, k2l, 1, 1))[0:1] + EPS)
    upper = jnp.where(iota((SEG, SEG), 0) <= iota((SEG, SEG), 1), 1.0, 0.0).astype(bf16)
    ld8 = jnp.broadcast_to(ld, (8, SEG))
    l1, rest = halves(ld8)
    l2 = (ld8 - l1.astype(f32) - rest.astype(f32)).astype(bf16)
    c_row = (dg(l1, upper) + dg(rest, upper) + dg(l2, upper))[0:1]
    last = c_row[:, SEG - 1 : SEG]
    rhs, kds, qds = [], [], []
    for n in range(SEG // DH):
        rows = slice(n * DH, (n + 1) * DH)
        ii = iota((DH, SEG), 0) + n * DH
        jj = iota((DH, SEG), 1)
        c_col = jnp.sum(jnp.where(jj <= ii, ld, 0.0), axis=1, keepdims=True)
        b_col = jnp.sum(jnp.where(jj == ii, beta, 0.0), axis=1, keepdims=True)
        kt = kf[rows]
        qt = qb[rows].astype(f32)
        rk_col = lax.rsqrt(jnp.sum(kt * kt, axis=1, keepdims=True) + EPS)
        rq_col = lax.rsqrt(jnp.sum(qt * qt, axis=1, keepdims=True) + EPS) * DH**-0.5
        decay = jnp.where(ii >= jj, jnp.exp(jnp.minimum(c_col - c_row, 0.0)), 0.0) * rk_row
        a_s[rows, :] = jnp.where(ii > jj, dg(kb[rows], kb, 1, 1) * decay * (b_col * rk_col), 0.0)
        s_s[rows, :] = dg(qb[rows], kb, 1, 1) * decay * rq_col
        kn = kt * rk_col
        ec = jnp.exp(c_col)
        rhs.append(jnp.concatenate([b_col * v_ref[rows, :].astype(f32), (b_col * ec) * kn], axis=1))
        p_s[rows, :] = qt * (rq_col * ec)
        ol_s[rows, :] = kn * jnp.exp(last - c_col)
    for n in range(SEG // DH):
        x_s[n * DH : (n + 1) * DH, :] = rhs[n]

    half = SEG // 2
    i2, j2 = iota((half, half), 0), iota((half, half), 1)

    def same(shift):
        return (i2 >> shift) == (j2 >> shift)

    big = [a_s[0:half, 0:half], a_s[half:, half:]]
    power = [jnp.where(same(4), -b, 0.0) for b in big]
    inv = [jnp.where(i2 == j2, 1.0, 0.0) + p for p in power]
    for _ in range(3):
        power = [dot3(p, p) for p in power]
        inv = [t + dot3(t, p) for t, p in zip(inv, power)]
    for shift in (4, 5, 6, 7):
        off = [jnp.where(same(shift + 1) & ~same(shift), b, 0.0) for b in big]
        mid = [dot3(t, o) for t, o in zip(inv, off)]
        inv = [t - dot3(m, t) for t, m in zip(inv, mid)]
    x1 = dot3(inv[0], x_s[0:half, :])
    x2 = dot3(inv[1], x_s[half:, :] - dot3(a_s[half:, 0:half], x1))
    x_s[0:half, :] = x1
    x_s[half:, :] = x2
    e = dot3(ol_s[...], x_s[...], 0, 0)
    diag = iota((DH, DH), 0) == iota((DH, DH), 1)
    st_own[:, 0:DH] = (jnp.where(diag, jnp.exp(last), 0.0) - e[:, DH:]).astype(bf16)
    st_own[:, DH:] = e[:, :DH].astype(bf16)

    def state(j):
        return remote(st_own, st_all.at[ep], ssend.at[j], srecv.at[ep], ep=j)

    for j in range(1, EP):

        @pl.when(ep < j)
        def _(j=j):
            state(j).start()

    step(0, 1)
    sx = dot3(s_s[...], x_s[...])
    ol_s[...] = sx[:, :DH]
    p_s[...] = p_s[...] - sx[:, DH:]
    d_forward(0, 4)
    step(1, 1)
    step(2, 1)
    absorb(dw.at[pl.ds(1, 3), 0, 0], ins.at[15])
    step(3, 0)
    d_forward(4, 7)
    step(0, 2)
    step(1, 2)
    step(2, 2)
    step(3, 1)

    m_s[...] = jnp.zeros((DH, DH), f32)
    for j in range(EP - 1):

        @pl.when(j < ep)
        def _(j=j):
            remote(st_own, st_all.at[j], ssend.at[0], srecv.at[j], ep=0).wait_recv()
            m_s[...] = bdot(st_all[j, :, 0:DH], m_s[...]) + st_all[j, :, DH:].astype(f32)

    att = (ol_s[...] + bdot(p_s[...], m_s[...])).astype(bf16)
    att_s[...] = att.reshape(NZ, 2, CAP, DH)
    for n in (6, 13, 14):
        loaded(n).wait()
    theirs[...] = dg(att_s[:, 1 - c].reshape(SEG // 2, DH), wo_ref[...]).astype(bf16).reshape(NZ, CAP, W)
    swap = remote(theirs, pbuf, xs.at[0], xs.at[1], tp=mate)
    swap.start()
    mine[...] = dg(att_s[:, c].reshape(SEG // 2, DH), wo_ref[...]).reshape(NZ, CAP, W)

    def grow(zs, k):
        cols = slice(k * W // 2, (k + 1) * W // 2)
        return mine[zs, :, cols] + pbuf[zs, :, cols].astype(f32)

    def sums(s, k, forward):
        if forward:
            return remote(rsp.at[s, k], rrp.at[s, k], qs.at[0], qr_p.at[s, k], tp=up)
        return remote(rsm.at[s, k], rrm.at[s, k], qs.at[1], qr_m.at[s, k], tp=down)

    def hidden(zs):
        weights = gu[zs].reshape(4 * SH, W)
        both = [dg(xbuf[rows, :], weights, 1, 1) for rows in ROWS]
        for rows, b in zip(ROWS, both):
            g, u = b[:, : 2 * SH], b[:, 2 * SH :]
            h_s[rows, pl.ds(pl.multiple_of(zs * 2 * SH, 2 * SH), 2 * SH)] = (g * sigmoid(g) * u).astype(bf16)

    def crossed(s):
        absorb(gu.at[0] if 0 < s < 4 else gu.at[0, 0], pr.at[s])

    def group(s):
        for zs in {0: (z,), 4: ((z + 4) % NZ,)}.get(s, ((z + NZ - s) % NZ, (z + s) % NZ)):
            hidden(zs)

    def results(n):
        absorb(dw.at[n, :, 0], pr.at[5 + n])
        weights = dw[n].reshape(16 * SH, COLS)
        block = 4 * CAP
        for pair in ((2, 1), (3, 0)):
            rows = [pl.ds(pl.multiple_of(((y + d) % 4) * block, block), block) for d in pair]
            both = dg(jnp.concatenate([h_s[r, :] for r in rows], axis=0), weights).astype(bf16)
            for k, r in enumerate(rows):
                ybuf[n, r, :] = both[k * block : (k + 1) * block]
            send(n, [i for i in ORDER if i // 4 in pair])
        rbuf[n, home, :] = ybuf[n, home, :]

    def send(n, messages):
        for i in messages:
            back[n][0](i).start()

    def relay(n):
        if n < CHUNKS - 1:
            back[n][1](0, 7)
        else:
            back[n][1](0, 4)
            back[n][1](4, 7)

    def begin(k):
        sums(0, k, True).start()
        sums(0, k, False).start()

    def add(s, k):
        sums(s - 1, k, True).wait_recv()
        rsp[s, k] = (rrp[s - 1, k].astype(f32) + grow((z + 4 - s) % NZ, k)).astype(bf16)
        sums(s, k, True).start()
        if s < 3:
            sums(s - 1, k, False).wait_recv()
            rsm[s, k] = (rrm[s - 1, k].astype(f32) + grow((z + NZ - 3 + s) % NZ, k)).astype(bf16)
            sums(s, k, False).start()

    def total(k):
        sums(2, k, False).wait_recv()
        sums(3, k, True).wait_recv()
        o1_ref[:, k * W // 2 : (k + 1) * W // 2] = (
            grow(z, k) + rrp[3, k].astype(f32) + rrm[2, k].astype(f32)
        ).astype(bf16)

    lead = sigmoid(eld_ref[...])
    w1 = jnp.sum(jnp.where(eye, grw_ref[...] * lead, 0.0), axis=1, keepdims=True)
    w2 = jnp.sum(jnp.where(eye, grw_ref[...] * (1.0 - lead), 0.0), axis=1, keepdims=True)

    def mix(n):
        absorb(rbuf.at[n, others], brecv.at[n])
        mixed = w1 * dg(pick1, rbuf[n]) + w2 * dg(pick2, rbuf[n])
        o2_ref[:, n * COLS : (n + 1) * COLS] = mixed.astype(bf16)

    step(0, 3)
    absorb(xbuf.at[others], dsem.at[1])
    crossed(0)
    group(0)
    crossed(1)
    group(1)
    step(1, 3)
    step(2, 3)
    step(4, 0)
    crossed(2)
    group(2)
    step(3, 2)
    step(5, 0)
    swap.wait_recv()
    for k in range(2):
        rsp[0, k] = grow((z + 4) % NZ, k).astype(bf16)
        rsm[0, k] = grow((z + NZ - 3) % NZ, k).astype(bf16)
    crossed(3)
    group(3)
    finish(0)
    finish(1)
    @pl.when(c == 0)
    def _():
        crossed(4)
        group(4)
        finish(2)
        results(0)
        send(0, DIRECT)
        step(4, 1)

    @pl.when(c == 1)
    def _():
        finish(2)
        step(4, 1)
        crossed(4)
        group(4)
        results(0)
        send(0, DIRECT)

    step(3, 3)
    step(5, 1)
    step(4, 2)
    begin(0)
    finish(3)
    step(5, 2)
    results(1)
    send(1, DIRECT)
    step(4, 3)
    begin(1)
    relay(0)
    step(5, 3)
    add(1, 0)
    finish(4)
    results(2)
    relay(1)
    add(1, 1)
    finish(5)
    results(3)
    send(2, DIRECT)
    add(2, 0)
    relay(2)
    send(3, DIRECT)
    add(2, 1)
    mix(0)
    mix(1)
    add(3, 0)
    relay(3)
    add(3, 1)
    mix(2)
    total(0)
    total(1)
    mix(3)

    absorb(gu.at[pl.ds(0, 7), :, 0], rs.at[0])
    absorb(dw.at[:, pl.ds(0, 7), 0], rs.at[1])
    absorb(gu.at[:, :, 0], ps.at[0])
    absorb(dw.at[:, :, 0], ps.at[1])
    absorb(obuf.at[others], dsem.at[0])
    absorb(dhop, dsem.at[2])
    absorb(ybuf.at[:, others], bsem.at[0])
    absorb(bhop, bsem.at[1])
    absorb(rsp, qs.at[0])
    absorb(rsm, qs.at[1])
    swap.wait_send()
    for j in range(1, EP):

        @pl.when(ep < j)
        def _(j=j):
            state(j).wait_send()


def shards(q, k, v, lg, pre, hdl, ex, wo, tok, sc, ch, grw, eld, wg, wu, wd):
    V = pltpu.VMEM
    dma = pltpu.SemaphoreType.DMA
    scratch = [
        V((SEG, DH), bf16), V((SEG, DH), bf16), V((SEG, DH), bf16), V((DH, W), bf16), V((TOK, W), bf16),
        V((1, SEG), bf16), V((1, SEG), bf16), pltpu.SMEM((1,), f32), V((1, SEG), f32),
        V((1, W), f32), V((2, TOK), jnp.int32), V((1, TOK), f32), V((1, TOK), f32),
        V((NZ, 2, 2, SH, W), bf16), V((CHUNKS, NZ, 2, SH, COLS), bf16),
        V((SLOTS, W), bf16), V((SLOTS, W), bf16), V((CHUNKS, SLOTS, COLS), bf16), V((CHUNKS, SLOTS, COLS), bf16),
        V((7, CAP, W), bf16), V((CHUNKS, 7, CAP, COLS), bf16), V((SLOTS, 16 * SH), bf16),
        V((SEG, SEG), f32), V((SEG, SEG), f32), V((SEG, 2 * DH), f32), V((SEG, DH), f32), V((SEG, DH), f32),
        V((DH, DH), f32), V((DH, 2 * DH), bf16), V((EP, DH, 2 * DH), bf16), V((NZ, 2, CAP, DH), bf16),
        V((NZ, CAP, W), f32), V((NZ, CAP, W), bf16), V((NZ, CAP, W), bf16),
        V((4, 2, CAP, W // 2), bf16), V((3, 2, CAP, W // 2), bf16),
        V((4, 2, CAP, W // 2), bf16), V((3, 2, CAP, W // 2), bf16),
        dma((2,)), dma((4, PIECES)), dma((2,)), dma((5 + CHUNKS,)),
        dma((3,)), dma((2,)), dma((2,)), dma((CHUNKS,)), dma((CHUNKS + 1,)),
        dma((EP,)), dma((EP,)), dma((2,)), dma((2,)), dma((4, 2)), dma((3, 2)), dma((16,)),
    ]
    vm = pl.BlockSpec(memory_space=pltpu.VMEM)
    hbm = pl.BlockSpec(memory_space=pl.ANY)
    outs = pl.pallas_call(
        kernel,
        name="mixer_and_experts",
        out_shape=(V((CAP, W), bf16), V((TOK, W), bf16)),
        in_specs=[hbm] * 16,
        out_specs=(vm, vm),
        scratch_shapes=scratch,
        compiler_params=pltpu.CompilerParams(
            collective_id=0, has_side_effects=True, vmem_limit_bytes=60 * 1024 * 1024
        ),
    )(
        q, k, v, lg, pre, hdl, ex, wo,
        tok, sc.reshape(1, W), ch.T, grw.reshape(1, TOK), eld.reshape(1, TOK), wg, wu, wd,
    )
    return pl.pallas_call(
        hand_over,
        name="hand_over",
        out_shape=(jax.ShapeDtypeStruct((CAP, W), bf16), jax.ShapeDtypeStruct((TOK, W), bf16)),
        in_specs=[vm, vm],
        out_specs=(vm, vm),
        compiler_params=pltpu.CompilerParams(vmem_limit_bytes=4 * 1024 * 1024),
    )(*outs)


def hand_over(a_ref, b_ref, c_ref, d_ref):
    c_ref[...] = a_ref[...]
    d_ref[...] = b_ref[...]


def solution(mesh):
    both = ("ep", "tp")
    placed = (
        P("ep", "tp"), P("ep", "tp"), P("ep", "tp"),
        P("tp", "ep"), P("tp", "ep"), P("tp"), P("tp", "ep"), P("tp", None),
        P(both, None), P(), P(both, None), P(both), P(both),
        P("ep", "tp", None), P("ep", "tp", None), P("ep", "tp", None),
    )
    return jax.shard_map(
        shards, mesh=mesh, in_specs=placed, out_specs=(P(both, None), P(both, None)), check_vma=False
    )
```
